256 devices in a mesh: ep: 64 (over z, y, core), tp: 4 (over x).
Axes of the slice: x: 4, y: 4, z: 8, core: 2. Of those that a mesh axis runs over, the one named last changes fastest.
Arguments:
- queries: bfloat16 [32768, 1536], P('ep', 'tp'), may hold values from -6 to 6
- keys: bfloat16 [32768, 1536], P('ep', 'tp'), may hold values from -6 to 6
- values: bfloat16 [32768, 1536], P('ep', 'tp'), may hold values from -6 to 6
- decay_gate_logits: float32 [32768, 12], P('ep', 'tp'), may hold values from -6 to 6
- correction_logits: bfloat16 [32768, 12], P('ep', 'tp'), may hold values from -6 to 6
- head_decay_speed: float32 [12], P('tp'), may hold values from 0 to 1
- position_log_decay: float32 [32768, 12], P('ep', 'tp'), may hold values from -1 to 0
- head_output_gain: float32 [128], replicated, may hold values from 0.1 to 1.9
- mixer_output_weight: bfloat16 [1536, 2048], P('tp'), may hold values from -0.15625 to 0.15625
- expert_input_tokens: bfloat16 [32768, 2048], P(('ep', 'tp')), may hold values from -6 to 6
- expert_norm_gain: float32 [2048], replicated, may hold values from 0.1 to 1.9
- routes: int32 [32768, 2], P(('ep', 'tp')), may hold values from 0 to 63, all different within a row; in each aligned block of 128 rows (0 to 127, 128 to 255, ...) at most 6 rows name the same one
- chosen_expert_weight: float32 [32768, 2], P(('ep', 'tp')), may hold values from 0.25 to 2.5
- routed_gate_weight: bfloat16 [64, 2048, 1024], P('ep', None, 'tp'), may hold values from -0.125 to 0.125
- routed_up_weight: bfloat16 [64, 2048, 1024], P('ep', None, 'tp'), may hold values from -0.125 to 0.125
- routed_down_weight: bfloat16 [64, 1024, 2048], P('ep', 'tp'), may hold values from -0.1875 to 0.1875
- common_gate_weight: bfloat16 [2048, 1024], P(None, 'tp'), may hold values from -0.125 to 0.125
- common_up_weight: bfloat16 [2048, 1024], P(None, 'tp'), may hold values from -0.125 to 0.125
- common_down_weight: bfloat16 [1024, 2048], P('tp'), may hold values from -0.1875 to 0.1875
Outputs:
- mixer_out: bfloat16 [32768, 2048], P(('ep', 'tp'))
- moe_out: bfloat16 [32768, 2048], P(('ep', 'tp'))
The draws below stay inside these ranges and needn't reach their ends.
Inputs may be any that keep to these rules, and one draw needn't show every extreme that they name: `routes`: each row names 2 different experts; the rows of one device name no expert more than 6 times, and some device names some expert exactly 6 times.
All inputs are finite; a program needn't handle non-finite values.
Results may differ from the reference program's by a relative error of at most 0.017.
Values may be sent and summed in bfloat16 or wider, within the bound.
A program may use at most 128 MiB of HBM per device.

```python
import math
import jax
import jax.numpy as jnp
import numpy as np
from jax import lax

D = 2048
HEADS = 12
HEAD_DIM = 128
BLOCK = 64
EXPERT_FF = 1024
SHARED_FF = 1024
TOP_K = 2
TOK_DEV = 128
EXPERTS = 64
CAP = 6
GROUP_ROWS = 512
TOKENS_A = 32768
TOKENS_B = 32768
N_EP = 64
N_TP = 4


def gentle_heads(key):
    order = jax.random.permutation(jax.random.fold_in(key, 41), HEADS)
    return order < max(1, HEADS // 4)


def draw_head_decay_speed(key, part):
    fast_share = 0.5
    gentle = gentle_heads(key)
    fast_head = (jax.random.uniform(jax.random.fold_in(key, 11), (HEADS,)) < fast_share) & jnp.logical_not(gentle)
    quick_rate = jax.random.uniform(jax.random.fold_in(key, 12), (HEADS,), jnp.float32, 0.02, 0.06)
    slow_rate = jax.random.uniform(jax.random.fold_in(key, 13), (HEADS,), jnp.float32, 0.5, 1.5) / TOKENS_A
    return jnp.where(fast_head, quick_rate, slow_rate).astype(jnp.float32)


def draw_correction_logits(key, part):
    gentle = gentle_heads(key)
    rough = jnp.clip(jax.random.normal(jax.random.fold_in(key, 42), (TOKENS_A, HEADS), jnp.float32), -6.0, 6.0)
    weak = jax.random.uniform(jax.random.fold_in(key, 43), (TOKENS_A, HEADS), jnp.float32, -6.0, -5.0)
    return jnp.where(gentle[None, :], weak, rough).astype(jnp.bfloat16)


def draw_position_log_decay(key, part):
    hit_draw = jax.random.uniform(jax.random.fold_in(key, 21), (TOKENS_A, HEADS))
    depth = jax.random.uniform(jax.random.fold_in(key, 22), (TOKENS_A, HEADS), jnp.float32, 0.5, 0.8)
    return jnp.where(hit_draw < 4.0 / TOKENS_A, jnp.log(depth), 0.0).astype(jnp.float32)


def draw_decay_gate_logits(key, part):
    lower_end = -1.5
    upper_end = 1.5
    base_draw = jax.random.normal(jax.random.fold_in(key, 31), (TOKENS_A, HEADS), jnp.float32)
    shifts = jax.random.uniform(jax.random.fold_in(key, 32), (TOKENS_A // GROUP_ROWS, 1), jnp.float32, lower_end, upper_end)
    owner = jnp.arange(TOKENS_A) // GROUP_ROWS
    return jnp.clip(base_draw + shifts[owner], -6.0, 6.0).astype(jnp.float32)


def block_scale(own_key, dims, split, low, top_value):
    def one(position, blocks):
        heights = jax.random.uniform(jax.random.fold_in(jax.random.fold_in(own_key, 6), position), (blocks,), jnp.float32, low / len(split), top_value / len(split))
        return jnp.repeat(jnp.exp(heights), dims[position] // blocks).reshape((-1,) + (1,) * (len(dims) - position - 1))

    gain = one(*split[0])
    for cut in split[1:]:
        gain = gain * one(*cut)
    return gain


def deal_out(key, own, number, rows, count, top, reach, skew):
    sequence = jax.random.permutation(key, count)
    heavy_load, common = portions_of(count, rows * top, reach, skew, True), portions_of(count, rows * top, reach, skew, False)
    places = jnp.arange(count)

    def named(sizes, offset_by):
        used = int((sizes > 0).sum())
        fixed = max(1, used // 4)
        moved = fixed + (places - fixed + offset_by * (used - fixed)) % max(1, count - fixed)
        return jnp.zeros((count,), jnp.int32).at[sequence[jnp.where(places < fixed, places, moved)]].set(jnp.asarray(sizes, jnp.int32))

    sizes = jnp.where(number % 4 == 0, named(heavy_load, number // 4), named(common, number - number // 4 - 1))
    mixed = jax.random.permutation(jax.random.fold_in(own, 3), count)
    giver, taker = mixed[0:count // 2 * 2:2], mixed[1:count // 2 * 2:2]
    margin = jnp.minimum(sizes[giver] - 1, reach - sizes[taker]) // 2
    margin = jnp.where((giver == sequence[0]) | (taker == sequence[0]) | (sizes[taker] == 0), 0, jnp.maximum(margin, 0))
    moved = jax.random.randint(jax.random.fold_in(own, 4), (count // 2,), 0, 1 << 20) % (margin + 1)
    sizes = sizes.at[giver].add(-moved).at[taker].add(moved)
    members = jnp.searchsorted(jnp.cumsum(sizes), jnp.arange(rows * top), side="right").astype(jnp.int32)
    grid = members.reshape(top, rows).T
    grid = grid[jax.random.permutation(jax.random.fold_in(own, 1), rows)]
    offset_by = jax.random.randint(jax.random.fold_in(own, 2), (rows, 1), 0, top)
    return jnp.take_along_axis(grid, (jnp.arange(top)[None, :] + offset_by) % top, axis=1)


def portions_of(amount, total, most, lean, full):
    loads = [(1 << 20) // math.isqrt(standing ** lean) + 1 for standing in range(1, amount + 1)]
    largest = most if full else min(most, max(-(-total // amount), total * loads[0] // sum(loads)))
    least = 1 if total - largest >= amount - 1 else 0
    counts, spare = [largest] + [least] * (amount - 1), total - largest - least * (amount - 1)
    while spare > 0:
        candidates = [i for i in range(1, amount) if counts[i] < largest] or [i for i in range(1, amount) if counts[i] < most]
        whole, budget = sum([loads[i] for i in candidates]), spare
        for i in candidates:
            addition = min(most - counts[i], max(1, budget * loads[i] // whole), spare)
            counts[i] = counts[i] + addition
            spare = spare - addition
    return np.array(counts)


def gaussian(rng, extent, deviation, bound, cuts=(), kind=jnp.bfloat16):
    array = jax.random.normal(rng, extent, jnp.float32) * deviation
    if len(cuts) > 0:
        array = block_scale(rng, extent, cuts, -0.22, 0.18) * array
    return jnp.clip(array, min=-bound, max=bound).astype(kind)


def setup_inputs(seed: int = 0) -> dict:
    seeds = jax.random.split(jax.random.key(seed), 20)
    queries = gaussian(seeds[0], (TOKENS_A, HEADS * HEAD_DIM), 1.0, 6.0, ((0, 64), (1, 4)))
    keys = gaussian(seeds[1], (TOKENS_A, HEADS * HEAD_DIM), 1.0, 6.0, ((0, 64), (1, 4)))
    values = gaussian(seeds[2], (TOKENS_A, HEADS * HEAD_DIM), 1.0, 6.0, ((0, 64), (1, 4)))
    decay_gate_logits = draw_decay_gate_logits(jax.random.fold_in(seeds[19], 71), 0)
    correction_logits = draw_correction_logits(jax.random.fold_in(seeds[19], 71), 0)
    head_decay_speed = draw_head_decay_speed(jax.random.fold_in(seeds[19], 71), 0)
    position_log_decay = draw_position_log_decay(jax.random.fold_in(seeds[19], 71), 0)
    head_output_gain = jnp.clip(1.0 + 0.18 * jax.random.normal(seeds[7], (HEAD_DIM,), jnp.float32), 0.1, 1.9)
    mixer_output_weight = gaussian(seeds[8], (HEADS * HEAD_DIM, D), (HEADS * HEAD_DIM) ** -0.5, 0.15625, ((0, 4),))
    expert_input_tokens = gaussian(seeds[9], (TOKENS_B, D), 1.0, 6.0, ((0, 256),))
    expert_norm_gain = jnp.clip(1.0 + 0.18 * jax.random.normal(seeds[10], (D,), jnp.float32), 0.1, 1.9)
    routes_keys = jax.random.split(jax.random.fold_in(seeds[11], 1), TOKENS_B // TOK_DEV)
    routes_turns = jax.random.permutation(jax.random.fold_in(seeds[11], 3), TOKENS_B // TOK_DEV)
    routes = jax.vmap(lambda own, number: deal_out(jax.random.fold_in(seeds[11], 2), own, number, TOK_DEV, EXPERTS, TOP_K, CAP, 2))(routes_keys, routes_turns).reshape((TOKENS_B, TOP_K))
    chosen_expert_weight = jnp.clip(jnp.exp(math.log(2.5) - 2.3025851 * jax.random.uniform(seeds[12], (TOKENS_B, TOP_K), jnp.float32) ** block_scale(seeds[12], (TOKENS_B, TOP_K), ((0, 256),), -0.2, 0.2)), 0.25, 2.5)
    routed_gate_weight = gaussian(seeds[13], (EXPERTS, D, EXPERT_FF), D ** -0.5, 0.125, ((0, 64), (2, 4)))
    routed_up_weight = gaussian(seeds[14], (EXPERTS, D, EXPERT_FF), D ** -0.5, 0.125, ((0, 64), (2, 4)))
    routed_down_weight = gaussian(seeds[15], (EXPERTS, EXPERT_FF, D), EXPERT_FF ** -0.5, 0.1875, ((0, 64), (1, 4)))
    common_gate_weight = gaussian(seeds[16], (D, SHARED_FF), D ** -0.5, 0.125, ((1, 4),))
    common_up_weight = gaussian(seeds[17], (D, SHARED_FF), D ** -0.5, 0.125, ((1, 4),))
    common_down_weight = gaussian(seeds[18], (SHARED_FF, D), SHARED_FF ** -0.5, 0.1875, ((0, 4),))
    return {"queries": queries, "keys": keys, "values": values, "decay_gate_logits": decay_gate_logits, "correction_logits": correction_logits, "head_decay_speed": head_decay_speed, "position_log_decay": position_log_decay, "head_output_gain": head_output_gain, "mixer_output_weight": mixer_output_weight, "expert_input_tokens": expert_input_tokens, "expert_norm_gain": expert_norm_gain, "routes": routes, "chosen_expert_weight": chosen_expert_weight, "routed_gate_weight": routed_gate_weight, "routed_up_weight": routed_up_weight, "routed_down_weight": routed_down_weight, "common_gate_weight": common_gate_weight, "common_up_weight": common_up_weight, "common_down_weight": common_down_weight}


EPS = 1e-06
HIGH = lax.Precision.HIGHEST

def separate_heads(source, number_of_heads):
    row_count = source.shape[0]
    shaped = source.astype(jnp.float32).reshape(row_count // BLOCK, BLOCK, number_of_heads, source.shape[1] // number_of_heads)
    return jnp.transpose(shaped, (2, 0, 1, 3))

def block_contributions(queries, keys, values, decay_gate_logits, correction_logits, head_decay_speed, position_log_decay):
    number_of_heads = decay_gate_logits.shape[1]
    q_heads = separate_heads(queries, number_of_heads)
    k_heads = separate_heads(keys, number_of_heads)
    v_heads = separate_heads(values, number_of_heads)
    q_heads = q_heads * lax.rsqrt(lax.optimization_barrier(jnp.sum(q_heads * q_heads, axis=-1, keepdims=True)) + EPS) * q_heads.shape[-1] ** (-0.5)
    k_heads = k_heads * lax.rsqrt(lax.optimization_barrier(jnp.sum(k_heads * k_heads, axis=-1, keepdims=True)) + EPS)
    decay_speed_column = head_decay_speed.astype(jnp.float32)[:, None, None]
    log_gate_value = -decay_speed_column * jax.nn.softplus(separate_heads(decay_gate_logits, number_of_heads)[..., 0]) + separate_heads(position_log_decay, number_of_heads)[..., 0]
    beta_gate = jax.nn.sigmoid(separate_heads(correction_logits, number_of_heads)[..., 0])
    cum_gate = jnp.cumsum(log_gate_value, axis=-1)
    positions = jnp.arange(log_gate_value.shape[-1])
    causal = positions[:, None] >= positions[None, :]
    strict = positions[:, None] > positions[None, :]
    decay_mat = jnp.exp(jnp.where(causal, cum_gate[..., :, None] - cum_gate[..., None, :], -jnp.inf))
    keyed = k_heads * beta_gate[..., None]
    lower_part = jnp.where(strict, jnp.einsum('hnld,hnsd->hnls', keyed, k_heads, precision=HIGH) * decay_mat, 0.0)
    right_side = jnp.concatenate([v_heads * beta_gate[..., None], keyed * jnp.exp(cum_gate)[..., None]], axis=-1)
    solved = lax.linalg.triangular_solve(lower_part, right_side, left_side=True, lower=True, unit_diagonal=True)
    value_width = v_heads.shape[-1]
    new_values = solved[..., :value_width]
    corr_weights = solved[..., value_width:]
    scores = jnp.einsum('hnld,hnsd->hnls', q_heads, k_heads, precision=HIGH) * decay_mat
    carried_keys = k_heads * jnp.exp(cum_gate[..., -1:] - cum_gate)[..., None]
    q_scaled = q_heads * jnp.exp(cum_gate)[..., None]
    return (q_scaled, cum_gate[..., -1], scores, new_values, corr_weights, carried_keys)

def advance(state, inputs):
    q_blk, last_blk, score_blk, value_blk, weight_blk, carry_blk = inputs
    corrected = value_blk - jnp.einsum('hld,hde->hle', weight_blk, state, precision=HIGH)
    output = jnp.einsum('hld,hde->hle', q_blk, state, precision=HIGH) + jnp.einsum('hls,hse->hle', score_blk, corrected, precision=HIGH)
    state = state * jnp.exp(last_blk)[:, None, None] + jnp.einsum('hld,hle->hde', carry_blk, corrected, precision=HIGH)
    return (state, output)

def finish_heads(outputs, head_output_gain):
    normed = outputs * lax.rsqrt(lax.optimization_barrier(jnp.mean(outputs * outputs, axis=-1, keepdims=True)) + EPS) * head_output_gain.astype(jnp.float32)
    block_count, number_of_heads, span_len, value_width = normed.shape
    normed = jnp.transpose(normed, (0, 2, 1, 3)).reshape(block_count * span_len, number_of_heads * value_width)
    return normed.astype(jnp.bfloat16)

def norm_rows(expert_input_tokens, expert_norm_gain):
    rows_f = expert_input_tokens.astype(jnp.float32)
    scaled = rows_f * lax.rsqrt(lax.optimization_barrier(jnp.mean(rows_f * rows_f, axis=-1, keepdims=True)) + EPS) * expert_norm_gain.astype(jnp.float32)
    return scaled.astype(jnp.bfloat16)

def gated_hidden(rows_in, w_gate, w_up):
    gate_val = jnp.dot(rows_in.astype(jnp.float32), w_gate.astype(jnp.float32), preferred_element_type=jnp.float32)
    up_val = jnp.dot(rows_in.astype(jnp.float32), w_up.astype(jnp.float32), preferred_element_type=jnp.float32)
    return (jax.nn.silu(gate_val) * up_val).astype(jnp.bfloat16)

def mix_routes(chosen_expert_weight, copies, shared):
    running = shared
    for slot_k in range(chosen_expert_weight.shape[1]):
        running = running + chosen_expert_weight[:, slot_k:slot_k + 1] * copies[:, slot_k].astype(jnp.float32)
    return running.astype(jnp.bfloat16)

def reference(queries, keys, values, decay_gate_logits, correction_logits, head_decay_speed, position_log_decay, head_output_gain, mixer_output_weight, expert_input_tokens, expert_norm_gain, routes, chosen_expert_weight, routed_gate_weight, routed_up_weight, routed_down_weight, common_gate_weight, common_up_weight, common_down_weight):
    summands = block_contributions(queries, keys, values, decay_gate_logits, correction_logits, head_decay_speed, position_log_decay)
    number_of_heads = summands[0].shape[0]
    key_width = summands[0].shape[-1]
    value_width = summands[3].shape[-1]
    inputs = tuple((jnp.moveaxis(item, 1, 0) for item in summands))
    zero_state = jnp.zeros((number_of_heads, key_width, value_width), jnp.float32)
    _, outputs = lax.scan(advance, zero_state, inputs)
    normed = finish_heads(outputs, head_output_gain)
    part_width = HEADS // N_TP * HEAD_DIM
    running = jnp.zeros((normed.shape[0], mixer_output_weight.shape[1]), jnp.float32)
    for member in range(N_TP):
        part_sum = jnp.dot(normed[:, member * part_width:(member + 1) * part_width].astype(jnp.float32), mixer_output_weight[member * part_width:(member + 1) * part_width].astype(jnp.float32), preferred_element_type=jnp.float32).astype(jnp.bfloat16)
        running = running + part_sum.astype(jnp.float32)
    mixer_out = running.astype(jnp.bfloat16)
    normed_in = norm_rows(expert_input_tokens, expert_norm_gain)
    token_count, top_k = routes.shape
    flat_routes = routes.reshape(-1).astype(jnp.int32)
    copy_count = flat_routes.shape[0]
    row_limit = N_EP * N_TP * CAP
    unit_width = EXPERT_FF // N_TP

    def one_expert(results, expert):
        chosen = flat_routes == expert
        before = jnp.cumsum(chosen.astype(jnp.int32)) - 1
        target = jnp.where(chosen, before, row_limit).astype(jnp.int32)
        owners = jnp.zeros((row_limit + 1,), jnp.int32).at[target].set(jnp.arange(copy_count, dtype=jnp.int32))
        in_use = jnp.arange(row_limit, dtype=jnp.int32) < jnp.sum(chosen.astype(jnp.int32))
        picked = owners[:row_limit]
        picked_rows = normed_in[(picked // top_k).astype(jnp.int32)]
        hidden = gated_hidden(picked_rows, routed_gate_weight[expert], routed_up_weight[expert])
        running_e = jnp.zeros((row_limit, normed_in.shape[1]), jnp.float32)
        for member in range(N_TP):
            part_sum = jnp.dot(hidden[:, member * unit_width:(member + 1) * unit_width].astype(jnp.float32), routed_down_weight[expert, member * unit_width:(member + 1) * unit_width].astype(jnp.float32), preferred_element_type=jnp.float32).astype(jnp.bfloat16)
            running_e = running_e + part_sum.astype(jnp.float32)
        result = running_e.astype(jnp.bfloat16)
        spots = jnp.where(in_use, picked, copy_count).astype(jnp.int32)
        results = results.at[spots].set(result, mode='drop')
        return (results, None)
    start_rows = jnp.zeros((copy_count, normed_in.shape[1]), jnp.bfloat16)
    copies, _ = lax.scan(one_expert, start_rows, jnp.arange(EXPERTS, dtype=jnp.int32))
    shared_hidden = gated_hidden(normed_in, common_gate_weight, common_up_weight)
    shared_width = SHARED_FF // N_TP
    shared = jnp.zeros((token_count, normed_in.shape[1]), jnp.float32)
    for member in range(N_TP):
        part_sum = jnp.dot(shared_hidden[:, member * shared_width:(member + 1) * shared_width].astype(jnp.float32), common_down_weight[member * shared_width:(member + 1) * shared_width].astype(jnp.float32), preferred_element_type=jnp.float32).astype(jnp.bfloat16)
        shared = shared + part_sum.astype(jnp.float32)
    moe_out = mix_routes(chosen_expert_weight, copies.reshape(token_count, top_k, -1), shared)
    return (mixer_out, moe_out)
```

```python
import functools

import jax
import jax.numpy as jnp
from jax import lax
from jax.experimental import pallas as pl
from jax.experimental.pallas import tpu as pltpu
from jax.sharding import Mesh
from jax.sharding import PartitionSpec as P

EP = ("ep_0", "ep_1", "ep_2")
EP_TP = ("ep_0", "ep_1", "ep_2", "tp")


EPS = 1e-06
HIGH = lax.Precision.HIGHEST
F32 = jnp.float32
BF16 = jnp.bfloat16
SLOT = 8


def halves(x):
    hi = x.astype(BF16)
    return hi, (x - hi.astype(F32)).astype(BF16)


def thirds(x):
    hi = x.astype(BF16)
    rest = x - hi.astype(F32)
    mid = rest.astype(BF16)
    return hi, mid, (rest - mid.astype(F32)).astype(BF16)


def mm(a, b):
    return jnp.dot(a, b, preferred_element_type=F32)


def dot3(a, b):
    ah, al = halves(a)
    bh, bl = halves(b)
    return mm(jnp.concatenate([ah, ah, al], 1), jnp.concatenate([bh, bl, bh], 0))


def dot2(a, b):
    ah, al = halves(a)
    return mm(jnp.concatenate([ah, al], 1), jnp.concatenate([b, b], 0))


def unit_lower_inverse(low, row, col):
    eye = (row == col).astype(F32)
    base = jnp.where((row >> 3) == (col >> 3), low, 0.0)
    squared = dot3(base, base)
    fourth = dot3(squared, squared)
    inv = eye - base
    inv = inv + dot3(inv, squared)
    inv = inv + dot3(inv, fourth)
    for bit in (3, 4, 5):
        across = jnp.where(
            ((row >> (bit + 1)) == (col >> (bit + 1))) & ((row >> bit) != (col >> bit)), low, 0.0
        )
        inv = inv - dot3(inv, dot3(across, inv))
    return inv


def local_mixer_kernel(
    q_ref, k_ref, v_ref, gate_ref, corr_ref, speed_ref, plog_ref, qt_ref, ol_ref, tr_ref, in_ref
):
    head = pl.program_id(0)
    heads = gate_ref.shape[1]
    rows = q_ref.shape[0]
    pair = 128
    lane_h = lax.broadcasted_iota(jnp.int32, (rows, heads), 1)
    here = lane_h == head

    log_gate = (
        -speed_ref[...]
        * (jnp.maximum(gate_ref[...], 0.0) + jnp.log1p(jnp.exp(-jnp.abs(gate_ref[...]))))
        + plog_ref[...]
    )
    beta_all = 1.0 / (1.0 + jnp.exp(-corr_ref[...].astype(F32)))
    g_col = jnp.sum(jnp.where(here, log_gate, 0.0), axis=1, keepdims=True)
    beta_col = jnp.sum(jnp.where(here, beta_all, 0.0), axis=1, keepdims=True)

    row = lax.broadcasted_iota(jnp.int32, (pair, pair), 0)
    col = lax.broadcasted_iota(jnp.int32, (pair, pair), 1)
    same = (row >> 6) == (col >> 6)
    causal = same & (row >= col)
    strict = same & (row > col)
    first = col < 64
    ones = causal.astype(BF16)
    ones = jnp.concatenate([ones, ones, ones], 1)

    packs = []
    for p in range(rows // pair):
        at = pl.ds(p * pair, pair)
        qb, kb, vb = q_ref[at, :], k_ref[at, :], v_ref[at, :]
        qf, kf = qb.astype(F32), kb.astype(F32)
        rq = lax.rsqrt(jnp.sum(qf * qf, axis=1, keepdims=True) + EPS) * (pair**-0.5)
        rk = lax.rsqrt(jnp.sum(kf * kf, axis=1, keepdims=True) + EPS)
        beta = beta_col[p * pair : (p + 1) * pair]
        g_mat = jnp.broadcast_to(g_col[p * pair : (p + 1) * pair], (pair, pair))
        c_mat = mm(ones, jnp.concatenate(thirds(g_mat), 0))
        c_row = c_mat.T
        last0, last1 = c_mat[63:64, :], c_mat[127:128, :]
        rk_row = jnp.broadcast_to(rk, (pair, pair)).T
        beta_row = jnp.broadcast_to(beta, (pair, pair)).T
        gram = lax.dot_general(
            jnp.concatenate([kb, qb], 0), kb, (((1,), (1,)), ((), ())), preferred_element_type=F32
        )
        decay = jnp.exp(jnp.where(causal, c_mat - c_row, -jnp.inf)) * rk_row
        low = jnp.where(strict, gram[:pair] * decay * (beta * rk), 0.0)
        scores = gram[pair:] * decay * rq
        inv = unit_lower_inverse(low, row, col)
        scale = beta_row * inv
        uw = jnp.concatenate(
            [dot2(scale, vb), dot2(scale * (jnp.exp(c_row) * rk_row), kb)], 1
        )
        suw = dot3(scores, uw)
        pq = qf * (rq * jnp.exp(c_mat)) - suw[:, pair:]
        tail = jnp.exp(jnp.where(first, last0, last1) - c_row)
        kt = kf.T * (tail * rk_row)
        kk = jnp.concatenate([jnp.where(first, kt, 0.0), jnp.where(first, 0.0, kt)], 0)
        mw = dot3(kk, uw)
        packs.append((suw[:, :pair], pq, mw, jnp.exp(last0), jnp.exp(last1)))

    ab = jnp.concatenate([(row == col).astype(F32), jnp.zeros((pair, pair), F32)], 1)
    for p, (su, pq, mw, keep0, keep1) in enumerate(packs):
        for b, keep in enumerate((keep0, keep1)):
            blk = slice(b * 64, (b + 1) * 64)
            at = pl.ds(p * pair + b * 64, 64)
            part = mw[b * pair : (b + 1) * pair]
            got = dot3(jnp.concatenate([pq[blk], part[:, pair:]], 0), ab)
            qt_ref[0, at, :] = got[:64, :pair]
            ol_ref[0, at, :] = got[:64, pair:] + su[blk]
            keep2 = jnp.concatenate([keep, keep], 1)
            ab = (
                keep2 * ab
                - got[64:]
                + jnp.concatenate([jnp.zeros((pair, pair), F32), part[:, :pair]], 1)
            )
    tr_ref[0] = ab[:, :pair]
    in_ref[0] = ab[:, pair:]


def local_mixer(queries, keys, values, gate, corr, speed, plog):
    rows, width = queries.shape
    heads = gate.shape[1]
    d = width // heads
    by_head = pl.BlockSpec((rows, d), lambda h: (0, h))
    whole = pl.BlockSpec((rows, heads), lambda h: (0, 0))
    return pl.pallas_call(
        local_mixer_kernel,
        grid=(heads,),
        in_specs=[
            by_head,
            by_head,
            by_head,
            whole,
            whole,
            pl.BlockSpec((1, heads), lambda h: (0, 0)),
            whole,
        ],
        out_specs=[
            pl.BlockSpec((1, rows, d), lambda h: (h, 0, 0)),
            pl.BlockSpec((1, rows, d), lambda h: (h, 0, 0)),
            pl.BlockSpec((1, d, d), lambda h: (h, 0, 0)),
            pl.BlockSpec((1, d, d), lambda h: (h, 0, 0)),
        ],
        out_shape=[
            jax.ShapeDtypeStruct((heads, rows, d), F32),
            jax.ShapeDtypeStruct((heads, rows, d), F32),
            jax.ShapeDtypeStruct((heads, d, d), F32),
            jax.ShapeDtypeStruct((heads, d, d), F32),
        ],
        cost_estimate=pl.CostEstimate(flops=30_000_000_000, bytes_accessed=4_000_000, transcendentals=0),
        name="local_mixer",
    )(queries, keys, values, gate, corr, speed.reshape(1, heads), plog)


def mixer_tail_kernel(qt_ref, ol_ref, state_ref, gain_ref, w_ref, out_ref):
    heads = qt_ref.shape[0]
    normed = []
    for h in range(heads):
        out = dot3(qt_ref[h], state_ref[h]) + ol_ref[h]
        out = out * lax.rsqrt(jnp.mean(out * out, axis=1, keepdims=True) + EPS) * gain_ref[...]
        normed.append(out.astype(BF16))
    out_ref[...] = mm(jnp.concatenate(normed, 1), w_ref[...]).astype(BF16)


def mixer_tail(qt, ol, state, gain, w):
    heads, rows, d = qt.shape
    width = w.shape[1]
    tile = 128
    return pl.pallas_call(
        mixer_tail_kernel,
        grid=(rows // tile,),
        in_specs=[
            pl.BlockSpec((heads, tile, d), lambda r: (0, r, 0)),
            pl.BlockSpec((heads, tile, d), lambda r: (0, r, 0)),
            pl.BlockSpec((heads, d, d), lambda r: (0, 0, 0)),
            pl.BlockSpec((1, d), lambda r: (0, 0)),
            pl.BlockSpec((heads * d, width), lambda r: (0, 0)),
        ],
        out_specs=pl.BlockSpec((tile, width), lambda r: (r, 0)),
        out_shape=jax.ShapeDtypeStruct((rows, width), BF16),
        cost_estimate=pl.CostEstimate(flops=3_000_000_000, bytes_accessed=6_000_000, transcendentals=0),
        name="mixer_tail",
    )(qt, ol, state, gain.reshape(1, d), w)


def dispatch_kernel(x_ref, gain_ref, routes_ref, weight_ref, xn_ref, out_ref, mix_ref):
    tokens = x_ref.shape[0]
    slots = out_ref.shape[0]
    x = x_ref[...].astype(F32)
    xn = (x * lax.rsqrt(jnp.mean(x * x, axis=1, keepdims=True) + EPS) * gain_ref[...]).astype(BF16)
    xn_ref[...] = xn
    lane = lax.broadcasted_iota(jnp.int32, (tokens, 128), 1)
    row = lax.broadcasted_iota(jnp.int32, (tokens, 128), 0)
    e0, e1 = routes_ref[:, 0:1], routes_ref[:, 1:2]
    chosen = ((lane == e0) | (lane == e1)).astype(BF16)
    before = mm((row > lane).astype(BF16), chosen)
    s0 = jnp.sum(jnp.where(lane == e0, before, 0.0), axis=1, keepdims=True)
    s1 = jnp.sum(jnp.where(lane == e1, before, 0.0), axis=1, keepdims=True)
    s0 = s0 + (e0 * SLOT).astype(F32)
    s1 = s1 + (e1 * SLOT).astype(F32)
    at = lax.broadcasted_iota(jnp.int32, (tokens, slots), 1).astype(F32)
    mix_ref[...] = jnp.where(at == s0, weight_ref[:, 0:1], 0.0) + jnp.where(
        at == s1, weight_ref[:, 1:2], 0.0
    )
    s0_row = jnp.broadcast_to(s0, (tokens, tokens)).T[0:1, :]
    s1_row = jnp.broadcast_to(s1, (tokens, tokens)).T[0:1, :]
    step = 128
    for base in range(0, slots, step):
        slot = (lax.broadcasted_iota(jnp.int32, (step, tokens), 0) + base).astype(F32)
        take = ((slot == s0_row) | (slot == s1_row)).astype(BF16)
        out_ref[base : base + step, :] = mm(take, xn).astype(BF16)


def dispatch(x, gain, routes, weight, experts):
    tokens, width = x.shape
    slots = experts * SLOT
    return pl.pallas_call(
        dispatch_kernel,
        out_shape=[
            jax.ShapeDtypeStruct((tokens, width), BF16),
            jax.ShapeDtypeStruct((slots, width), BF16),
            jax.ShapeDtypeStruct((tokens, slots), F32),
        ],
        name="dispatch",
    )(x, gain.reshape(1, width), routes, weight)


def combine_kernel(shared_ref, back_ref, mix_ref, out_ref):
    total = dot2(mix_ref[...], back_ref[...])
    for member in range(shared_ref.shape[0]):
        total = total + shared_ref[member].astype(F32)
    out_ref[...] = total.astype(BF16)


def combine(shared, back, mix):
    members, tokens, width = shared.shape
    slots = back.shape[0]
    tile = 512
    return pl.pallas_call(
        combine_kernel,
        grid=(width // tile,),
        in_specs=[
            pl.BlockSpec((members, tokens, tile), lambda c: (0, 0, c)),
            pl.BlockSpec((slots, tile), lambda c: (0, c)),
            pl.BlockSpec((tokens, slots), lambda c: (0, 0)),
        ],
        out_specs=pl.BlockSpec((tokens, tile), lambda c: (0, c)),
        out_shape=jax.ShapeDtypeStruct((tokens, width), BF16),
        name="combine",
    )(shared, back, mix)


def nothing_yet(x, identity):
    return jax.tree.map(
        lambda a, e: jnp.broadcast_to(jnp.asarray(e, a.dtype), a.shape), x, identity
    )


def carried_in(x, axes, combine, identity):
    before = start = nothing_yet(x, identity)
    so_far = x
    for axis in reversed(axes):
        peers, here = (lax.axis_size(axis), lax.axis_index(axis))
        pieces = jax.tree.map(
            lambda part, kind: lax.all_gather(part.astype(kind), axis),
            so_far,
            (jnp.bfloat16, jnp.bfloat16),
        )
        inside, so_far = (start, start)
        for k in range(peers):
            passed = k < here
            so_far = combine(
                so_far, jax.tree.map(lambda part, own: part[k].astype(own.dtype), pieces, x)
            )
            inside = jax.tree.map(lambda new, old: jnp.where(passed, new, old), so_far, inside)
        before = combine(inside, before)
    return before


def mat_product(left_mat, right_mat):
    return jnp.einsum("hde,hef->hdf", left_mat, right_mat, precision=HIGH)


def entry_state(trans, inject):
    heads, d, _ = trans.shape
    identity = jnp.broadcast_to(jnp.eye(d, dtype=F32), (heads, d, d))
    zero_state = jnp.zeros((heads, d, d), F32)

    def compose(earlier, later):
        return (mat_product(later[0], earlier[0]), mat_product(later[0], earlier[1]) + later[1])

    return carried_in((trans, inject), EP, compose, (identity, zero_state))[1]


def exchanged(x, axis):
    peers = lax.axis_size(axis)
    parts = x.reshape(peers, x.shape[0] // peers, *x.shape[1:])
    return lax.all_to_all(parts, axis, split_axis=0, concat_axis=0, tiled=True)


def from_everyone(x, axis):
    copies = jnp.broadcast_to(x, (lax.axis_size(axis), *x.shape))
    got = lax.all_to_all(copies, axis, split_axis=0, concat_axis=0, tiled=True)
    return got.reshape(-1, *x.shape[1:])


def ring_of_shards(gate, up, down, axis):
    peers = lax.axis_size(axis)
    right = [(i, (i + 1) % peers) for i in range(peers)]
    left = [(i, (i - 1) % peers) for i in range(peers)]
    from_left = [lax.ppermute(w, axis, right) for w in (gate, up, down)]
    from_right = [lax.ppermute(w, axis, left) for w in (gate, up, down)]
    half = up.shape[0] // 2
    far_gate = lax.ppermute(from_left[0], axis, right)
    far_up_0 = lax.ppermute(from_left[1][:half], axis, right)
    far_down = lax.ppermute(from_right[2], axis, left)
    far_up_1 = lax.ppermute(from_right[1][half:], axis, left)
    return from_left, from_right, (far_gate, (far_up_0, far_up_1), far_down)


def gated(gate_val, up_val):
    return (jax.nn.silu(gate_val) * up_val).astype(BF16)


def dot32(a, b):
    return jnp.dot(a, b, preferred_element_type=F32)


def shards(
    queries,
    keys,
    values,
    decay_gate_logits,
    correction_logits,
    head_decay_speed,
    position_log_decay,
    head_output_gain,
    mixer_output_weight,
    expert_input_tokens,
    expert_norm_gain,
    routes,
    chosen_expert_weight,
    routed_gate_weight,
    routed_up_weight,
    routed_down_weight,
    common_gate_weight,
    common_up_weight,
    common_down_weight,
):
    experts = lax.axis_size(EP)
    tokens, width = expert_input_tokens.shape
    own = (routed_gate_weight[0], routed_up_weight[0], routed_down_weight[0])
    from_left, from_right, far = ring_of_shards(*own, "tp")

    xn, outgoing, mix = dispatch(
        expert_input_tokens, expert_norm_gain, routes, chosen_expert_weight, experts
    )
    arrived = lax.all_to_all(
        outgoing.reshape(experts, SLOT, width), EP, split_axis=0, concat_axis=0, tiled=True
    ).reshape(experts * SLOT, width)
    group = from_everyone(xn, "tp")

    qt, ol, trans, inject = local_mixer(
        queries,
        keys,
        values,
        decay_gate_logits,
        correction_logits,
        head_decay_speed,
        position_log_decay,
    )
    state = entry_state(trans, inject)
    mixer_part = mixer_tail(qt, ol, state, head_output_gain, mixer_output_weight)
    mixer_got = exchanged(mixer_part, "tp")

    shared_hidden = gated(dot32(group, common_gate_weight), dot32(group, common_up_weight))
    shared_got = exchanged(dot32(shared_hidden, common_down_weight).astype(BF16), "tp")

    total = None
    for gate, up, down in (own, from_left, from_right):
        hidden = gated(dot32(arrived, gate), dot32(arrived, up))
        part = dot32(hidden, down)
        total = part if total is None else total + part
    gate, (up_0, up_1), down = far
    half = up_0.shape[0]
    hidden = gated(
        dot32(arrived, gate), dot32(arrived[:, :half], up_0) + dot32(arrived[:, half:], up_1)
    )
    total = (total + dot32(hidden, down)).astype(BF16)
    back = lax.all_to_all(
        total.reshape(experts, SLOT, width), EP, split_axis=0, concat_axis=0, tiled=True
    ).reshape(experts * SLOT, width)

    mixer_out = mixer_got.astype(F32).sum(axis=0).astype(BF16)
    moe_out = combine(shared_got, back, mix)
    return (mixer_out, moe_out)


def solution(mesh):
    finer = Mesh(mesh.devices.reshape(8, 4, 2, mesh.shape["tp"]), ("ep_0", "ep_1", "ep_2", "tp"))
    placed = (
        P(EP, "tp"),
        P(EP, "tp"),
        P(EP, "tp"),
        P(EP, "tp"),
        P(EP, "tp"),
        P("tp"),
        P(EP, "tp"),
        P(),
        P("tp", None),
        P(EP_TP, None),
        P(),
        P(EP_TP, None),
        P(EP_TP, None),
        P(EP, None, "tp"),
        P(EP, None, "tp"),
        P(EP, "tp", None),
        P(None, "tp"),
        P(None, "tp"),
        P("tp", None),
    )
    return jax.shard_map(
        shards,
        mesh=finer,
        in_specs=placed,
        out_specs=(P(EP_TP, None), P(EP_TP, None)),
        check_vma=False,
    )
```

```python
import jax
import jax.numpy as jnp
from jax import lax
from jax.experimental import pallas as pl
from jax.experimental.pallas import tpu as pltpu
from jax.sharding import Mesh
from jax.sharding import PartitionSpec as P

EP = ("ep_0", "ep_1", "ep_2")
EP_TP = ("ep_0", "ep_1", "ep_2", "tp")


EPS = 1e-06
F32 = jnp.float32
BF16 = jnp.bfloat16
SLOT = 8
MESH = pl.DeviceIdType.MESH


def halves(x):
    hi = x.astype(BF16)
    return hi, (x - hi.astype(F32)).astype(BF16)


def thirds(x):
    hi = x.astype(BF16)
    rest = x - hi.astype(F32)
    mid = rest.astype(BF16)
    return hi, mid, (rest - mid.astype(F32)).astype(BF16)


def mm(a, b):
    return jnp.dot(a, b, preferred_element_type=F32)


def dot3(a, b):
    ah, al = halves(a)
    bh, bl = halves(b)
    return mm(jnp.concatenate([ah, ah, al], 1), jnp.concatenate([bh, bl, bh], 0))


def dot2(a, b):
    ah, al = halves(a)
    return mm(jnp.concatenate([ah, al], 1), jnp.concatenate([b, b], 0))


def unit_lower_inverse(low, row, col):
    eye = (row == col).astype(F32)
    base = jnp.where((row >> 3) == (col >> 3), low, 0.0)
    squared = dot3(base, base)
    fourth = dot3(squared, squared)
    inv = eye - base
    inv = inv + dot3(inv, squared)
    inv = inv + dot3(inv, fourth)
    for bit in (3, 4, 5):
        across = jnp.where(
            ((row >> (bit + 1)) == (col >> (bit + 1))) & ((row >> bit) != (col >> bit)), low, 0.0
        )
        inv = inv - dot3(inv, dot3(across, inv))
    return inv


def local_mixer_kernel(
    q_ref, k_ref, v_ref, gate_ref, corr_ref, speed_ref, plog_ref, qt_ref, ol_ref, tr_ref, in_ref
):
    head = pl.program_id(0)
    heads = gate_ref.shape[1]
    rows = q_ref.shape[0]
    pair = 128
    lane_h = lax.broadcasted_iota(jnp.int32, (rows, heads), 1)
    here = lane_h == head

    log_gate = (
        -speed_ref[...]
        * (jnp.maximum(gate_ref[...], 0.0) + jnp.log1p(jnp.exp(-jnp.abs(gate_ref[...]))))
        + plog_ref[...]
    )
    beta_all = 1.0 / (1.0 + jnp.exp(-corr_ref[...].astype(F32)))
    g_col = jnp.sum(jnp.where(here, log_gate, 0.0), axis=1, keepdims=True)
    beta_col = jnp.sum(jnp.where(here, beta_all, 0.0), axis=1, keepdims=True)

    row = lax.broadcasted_iota(jnp.int32, (pair, pair), 0)
    col = lax.broadcasted_iota(jnp.int32, (pair, pair), 1)
    same = (row >> 6) == (col >> 6)
    causal = same & (row >= col)
    strict = same & (row > col)
    first = col < 64
    ones = causal.astype(BF16)
    ones = jnp.concatenate([ones, ones, ones], 1)

    packs = []
    for p in range(rows // pair):
        at = pl.ds(p * pair, pair)
        qb, kb, vb = q_ref[at, :], k_ref[at, :], v_ref[at, :]
        qf, kf = qb.astype(F32), kb.astype(F32)
        rq = lax.rsqrt(jnp.sum(qf * qf, axis=1, keepdims=True) + EPS) * (pair**-0.5)
        rk = lax.rsqrt(jnp.sum(kf * kf, axis=1, keepdims=True) + EPS)
        beta = beta_col[p * pair : (p + 1) * pair]
        g_mat = jnp.broadcast_to(g_col[p * pair : (p + 1) * pair], (pair, pair))
        c_mat = mm(ones, jnp.concatenate(thirds(g_mat), 0))
        c_row = c_mat.T
        last0, last1 = c_mat[63:64, :], c_mat[127:128, :]
        rk_row = jnp.broadcast_to(rk, (pair, pair)).T
        beta_row = jnp.broadcast_to(beta, (pair, pair)).T
        gram = lax.dot_general(
            jnp.concatenate([kb, qb], 0), kb, (((1,), (1,)), ((), ())), preferred_element_type=F32
        )
        decay = jnp.exp(jnp.where(causal, c_mat - c_row, -jnp.inf)) * rk_row
        low = jnp.where(strict, gram[:pair] * decay * (beta * rk), 0.0)
        scores = gram[pair:] * decay * rq
        inv = unit_lower_inverse(low, row, col)
        scale = beta_row * inv
        uw = jnp.concatenate(
            [dot2(scale, vb), dot2(scale * (jnp.exp(c_row) * rk_row), kb)], 1
        )
        suw = dot3(scores, uw)
        pq = qf * (rq * jnp.exp(c_mat)) - suw[:, pair:]
        tail = jnp.exp(jnp.where(first, last0, last1) - c_row)
        kt = kf.T * (tail * rk_row)
        kk = jnp.concatenate([jnp.where(first, kt, 0.0), jnp.where(first, 0.0, kt)], 0)
        mw = dot3(kk, uw)
        packs.append((suw[:, :pair], pq, mw, jnp.exp(last0), jnp.exp(last1)))

    ab = jnp.concatenate([(row == col).astype(F32), jnp.zeros((pair, pair), F32)], 1)
    for p, (su, pq, mw, keep0, keep1) in enumerate(packs):
        for b, keep in enumerate((keep0, keep1)):
            blk = slice(b * 64, (b + 1) * 64)
            at = pl.ds(p * pair + b * 64, 64)
            part = mw[b * pair : (b + 1) * pair]
            got = dot3(jnp.concatenate([pq[blk], part[:, pair:]], 0), ab)
            qt_ref[0, at, :] = got[:64, :pair]
            ol_ref[0, at, :] = got[:64, pair:] + su[blk]
            keep2 = jnp.concatenate([keep, keep], 1)
            ab = (
                keep2 * ab
                - got[64:]
                + jnp.concatenate([jnp.zeros((pair, pair), F32), part[:, :pair]], 1)
            )
    tr_ref[0] = ab[:, :pair]
    in_ref[0] = ab[:, pair:]


def local_mixer(queries, keys, values, gate, corr, speed, plog):
    rows, width = queries.shape
    heads = gate.shape[1]
    d = width // heads
    by_head = pl.BlockSpec((rows, d), lambda h: (0, h))
    whole = pl.BlockSpec((rows, heads), lambda h: (0, 0))
    return pl.pallas_call(
        local_mixer_kernel,
        grid=(heads,),
        in_specs=[
            by_head,
            by_head,
            by_head,
            whole,
            whole,
            pl.BlockSpec((1, heads), lambda h: (0, 0)),
            whole,
        ],
        out_specs=[
            pl.BlockSpec((1, rows, d), lambda h: (h, 0, 0)),
            pl.BlockSpec((1, rows, d), lambda h: (h, 0, 0)),
            pl.BlockSpec((1, d, d), lambda h: (h, 0, 0)),
            pl.BlockSpec((1, d, d), lambda h: (h, 0, 0)),
        ],
        out_shape=[
            jax.ShapeDtypeStruct((heads, rows, d), F32),
            jax.ShapeDtypeStruct((heads, rows, d), F32),
            jax.ShapeDtypeStruct((heads, d, d), F32),
            jax.ShapeDtypeStruct((heads, d, d), F32),
        ],
        cost_estimate=pl.CostEstimate(flops=30_000_000_000, bytes_accessed=4_000_000, transcendentals=0),
        name="local_mixer",
    )(queries, keys, values, gate, corr, speed.reshape(1, heads), plog)


def entry_state_kernel(
    t_ref, i_ref, s_ref, own, peer, ypack, zpack,
    send_c, recv_c, send_y, recv_y, send_yc, recv_yc,
    send_r, recv_r, send_l, recv_l, send_rc, recv_rc, send_lc, recv_lc,
):
    heads, d, _ = t_ref.shape
    half = d // 2
    nz, ny = zpack.shape[0], ypack.shape[0]
    z, y, c = lax.axis_index("ep_0"), lax.axis_index("ep_1"), lax.axis_index("ep_2")
    other = {"ep_2": 1 - c}
    right, left = {"ep_0": lax.rem(z + 1, nz)}, {"ep_0": lax.rem(z + nz - 1, nz)}
    across = [{"ep_1": lax.rem(y + k, ny)} for k in range(1, ny)]

    barrier = pltpu.get_barrier_semaphore()
    for who in (other, right, left, *across):
        pl.semaphore_signal(barrier, inc=1, device_id=who, device_id_type=MESH)
    pl.semaphore_wait(barrier, 3 + len(across))

    def send(src, dst, send_sem, recv_sem, who):
        return pltpu.make_async_remote_copy(
            src_ref=src, dst_ref=dst, send_sem=send_sem, recv_sem=recv_sem,
            device_id=who, device_id_type=MESH,
        )

    def store(ref, h, both):
        both = both.astype(BF16)
        ref[0, h] = both[:half]
        ref[1, h] = both[half:]

    def load(ref, h):
        return jnp.concatenate([ref[0, h], ref[1, h]], 0)

    def after(pack, so_far):
        hi, lo = halves(so_far)
        t = pack[:, :d]
        return mm(jnp.concatenate([t, t], 1), jnp.concatenate([hi, lo], 0))

    def added(pack):
        return pack[:, d:].astype(F32)

    nothing = jnp.zeros((d, d), F32)
    for h in range(heads):
        store(own, h, jnp.concatenate([t_ref[h], i_ref[h]], 1))
    swap = send(own, peer, send_c, recv_c, other)
    swap.start()
    swap.wait()
    for h in range(heads):
        mine, theirs = load(own, h), load(peer, h)
        early = jnp.where(c == 0, mine.astype(F32), theirs.astype(F32)).astype(BF16)
        late = jnp.where(c == 0, theirs.astype(F32), mine.astype(F32)).astype(BF16)
        both = mm(late[:, :d], early) + jnp.concatenate([nothing, added(late)], 1)
        store(ypack.at[y], h, both)

    out = [
        send(ypack.at[y, c], ypack.at[y, c], send_y.at[k - 1], recv_y.at[k - 1], across[k - 1])
        for k in range(1, ny)
    ]
    for copy in out:
        copy.start()
    over = []
    for k in range(1, ny):
        slot = ypack.at[lax.rem(y + ny - k, ny), c]
        out[k - 1].wait_recv()
        over.append(send(slot, slot, send_yc.at[k - 1], recv_yc.at[k - 1], other))
        over[-1].start()
    for copy in out:
        copy.wait_send()
    for copy in over:
        copy.wait()
    for h in range(heads):
        both = load(ypack.at[0], h).astype(F32)
        for k in range(1, ny):
            pack = load(ypack.at[k], h)
            both = after(pack, both) + jnp.concatenate([nothing, added(pack)], 1)
        store(zpack.at[z], h, both)

    def going(r, h, sign, who, send_sem, recv_sem):
        slot = zpack.at[lax.rem(z + nz - sign * (r - 1), nz), c, h]
        return send(slot, slot, send_sem.at[r - 1, h], recv_sem.at[r - 1, h], who)

    def shared_with_other(r, h, sign, send_sem, recv_sem):
        slot = zpack.at[lax.rem(z + nz - sign * r, nz), c, h]
        return send(slot, slot, send_sem.at[r - 1, h], recv_sem.at[r - 1, h], other)

    rings = (
        (nz // 2, 1, right, send_r, recv_r, send_rc, recv_rc),
        ((nz - 1) // 2, -1, left, send_l, recv_l, send_lc, recv_lc),
    )
    pending = []
    for rounds, sign, who, ss, rs, _, _ in rings:
        for h in range(heads):
            if rounds > 0:
                going(1, h, sign, who, ss, rs).start()
    for r in range(1, nz // 2 + 1):
        for h in range(heads):
            for rounds, sign, who, ss, rs, sc, rc in rings:
                if r > rounds:
                    continue
                copy = going(r, h, sign, who, ss, rs)
                copy.wait_recv()
                pending.append((copy, False))
                if r < rounds:
                    going(r + 1, h, sign, who, ss, rs).start()
                hand = shared_with_other(r, h, sign, sc, rc)
                hand.start()
                pending.append((hand, True))
    for copy, both_ways in pending:
        copy.wait_send()
        if both_ways:
            copy.wait_recv()

    for h in range(heads):
        s_ref[h] = nothing
    for k in range(nz - 1):
        for h in range(heads):
            pack = load(zpack.at[k], h)
            s_ref[h] = jnp.where(k < z, after(pack, s_ref[h]) + added(pack), s_ref[h])
    for k in range(ny - 1):
        for h in range(heads):
            pack = load(ypack.at[k], h)
            s_ref[h] = jnp.where(k < y, after(pack, s_ref[h]) + added(pack), s_ref[h])
    for h in range(heads):
        pack = load(peer, h)
        s_ref[h] = jnp.where(c == 1, after(pack, s_ref[h]) + added(pack), s_ref[h])


def entry_state(trans, inject):
    heads, d, _ = trans.shape
    nz, ny = lax.axis_size("ep_0"), lax.axis_size("ep_1")
    half = (2, heads, d // 2, 2 * d)
    dma = pltpu.SemaphoreType.DMA
    rounds = max(nz // 2, 1)
    vmem = pl.BlockSpec(memory_space=pltpu.VMEM)
    return pl.pallas_call(
        entry_state_kernel,
        in_specs=[vmem, vmem],
        out_specs=vmem,
        out_shape=jax.ShapeDtypeStruct((heads, d, d), F32),
        scratch_shapes=[
            pltpu.VMEM(half, BF16),
            pltpu.VMEM(half, BF16),
            pltpu.VMEM((ny, *half), BF16),
            pltpu.VMEM((nz, *half), BF16),
            dma, dma,
            dma((max(ny - 1, 1),)), dma((max(ny - 1, 1),)), dma((max(ny - 1, 1),)), dma((max(ny - 1, 1),)),
            *[dma((rounds, heads)) for _ in range(8)],
        ],
        compiler_params=pltpu.CompilerParams(collective_id=0, has_side_effects=True),
        cost_estimate=pl.CostEstimate(flops=30_000_000_000, bytes_accessed=4_000_000, transcendentals=0),
        name="entry_state",
    )(trans, inject)


def parts_kernel(
    me_ref, qt_ref, ol_ref, state_ref, gain_ref, w_ref, x_ref, gate_ref, up_ref, down_ref, out_ref
):
    heads, tile, _ = qt_ref.shape
    normed = []
    for h in range(heads):
        out = dot3(qt_ref[h], state_ref[h]) + ol_ref[h]
        out = out * lax.rsqrt(jnp.mean(out * out, axis=1, keepdims=True) + EPS) * gain_ref[...]
        normed.append(out.astype(BF16))
    out_ref[0, :tile] = mm(jnp.concatenate(normed, 1), w_ref[...]).astype(BF16)
    x = x_ref[...]
    hidden = gated(mm(x, gate_ref[...]), mm(x, up_ref[...]))
    out_ref[0, tile:] = mm(hidden, down_ref[...]).astype(BF16)


def parts_for_peers(me, peers, qt, ol, state, gain, w, group, gate, up, down):
    heads, rows, d = qt.shape
    width = w.shape[1]
    tile = rows // peers

    def whole(x):
        return pl.BlockSpec(x.shape, lambda r, me: (0,) * x.ndim)

    def turn(r, me):
        return lax.rem(me[0] + r, peers)

    gain = gain.reshape(1, d)
    return pl.pallas_call(
        parts_kernel,
        grid_spec=pltpu.PrefetchScalarGridSpec(
            num_scalar_prefetch=1,
            grid=(peers,),
            in_specs=[
                pl.BlockSpec((heads, tile, d), lambda r, me: (0, turn(r, me), 0)),
                pl.BlockSpec((heads, tile, d), lambda r, me: (0, turn(r, me), 0)),
                whole(state),
                whole(gain),
                whole(w),
                pl.BlockSpec((tile, group.shape[1]), lambda r, me: (turn(r, me), 0)),
                whole(gate),
                whole(up),
                whole(down),
            ],
            out_specs=pl.BlockSpec((1, 2 * tile, width), lambda r, me: (r, 0, 0)),
        ),
        out_shape=jax.ShapeDtypeStruct((peers, 2 * tile, width), BF16),
        cost_estimate=pl.CostEstimate(flops=6_000_000_000, bytes_accessed=12_000_000, transcendentals=0),
        name="parts_for_peers",
    )(me, qt, ol, state, gain, w, group, gate, up, down)


def near_experts_kernel(x_ref, *refs):
    *weights, out_ref = refs
    x = x_ref[...]
    total = None
    for m in range(0, len(weights), 3):
        gate, up, down = weights[m : m + 3]
        part = mm(gated(mm(x, gate[...]), mm(x, up[...])), down[...])
        total = part if total is None else total + part
    out_ref[...] = total


def near_experts(x, shards_):
    rows, width = x.shape
    tile = 128
    weights = [w for shard in shards_ for w in shard]
    return pl.pallas_call(
        near_experts_kernel,
        grid=(rows // tile,),
        in_specs=[pl.BlockSpec((tile, width), lambda r: (r, 0))]
        + [pl.BlockSpec(w.shape, lambda r: (0, 0)) for w in weights],
        out_specs=pl.BlockSpec((tile, width), lambda r: (r, 0)),
        out_shape=jax.ShapeDtypeStruct((rows, width), F32),
        cost_estimate=pl.CostEstimate(flops=5_000_000_000, bytes_accessed=16_000_000, transcendentals=0),
        name="near_experts",
    )(x, *weights)


def far_expert_kernel(x_ref, near_ref, gate_ref, up0_ref, up1_ref, down_ref, out_ref):
    x = x_ref[...]
    half = up0_ref.shape[0]
    up = mm(x[:, :half], up0_ref[...]) + mm(x[:, half:], up1_ref[...])
    total = near_ref[...] + mm(gated(mm(x, gate_ref[...]), up), down_ref[...])
    out_ref[...] = total.astype(BF16)


def far_expert(x, near, gate, up0, up1, down):
    rows, width = x.shape
    tile = 128
    weights = (gate, up0, up1, down)
    by_rows = pl.BlockSpec((tile, width), lambda r: (r, 0))
    return pl.pallas_call(
        far_expert_kernel,
        grid=(rows // tile,),
        in_specs=[by_rows, by_rows] + [pl.BlockSpec(w.shape, lambda r: (0, 0)) for w in weights],
        out_specs=by_rows,
        out_shape=jax.ShapeDtypeStruct((rows, width), BF16),
        cost_estimate=pl.CostEstimate(flops=2_000_000_000, bytes_accessed=12_000_000, transcendentals=0),
        name="far_expert",
    )(x, near, *weights)


def dispatch_kernel(x_ref, gain_ref, routes_ref, weight_ref, xn_ref, out_ref, mix_ref):
    tokens = x_ref.shape[0]
    slots = out_ref.shape[0]
    x = x_ref[...].astype(F32)
    xn = (x * lax.rsqrt(jnp.mean(x * x, axis=1, keepdims=True) + EPS) * gain_ref[...]).astype(BF16)
    xn_ref[...] = xn
    lane = lax.broadcasted_iota(jnp.int32, (tokens, 128), 1)
    row = lax.broadcasted_iota(jnp.int32, (tokens, 128), 0)
    e0, e1 = routes_ref[:, 0:1], routes_ref[:, 1:2]
    chosen = ((lane == e0) | (lane == e1)).astype(BF16)
    before = mm((row > lane).astype(BF16), chosen)
    s0 = jnp.sum(jnp.where(lane == e0, before, 0.0), axis=1, keepdims=True)
    s1 = jnp.sum(jnp.where(lane == e1, before, 0.0), axis=1, keepdims=True)
    s0 = s0 + (e0 * SLOT).astype(F32)
    s1 = s1 + (e1 * SLOT).astype(F32)
    at = lax.broadcasted_iota(jnp.int32, (tokens, slots), 1).astype(F32)
    mix_ref[...] = jnp.where(at == s0, weight_ref[:, 0:1], 0.0) + jnp.where(
        at == s1, weight_ref[:, 1:2], 0.0
    )
    s0_row = jnp.broadcast_to(s0, (tokens, tokens)).T[0:1, :]
    s1_row = jnp.broadcast_to(s1, (tokens, tokens)).T[0:1, :]
    step = 128
    for base in range(0, slots, step):
        slot = (lax.broadcasted_iota(jnp.int32, (step, tokens), 0) + base).astype(F32)
        take = ((slot == s0_row) | (slot == s1_row)).astype(BF16)
        out_ref[base : base + step, :] = mm(take, xn).astype(BF16)


def dispatch(x, gain, routes, weight, experts):
    tokens, width = x.shape
    slots = experts * SLOT
    return pl.pallas_call(
        dispatch_kernel,
        out_shape=[
            jax.ShapeDtypeStruct((tokens, width), BF16),
            jax.ShapeDtypeStruct((slots, width), BF16),
            jax.ShapeDtypeStruct((tokens, slots), F32),
        ],
        name="dispatch",
    )(x, gain.reshape(1, width), routes, weight)


def combine_kernel(p0_ref, p1_ref, p2_ref, p3_ref, back_ref, mix_ref, mixer_ref, moe_ref):
    tokens = moe_ref.shape[0]
    total = dot2(mix_ref[...], back_ref[...])
    mixer = jnp.zeros_like(total)
    for part in (p0_ref, p1_ref, p2_ref, p3_ref):
        mixer = mixer + part[:tokens].astype(F32)
        total = total + part[tokens:].astype(F32)
    mixer_ref[...] = mixer.astype(BF16)
    moe_ref[...] = total.astype(BF16)


def combine(parts, back, mix):
    tokens, slots = mix.shape
    width = back.shape[1]
    tile = 512
    part = pl.BlockSpec((2 * tokens, tile), lambda c: (0, c))
    out = pl.BlockSpec((tokens, tile), lambda c: (0, c))
    return pl.pallas_call(
        combine_kernel,
        grid=(width // tile,),
        in_specs=[part] * 4
        + [
            pl.BlockSpec((slots, tile), lambda c: (0, c)),
            pl.BlockSpec((tokens, slots), lambda c: (0, 0)),
        ],
        out_specs=[out, out],
        out_shape=[jax.ShapeDtypeStruct((tokens, width), BF16)] * 2,
        name="combine",
    )(*parts, back, mix)


def ring(axis):
    peers = lax.axis_size(axis)
    return (
        [(i, (i + 1) % peers) for i in range(peers)],
        [(i, (i - 1) % peers) for i in range(peers)],
    )


def neighbours_shards(shard, axis):
    right, left = ring(axis)
    from_left = [lax.ppermute(w, axis, right) for w in shard]
    from_right = [lax.ppermute(w, axis, left) for w in shard]
    return from_left, from_right


def far_shard(from_left, from_right, axis):
    right, left = ring(axis)
    half = from_left[1].shape[0] // 2
    return (
        lax.ppermute(from_left[0], axis, right),
        lax.ppermute(from_left[1][:half], axis, right),
        lax.ppermute(from_right[1][half:], axis, left),
        lax.ppermute(from_right[2], axis, left),
    )


def gated(gate_val, up_val):
    return (jax.nn.silu(gate_val) * up_val).astype(BF16)


def shards(
    queries,
    keys,
    values,
    decay_gate_logits,
    correction_logits,
    head_decay_speed,
    position_log_decay,
    head_output_gain,
    mixer_output_weight,
    expert_input_tokens,
    expert_norm_gain,
    routes,
    chosen_expert_weight,
    routed_gate_weight,
    routed_up_weight,
    routed_down_weight,
    common_gate_weight,
    common_up_weight,
    common_down_weight,
):
    experts = lax.axis_size(EP)
    tokens, width = expert_input_tokens.shape
    own = (routed_gate_weight[0], routed_up_weight[0], routed_down_weight[0])
    from_left, from_right = neighbours_shards(own, "tp")

    xn, outgoing, mix = dispatch(
        expert_input_tokens, expert_norm_gain, routes, chosen_expert_weight, experts
    )
    arrived = lax.all_to_all(
        outgoing.reshape(experts, SLOT, width), EP, split_axis=0, concat_axis=0, tiled=True
    ).reshape(experts * SLOT, width)
    group = lax.all_gather(xn, "tp", axis=0, tiled=True)

    qt, ol, trans, inject = local_mixer(
        queries,
        keys,
        values,
        decay_gate_logits,
        correction_logits,
        head_decay_speed,
        position_log_decay,
    )
    state = entry_state(trans, inject)
    state, from_left, from_right = lax.optimization_barrier((state, from_left, from_right))
    far = far_shard(from_left, from_right, "tp")
    me = lax.axis_index("tp").astype(jnp.int32).reshape(1)
    parts = parts_for_peers(
        me,
        lax.axis_size("tp"),
        qt,
        ol,
        state,
        head_output_gain,
        mixer_output_weight,
        group,
        common_gate_weight,
        common_up_weight,
        common_down_weight,
    )
    near = near_experts(arrived, (own, from_left, from_right))
    slot_sums = far_expert(arrived, near, *far)
    parts, slot_sums = lax.optimization_barrier((parts, slot_sums))
    back = lax.all_to_all(
        slot_sums.reshape(experts, SLOT, width), EP, split_axis=0, concat_axis=0, tiled=True
    ).reshape(experts * SLOT, width)
    peers = lax.axis_size("tp")
    got = [parts[0]] + [
        lax.ppermute(parts[r], "tp", [(i, (i + r) % peers) for i in range(peers)])
        for r in range(1, peers)
    ]
    return tuple(combine(got, back, mix))


def solution(mesh):
    finer = Mesh(mesh.devices.reshape(8, 4, 2, mesh.shape["tp"]), ("ep_0", "ep_1", "ep_2", "tp"))
    placed = (
        P(EP, "tp"),
        P(EP, "tp"),
        P(EP, "tp"),
        P(EP, "tp"),
        P(EP, "tp"),
        P("tp"),
        P(EP, "tp"),
        P(),
        P("tp", None),
        P(EP_TP, None),
        P(),
        P(EP_TP, None),
        P(EP_TP, None),
        P(EP, None, "tp"),
        P(EP, None, "tp"),
        P(EP, "tp", None),
        P(None, "tp"),
        P(None, "tp"),
        P("tp", None),
    )
    return jax.shard_map(
        shards,
        mesh=finer,
        in_specs=placed,
        out_specs=(P(EP_TP, None), P(EP_TP, None)),
        check_vma=False,
    )
```

```python
import jax
import jax.numpy as jnp
from jax import lax
from jax.experimental import pallas as pl
from jax.experimental.pallas import tpu as pltpu
from jax.sharding import Mesh
from jax.sharding import PartitionSpec as P

EP = ("ep_0", "ep_1", "ep_2")
EP_TP = ("ep_0", "ep_1", "ep_2", "tp")


EPS = 1e-06
F32 = jnp.float32
BF16 = jnp.bfloat16
SLOT = 8
MESH = pl.DeviceIdType.MESH


def halves(x):
    hi = x.astype(BF16)
    return hi, (x - hi.astype(F32)).astype(BF16)


def thirds(x):
    hi = x.astype(BF16)
    rest = x - hi.astype(F32)
    mid = rest.astype(BF16)
    return hi, mid, (rest - mid.astype(F32)).astype(BF16)


def mm(a, b):
    return jnp.dot(a, b, preferred_element_type=F32)


def dot3(a, b):
    ah, al = halves(a)
    bh, bl = halves(b)
    return mm(jnp.concatenate([ah, ah, al], 1), jnp.concatenate([bh, bl, bh], 0))


def dot2(a, b):
    ah, al = halves(a)
    return mm(jnp.concatenate([ah, al], 1), jnp.concatenate([b, b], 0))


def unit_lower_inverse(low, row, col):
    eye = (row == col).astype(F32)
    base = jnp.where((row >> 3) == (col >> 3), low, 0.0)
    squared = dot3(base, base)
    fourth = dot3(squared, squared)
    inv = eye - base
    inv = inv + dot3(inv, squared)
    inv = inv + dot3(inv, fourth)
    for bit in (3, 4, 5):
        across = jnp.where(
            ((row >> (bit + 1)) == (col >> (bit + 1))) & ((row >> bit) != (col >> bit)), low, 0.0
        )
        inv = inv - dot3(inv, dot3(across, inv))
    return inv


def local_mixer_kernel(
    q_ref, k_ref, v_ref, gate_ref, corr_ref, speed_ref, plog_ref, qt_ref, ol_ref, tr_ref, in_ref
):
    head = pl.program_id(0)
    heads, rows = gate_ref.shape
    pair = 128
    here = lax.broadcasted_iota(jnp.int32, (heads, rows), 0) == head

    log_gate = (
        -speed_ref[...]
        * (jnp.maximum(gate_ref[...], 0.0) + jnp.log1p(jnp.exp(-jnp.abs(gate_ref[...]))))
        + plog_ref[...]
    )
    beta_all = 1.0 / (1.0 + jnp.exp(-corr_ref[...].astype(F32)))
    g_row = jnp.sum(jnp.where(here, log_gate, 0.0), axis=0, keepdims=True)
    beta_row_all = jnp.sum(jnp.where(here, beta_all, 0.0), axis=0, keepdims=True)

    row = lax.broadcasted_iota(jnp.int32, (pair, pair), 0)
    col = lax.broadcasted_iota(jnp.int32, (pair, pair), 1)
    same = (row >> 6) == (col >> 6)
    causal = same & (row >= col)
    strict = same & (row > col)
    first = col < 64
    ones = (same & (row <= col)).astype(BF16)
    ones = jnp.concatenate([ones, ones, ones], 0)

    packs = []
    for p in range(rows // pair):
        at = pl.ds(p * pair, pair)
        qb, kb, vb = q_ref[at, :], k_ref[at, :], v_ref[at, :]
        qf, kf = qb.astype(F32), kb.astype(F32)
        rq = lax.rsqrt(jnp.sum(qf * qf, axis=1, keepdims=True) + EPS) * (pair**-0.5)
        rk = lax.rsqrt(jnp.sum(kf * kf, axis=1, keepdims=True) + EPS)
        g_mat = jnp.broadcast_to(g_row[:, p * pair : (p + 1) * pair], (pair, pair))
        c_row = mm(jnp.concatenate(thirds(g_mat), 1), ones)
        c_mat = c_row.T
        last0, last1 = c_mat[63:64, :], c_mat[127:128, :]
        rk_row = jnp.broadcast_to(rk, (pair, pair)).T
        beta_row = jnp.broadcast_to(beta_row_all[:, p * pair : (p + 1) * pair], (pair, pair))
        beta = beta_row.T
        gram = lax.dot_general(
            jnp.concatenate([kb, qb], 0), kb, (((1,), (1,)), ((), ())), preferred_element_type=F32
        )
        decay = jnp.exp(jnp.where(causal, c_mat - c_row, -jnp.inf)) * rk_row
        low = jnp.where(strict, gram[:pair] * decay * (beta * rk), 0.0)
        scores = gram[pair:] * decay * rq
        inv = unit_lower_inverse(low, row, col)
        scale = beta_row * inv
        uw = jnp.concatenate(
            [dot2(scale, vb), dot2(scale * (jnp.exp(c_row) * rk_row), kb)], 1
        )
        suw = dot3(scores, uw)
        pq = qf * (rq * jnp.exp(c_mat)) - suw[:, pair:]
        tail = jnp.exp(jnp.where(first, last0, last1) - c_row)
        kt = kf.T * (tail * rk_row)
        kk = jnp.concatenate([jnp.where(first, kt, 0.0), jnp.where(first, 0.0, kt)], 0)
        mw = dot3(kk, uw)
        packs.append((suw[:, :pair], pq, mw, jnp.exp(last0), jnp.exp(last1)))

    ab = jnp.concatenate([(row == col).astype(F32), jnp.zeros((pair, pair), F32)], 1)
    for p, (su, pq, mw, keep0, keep1) in enumerate(packs):
        for b, keep in enumerate((keep0, keep1)):
            blk = slice(b * 64, (b + 1) * 64)
            at = pl.ds(p * pair + b * 64, 64)
            part = mw[b * pair : (b + 1) * pair]
            got = dot3(jnp.concatenate([pq[blk], part[:, pair:]], 0), ab)
            qt_ref[0, at, :] = got[:64, :pair]
            ol_ref[0, at, :] = got[:64, pair:] + su[blk]
            keep2 = jnp.concatenate([keep, keep], 1)
            ab = (
                keep2 * ab
                - got[64:]
                + jnp.concatenate([jnp.zeros((pair, pair), F32), part[:, :pair]], 1)
            )
    tr_ref[0] = ab[:, :pair]
    in_ref[0] = ab[:, pair:]


def local_mixer(queries, keys, values, gate, corr, speed, plog):
    rows, width = queries.shape
    heads = gate.shape[0]
    d = width // heads
    by_head = pl.BlockSpec((rows, d), lambda h: (0, h))
    whole = pl.BlockSpec((heads, rows), lambda h: (0, 0))
    return pl.pallas_call(
        local_mixer_kernel,
        grid=(heads,),
        in_specs=[
            by_head,
            by_head,
            by_head,
            whole,
            whole,
            pl.BlockSpec((heads, 1), lambda h: (0, 0)),
            whole,
        ],
        out_specs=[
            pl.BlockSpec((1, rows, d), lambda h: (h, 0, 0)),
            pl.BlockSpec((1, rows, d), lambda h: (h, 0, 0)),
            pl.BlockSpec((1, d, d), lambda h: (h, 0, 0)),
            pl.BlockSpec((1, d, d), lambda h: (h, 0, 0)),
        ],
        out_shape=[
            jax.ShapeDtypeStruct((heads, rows, d), F32),
            jax.ShapeDtypeStruct((heads, rows, d), F32),
            jax.ShapeDtypeStruct((heads, d, d), F32),
            jax.ShapeDtypeStruct((heads, d, d), F32),
        ],
        cost_estimate=pl.CostEstimate(flops=30_000_000_000, bytes_accessed=4_000_000, transcendentals=0),
        name="local_mixer",
    )(queries, keys, values, gate, corr, speed.reshape(heads, 1), plog)


def entry_state_kernel(
    t_ref, i_ref, xn_ref, s_ref, group_ref, send_x, recv_x, keep_x, own, peer, ypack, zpack,
    send_c, recv_c, send_y, recv_y, send_yc, recv_yc,
    send_r, recv_r, send_l, recv_l, send_rc, recv_rc, send_lc, recv_lc,
):
    heads, d, _ = t_ref.shape
    half = d // 2
    nz, ny = zpack.shape[0], ypack.shape[0]
    z, y, c = lax.axis_index("ep_0"), lax.axis_index("ep_1"), lax.axis_index("ep_2")
    other = {"ep_2": 1 - c}
    right, left = {"ep_0": lax.rem(z + 1, nz)}, {"ep_0": lax.rem(z + nz - 1, nz)}
    across = [{"ep_1": lax.rem(y + k, ny)} for k in range(1, ny)]
    members, me = group_ref.shape[0], lax.axis_index("tp")
    fellows = [{"tp": lax.rem(me + k, members)} for k in range(1, members)]

    barrier = pltpu.get_barrier_semaphore()
    for who in (other, right, left, *across, *fellows):
        pl.semaphore_signal(barrier, inc=1, device_id=who, device_id_type=MESH)
    pl.semaphore_wait(barrier, 3 + len(across) + len(fellows))

    def send(src, dst, send_sem, recv_sem, who):
        return pltpu.make_async_remote_copy(
            src_ref=src, dst_ref=dst, send_sem=send_sem, recv_sem=recv_sem,
            device_id=who, device_id_type=MESH,
        )

    def store(ref, h, both):
        both = both.astype(BF16)
        ref[0, h] = both[:half]
        ref[1, h] = both[half:]

    def load(ref, h):
        return jnp.concatenate([ref[0, h], ref[1, h]], 0)

    def after(pack, so_far):
        hi, lo = halves(so_far)
        t = pack[:, :d]
        return mm(jnp.concatenate([t, t], 1), jnp.concatenate([hi, lo], 0))

    def added(pack):
        return pack[:, d:].astype(F32)

    tokens = [
        send(xn_ref, group_ref.at[me], send_x.at[k], recv_x.at[k], who)
        for k, who in enumerate(fellows)
    ]
    kept = pltpu.make_async_copy(xn_ref, group_ref.at[me], keep_x)

    nothing = jnp.zeros((d, d), F32)
    for h in range(heads):
        store(own, h, jnp.concatenate([t_ref[h], i_ref[h]], 1))
    swap = send(own, peer, send_c, recv_c, other)
    swap.start()
    for copy in tokens:
        copy.start()
    kept.start()
    swap.wait()
    for h in range(heads):
        mine, theirs = load(own, h), load(peer, h)
        early = jnp.where(c == 0, mine.astype(F32), theirs.astype(F32)).astype(BF16)
        late = jnp.where(c == 0, theirs.astype(F32), mine.astype(F32)).astype(BF16)
        both = mm(late[:, :d], early) + jnp.concatenate([nothing, added(late)], 1)
        store(ypack.at[y], h, both)

    out = [
        send(ypack.at[y, c], ypack.at[y, c], send_y.at[k - 1], recv_y.at[k - 1], across[k - 1])
        for k in range(1, ny)
    ]
    for copy in out:
        copy.start()
    over = []
    for k in range(1, ny):
        slot = ypack.at[lax.rem(y + ny - k, ny), c]
        out[k - 1].wait_recv()
        over.append(send(slot, slot, send_yc.at[k - 1], recv_yc.at[k - 1], other))
        over[-1].start()
    for copy in out:
        copy.wait_send()
    for copy in over:
        copy.wait()
    for h in range(heads):
        both = load(ypack.at[0], h).astype(F32)
        for k in range(1, ny):
            pack = load(ypack.at[k], h)
            both = after(pack, both) + jnp.concatenate([nothing, added(pack)], 1)
        store(zpack.at[z], h, both)

    def going(r, h, sign, who, send_sem, recv_sem):
        slot = zpack.at[lax.rem(z + nz - sign * (r - 1), nz), c, h]
        return send(slot, slot, send_sem.at[r - 1, h], recv_sem.at[r - 1, h], who)

    def shared_with_other(r, h, sign, send_sem, recv_sem):
        slot = zpack.at[lax.rem(z + nz - sign * r, nz), c, h]
        return send(slot, slot, send_sem.at[r - 1, h], recv_sem.at[r - 1, h], other)

    rings = (
        (nz // 2, 1, right, send_r, recv_r, send_rc, recv_rc),
        ((nz - 1) // 2, -1, left, send_l, recv_l, send_lc, recv_lc),
    )
    pending = []
    for rounds, sign, who, ss, rs, _, _ in rings:
        for h in range(heads):
            if rounds > 0:
                going(1, h, sign, who, ss, rs).start()
    for r in range(1, nz // 2 + 1):
        for h in range(heads):
            for rounds, sign, who, ss, rs, sc, rc in rings:
                if r > rounds:
                    continue
                copy = going(r, h, sign, who, ss, rs)
                copy.wait_recv()
                pending.append((copy, False))
                if r < rounds:
                    going(r + 1, h, sign, who, ss, rs).start()
                hand = shared_with_other(r, h, sign, sc, rc)
                hand.start()
                pending.append((hand, True))
    for copy, both_ways in pending:
        copy.wait_send()
        if both_ways:
            copy.wait_recv()

    for h in range(heads):
        s_ref[h] = nothing
    for k in range(nz - 1):
        for h in range(heads):
            pack = load(zpack.at[k], h)
            s_ref[h] = jnp.where(k < z, after(pack, s_ref[h]) + added(pack), s_ref[h])
    for k in range(ny - 1):
        for h in range(heads):
            pack = load(ypack.at[k], h)
            s_ref[h] = jnp.where(k < y, after(pack, s_ref[h]) + added(pack), s_ref[h])
    for h in range(heads):
        pack = load(peer, h)
        s_ref[h] = jnp.where(c == 1, after(pack, s_ref[h]) + added(pack), s_ref[h])
    kept.wait()
    for copy in tokens:
        copy.wait()


def entry_state(trans, inject, xn):
    heads, d, _ = trans.shape
    nz, ny = lax.axis_size("ep_0"), lax.axis_size("ep_1")
    half = (2, heads, d // 2, 2 * d)
    dma = pltpu.SemaphoreType.DMA
    rounds = max(nz // 2, 1)
    members = lax.axis_size("tp")
    vmem = pl.BlockSpec(memory_space=pltpu.VMEM)
    return pl.pallas_call(
        entry_state_kernel,
        in_specs=[vmem, vmem, pl.BlockSpec(memory_space=pl.ANY)],
        out_specs=[vmem, pl.BlockSpec(memory_space=pl.ANY)],
        out_shape=[
            jax.ShapeDtypeStruct((heads, d, d), F32),
            jax.ShapeDtypeStruct((members, *xn.shape), BF16),
        ],
        scratch_shapes=[
            dma((max(members - 1, 1),)), dma((max(members - 1, 1),)), dma,
            pltpu.VMEM(half, BF16),
            pltpu.VMEM(half, BF16),
            pltpu.VMEM((ny, *half), BF16),
            pltpu.VMEM((nz, *half), BF16),
            dma, dma,
            dma((max(ny - 1, 1),)), dma((max(ny - 1, 1),)), dma((max(ny - 1, 1),)), dma((max(ny - 1, 1),)),
            *[dma((rounds, heads)) for _ in range(8)],
        ],
        compiler_params=pltpu.CompilerParams(collective_id=0, has_side_effects=True),
        cost_estimate=pl.CostEstimate(flops=30_000_000_000, bytes_accessed=4_000_000, transcendentals=0),
        name="entry_state",
    )(trans, inject, xn)


def parts_kernel(
    me_ref, qt_ref, ol_ref, state_ref, gain_ref, w_ref, x_ref, gate_ref, up_ref, down_ref, *out_refs
):
    heads, tile, _ = qt_ref.shape
    normed = []
    for h in range(heads):
        out = dot3(qt_ref[h], state_ref[h]) + ol_ref[h]
        out = out * lax.rsqrt(jnp.mean(out * out, axis=1, keepdims=True) + EPS) * gain_ref[...]
        normed.append(out.astype(BF16))
    mixer = mm(jnp.concatenate(normed, 1), w_ref[...]).astype(BF16)
    x = x_ref[0]
    hidden = gated(mm(x, gate_ref[...]), mm(x, up_ref[...]))
    shared = mm(hidden, down_ref[...]).astype(BF16)
    for r, out_ref in enumerate(out_refs):

        @pl.when(pl.program_id(0) == r)
        def _():
            out_ref[:tile] = mixer
            out_ref[tile:] = shared


def parts_for_peers(me, peers, qt, ol, state, gain, w, group, gate, up, down):
    heads, rows, d = qt.shape
    width = w.shape[1]
    tile = rows // peers

    def whole(x):
        return pl.BlockSpec(x.shape, lambda r, me: (0,) * x.ndim)

    def turn(r, me):
        return lax.rem(me[0] + r, peers)

    gain = gain.reshape(1, d)
    return pl.pallas_call(
        parts_kernel,
        grid_spec=pltpu.PrefetchScalarGridSpec(
            num_scalar_prefetch=1,
            grid=(peers,),
            in_specs=[
                pl.BlockSpec((heads, tile, d), lambda r, me: (0, turn(r, me), 0)),
                pl.BlockSpec((heads, tile, d), lambda r, me: (0, turn(r, me), 0)),
                whole(state),
                whole(gain),
                whole(w),
                pl.BlockSpec((1, tile, group.shape[2]), lambda r, me: (turn(r, me), 0, 0)),
                whole(gate),
                whole(up),
                whole(down),
            ],
            out_specs=[pl.BlockSpec((2 * tile, width), lambda r, me: (0, 0))] * peers,
        ),
        out_shape=[jax.ShapeDtypeStruct((2 * tile, width), BF16)] * peers,
        cost_estimate=pl.CostEstimate(flops=6_000_000_000, bytes_accessed=12_000_000, transcendentals=0),
        name="parts_for_peers",
    )(me, qt, ol, state, gain, w, group, gate, up, down)


def near_experts_kernel(x_ref, *refs):
    *weights, out_ref = refs
    x = x_ref[...]
    total = None
    for m in range(0, len(weights), 3):
        gate, up, down = weights[m : m + 3]
        part = mm(gated(mm(x, gate[...]), mm(x, up[...])), down[...])
        total = part if total is None else total + part
    out_ref[...] = total


def near_experts(x, shards_):
    rows, width = x.shape
    tile = 128
    weights = [w for shard in shards_ for w in shard]
    return pl.pallas_call(
        near_experts_kernel,
        grid=(rows // tile,),
        in_specs=[pl.BlockSpec((tile, width), lambda r: (r, 0))]
        + [pl.BlockSpec(w.shape, lambda r: (0, 0)) for w in weights],
        out_specs=pl.BlockSpec((tile, width), lambda r: (r, 0)),
        out_shape=jax.ShapeDtypeStruct((rows, width), F32),
        cost_estimate=pl.CostEstimate(flops=5_000_000_000, bytes_accessed=16_000_000, transcendentals=0),
        name="near_experts",
    )(x, *weights)


def far_expert_kernel(x_ref, near_ref, gate_ref, up0_ref, up1_ref, down_ref, out_ref):
    x = x_ref[...]
    half = up0_ref.shape[0]
    up = mm(x[:, :half], up0_ref[...]) + mm(x[:, half:], up1_ref[...])
    total = near_ref[...] + mm(gated(mm(x, gate_ref[...]), up), down_ref[...])
    out_ref[...] = total.astype(BF16)


def far_expert(x, near, gate, up0, up1, down):
    rows, width = x.shape
    tile = 128
    weights = (gate, up0, up1, down)
    by_rows = pl.BlockSpec((tile, width), lambda r: (r, 0))
    return pl.pallas_call(
        far_expert_kernel,
        grid=(rows // tile,),
        in_specs=[by_rows, by_rows] + [pl.BlockSpec(w.shape, lambda r: (0, 0)) for w in weights],
        out_specs=by_rows,
        out_shape=jax.ShapeDtypeStruct((rows, width), BF16),
        cost_estimate=pl.CostEstimate(flops=2_000_000_000, bytes_accessed=12_000_000, transcendentals=0),
        name="far_expert",
    )(x, near, *weights)


def dispatch_kernel(x_ref, gain_ref, routes_ref, weight_ref, xn_ref, out_ref, mix_ref):
    tokens = x_ref.shape[0]
    slots = out_ref.shape[0]
    x = x_ref[...].astype(F32)
    xn = (x * lax.rsqrt(jnp.mean(x * x, axis=1, keepdims=True) + EPS) * gain_ref[...]).astype(BF16)
    xn_ref[...] = xn
    expert = lax.broadcasted_iota(jnp.int32, (128, tokens), 0)
    first, second = expert == routes_ref[0:1, :], expert == routes_ref[1:2, :]
    chosen = (first | second).astype(BF16)
    token = lax.broadcasted_iota(jnp.int32, (tokens, tokens), 0)
    later = lax.broadcasted_iota(jnp.int32, (tokens, tokens), 1)
    place = mm(chosen, (token < later).astype(BF16)) + (expert * SLOT).astype(F32)
    s0 = jnp.sum(jnp.where(first, place, 0.0), axis=0, keepdims=True)
    s1 = jnp.sum(jnp.where(second, place, 0.0), axis=0, keepdims=True)
    step = 128
    for base in range(0, slots, step):
        slot = (lax.broadcasted_iota(jnp.int32, (step, tokens), 0) + base).astype(F32)
        is0, is1 = slot == s0, slot == s1
        out_ref[base : base + step, :] = mm((is0 | is1).astype(BF16), xn).astype(BF16)
        mix = jnp.where(is0, weight_ref[0:1, :], 0.0) + jnp.where(is1, weight_ref[1:2, :], 0.0)
        mix_ref[:, base : base + step] = mix.T


def dispatch(x, gain, routes, weight, experts):
    tokens, width = x.shape
    slots = experts * SLOT
    return pl.pallas_call(
        dispatch_kernel,
        out_shape=[
            jax.ShapeDtypeStruct((tokens, width), BF16),
            jax.ShapeDtypeStruct((slots, width), BF16),
            jax.ShapeDtypeStruct((tokens, slots), F32),
        ],
        name="dispatch",
    )(x, gain.reshape(1, width), routes, weight)


def mixer_sum_kernel(*refs):
    *part_refs, out_ref = refs
    total = part_refs[0][...].astype(F32)
    for part in part_refs[1:]:
        total = total + part[...].astype(F32)
    out_ref[...] = total.astype(BF16)


def mixer_sum(parts):
    rows, width = parts[0].shape
    half = pl.BlockSpec((rows // 2, width), lambda c: (0, 0))
    return pl.pallas_call(
        mixer_sum_kernel,
        grid=(1,),
        in_specs=[half] * len(parts),
        out_specs=half,
        out_shape=jax.ShapeDtypeStruct((rows // 2, width), BF16),
        cost_estimate=pl.CostEstimate(flops=1_000_000_000, bytes_accessed=3_000_000, transcendentals=0),
        name="mixer_sum",
    )(*parts)


def combine_kernel(*refs):
    *part_refs, back_ref, mix_ref, out_ref = refs
    total = dot2(mix_ref[...], back_ref[...])
    for part in part_refs:
        total = total + part[...].astype(F32)
    out_ref[...] = total.astype(BF16)


def combine(parts, back, mix):
    tokens, slots = mix.shape
    width = back.shape[1]
    tile = 512
    return pl.pallas_call(
        combine_kernel,
        grid=(width // tile,),
        in_specs=[pl.BlockSpec((tokens, tile), lambda c: (1, c))] * len(parts)
        + [
            pl.BlockSpec((slots, tile), lambda c: (0, c)),
            pl.BlockSpec((tokens, slots), lambda c: (0, 0)),
        ],
        out_specs=pl.BlockSpec((tokens, tile), lambda c: (0, c)),
        out_shape=jax.ShapeDtypeStruct((tokens, width), BF16),
        name="combine",
    )(*parts, back, mix)


def ring(axis):
    peers = lax.axis_size(axis)
    return (
        [(i, (i + 1) % peers) for i in range(peers)],
        [(i, (i - 1) % peers) for i in range(peers)],
    )


def neighbours_shards(shard, axis):
    right, left = ring(axis)
    from_left = [lax.ppermute(w, axis, right) for w in shard]
    from_right = [lax.ppermute(w, axis, left) for w in shard]
    return from_left, from_right


def far_shard(from_left, from_right, axis):
    right, left = ring(axis)
    half = from_left[1].shape[0] // 2
    return (
        lax.ppermute(from_left[0], axis, right),
        lax.ppermute(from_left[1][:half], axis, right),
        lax.ppermute(from_right[1][half:], axis, left),
        lax.ppermute(from_right[2], axis, left),
    )


def gated(gate_val, up_val):
    return (jax.nn.silu(gate_val) * up_val).astype(BF16)


def shards(
    queries,
    keys,
    values,
    decay_gate_logits,
    correction_logits,
    head_decay_speed,
    position_log_decay,
    head_output_gain,
    mixer_output_weight,
    expert_input_tokens,
    expert_norm_gain,
    routes,
    chosen_expert_weight,
    routed_gate_weight,
    routed_up_weight,
    routed_down_weight,
    common_gate_weight,
    common_up_weight,
    common_down_weight,
):
    experts = lax.axis_size(EP)
    tokens, width = expert_input_tokens.shape
    own = (routed_gate_weight[0], routed_up_weight[0], routed_down_weight[0])
    from_left, from_right = neighbours_shards(own, "tp")

    xn, outgoing, mix = dispatch(
        expert_input_tokens, expert_norm_gain, routes.T, chosen_expert_weight.T, experts
    )
    arrived = lax.all_to_all(
        outgoing.reshape(experts, SLOT, width), EP, split_axis=0, concat_axis=0, tiled=True
    ).reshape(experts * SLOT, width)

    qt, ol, trans, inject = local_mixer(
        queries,
        keys,
        values,
        decay_gate_logits.T,
        correction_logits.T,
        head_decay_speed,
        position_log_decay.T,
    )
    state, group = entry_state(trans, inject, xn)
    state, from_left, from_right = lax.optimization_barrier((state, from_left, from_right))
    far = far_shard(from_left, from_right, "tp")
    me = lax.axis_index("tp").astype(jnp.int32).reshape(1)
    parts = parts_for_peers(
        me,
        lax.axis_size("tp"),
        qt,
        ol,
        state,
        head_output_gain,
        mixer_output_weight,
        group,
        common_gate_weight,
        common_up_weight,
        common_down_weight,
    )
    near = near_experts(arrived, (own, from_left, from_right))
    parts, far, near = lax.optimization_barrier((parts, far, near))
    peers = lax.axis_size("tp")
    got = [parts[0]] + [
        lax.ppermute(parts[r], "tp", [(i, (i + r) % peers) for i in range(peers)])
        for r in range(1, peers)
    ]
    slot_sums = far_expert(arrived, near, *far)
    back = lax.all_to_all(
        slot_sums.reshape(experts, SLOT, width), EP, split_axis=0, concat_axis=0, tiled=True
    ).reshape(experts * SLOT, width)
    return (mixer_sum(got), combine(got, back, mix))


def solution(mesh):
    finer = Mesh(mesh.devices.reshape(8, 4, 2, mesh.shape["tp"]), ("ep_0", "ep_1", "ep_2", "tp"))
    placed = (
        P(EP, "tp"),
        P(EP, "tp"),
        P(EP, "tp"),
        P(EP, "tp"),
        P(EP, "tp"),
        P("tp"),
        P(EP, "tp"),
        P(),
        P("tp", None),
        P(EP_TP, None),
        P(),
        P(EP_TP, None),
        P(EP_TP, None),
        P(EP, None, "tp"),
        P(EP, None, "tp"),
        P(EP, "tp", None),
        P(None, "tp"),
        P(None, "tp"),
        P("tp", None),
    )
    return jax.shard_map(
        shards,
        mesh=finer,
        in_specs=placed,
        out_specs=(P(EP_TP, None), P(EP_TP, None)),
        check_vma=False,
    )
```

```python
import functools

import jax
import jax.numpy as jnp
from jax import lax
from jax.experimental import pallas as pl
from jax.experimental.pallas import tpu as pltpu
from jax.sharding import Mesh
from jax.sharding import PartitionSpec as P


EP = ("ep_0", "ep_1", "ep_2")
EP_TP = ("ep_0", "ep_1", "ep_2", "tp")


EPS = 1e-06
F32 = jnp.float32
BF16 = jnp.bfloat16
LANES = 128
MESH = pl.DeviceIdType.MESH


def halves(x):
    hi = x.astype(BF16)
    return hi, (x - hi.astype(F32)).astype(BF16)


def thirds(x):
    hi = x.astype(BF16)
    rest = x - hi.astype(F32)
    mid = rest.astype(BF16)
    return hi, mid, (rest - mid.astype(F32)).astype(BF16)


def mm(a, b):
    return jnp.dot(a, b, preferred_element_type=F32)


def dot3(a, b):
    ah, al = halves(a)
    bh, bl = halves(b)
    return mm(jnp.concatenate([ah, ah, al], 1), jnp.concatenate([bh, bl, bh], 0))


def dot2(a, b):
    ah, al = halves(a)
    return mm(jnp.concatenate([ah, al], 1), jnp.concatenate([b, b], 0))


def unit_lower_inverse(low, row, col):
    eye = (row == col).astype(F32)
    base = jnp.where((row >> 3) == (col >> 3), low, 0.0)
    squared = dot3(base, base)
    fourth = dot3(squared, squared)
    inv = eye - base
    inv = inv + dot3(inv, squared)
    inv = inv + dot3(inv, fourth)
    for bit in (3, 4, 5):
        across = jnp.where(
            ((row >> (bit + 1)) == (col >> (bit + 1))) & ((row >> bit) != (col >> bit)), low, 0.0
        )
        inv = inv - dot3(inv, dot3(across, inv))
    return inv


def local_mixer_kernel(
    q_ref, k_ref, v_ref, gate_ref, corr_ref, speed_ref, plog_ref, qt_ref, ol_ref, tr_ref, in_ref
):
    head = pl.program_id(0)
    heads, rows = gate_ref.shape
    pair = 128
    here = lax.broadcasted_iota(jnp.int32, (heads, rows), 0) == head

    log_gate = (
        -speed_ref[...]
        * (jnp.maximum(gate_ref[...], 0.0) + jnp.log1p(jnp.exp(-jnp.abs(gate_ref[...]))))
        + plog_ref[...]
    )
    beta_all = 1.0 / (1.0 + jnp.exp(-corr_ref[...].astype(F32)))
    g_row = jnp.sum(jnp.where(here, log_gate, 0.0), axis=0, keepdims=True)
    beta_row_all = jnp.sum(jnp.where(here, beta_all, 0.0), axis=0, keepdims=True)

    row = lax.broadcasted_iota(jnp.int32, (pair, pair), 0)
    col = lax.broadcasted_iota(jnp.int32, (pair, pair), 1)
    same = (row >> 6) == (col >> 6)
    causal = same & (row >= col)
    strict = same & (row > col)
    first = col < 64
    ones = (same & (row <= col)).astype(BF16)
    ones = jnp.concatenate([ones, ones, ones], 0)

    packs = []
    for p in range(rows // pair):
        at = pl.ds(p * pair, pair)
        qb, kb, vb = q_ref[at, :], k_ref[at, :], v_ref[at, :]
        qf, kf = qb.astype(F32), kb.astype(F32)
        rq = lax.rsqrt(jnp.sum(qf * qf, axis=1, keepdims=True) + EPS) * (pair**-0.5)
        rk = lax.rsqrt(jnp.sum(kf * kf, axis=1, keepdims=True) + EPS)
        g_mat = jnp.broadcast_to(g_row[:, p * pair : (p + 1) * pair], (pair, pair))
        c_row = mm(jnp.concatenate(thirds(g_mat), 1), ones)
        c_mat = c_row.T
        last0, last1 = c_mat[63:64, :], c_mat[127:128, :]
        rk_row = jnp.broadcast_to(rk, (pair, pair)).T
        beta_row = jnp.broadcast_to(beta_row_all[:, p * pair : (p + 1) * pair], (pair, pair))
        beta = beta_row.T
        gram = lax.dot_general(
            jnp.concatenate([kb, qb], 0), kb, (((1,), (1,)), ((), ())), preferred_element_type=F32
        )
        decay = jnp.exp(jnp.where(causal, c_mat - c_row, -jnp.inf)) * rk_row
        low = jnp.where(strict, gram[:pair] * decay * (beta * rk), 0.0)
        scores = gram[pair:] * decay * rq
        inv = unit_lower_inverse(low, row, col)
        scale = beta_row * inv
        uw = jnp.concatenate(
            [dot2(scale, vb), dot2(scale * (jnp.exp(c_row) * rk_row), kb)], 1
        )
        suw = dot3(scores, uw)
        pq = qf * (rq * jnp.exp(c_mat)) - suw[:, pair:]
        tail = jnp.exp(jnp.where(first, last0, last1) - c_row)
        kt = kf.T * (tail * rk_row)
        kk = jnp.concatenate([jnp.where(first, kt, 0.0), jnp.where(first, 0.0, kt)], 0)
        mw = dot3(kk, uw)
        packs.append((suw[:, :pair], pq, mw, jnp.exp(last0), jnp.exp(last1)))

    ab = jnp.concatenate([(row == col).astype(F32), jnp.zeros((pair, pair), F32)], 1)
    for p, (su, pq, mw, keep0, keep1) in enumerate(packs):
        for b, keep in enumerate((keep0, keep1)):
            blk = slice(b * 64, (b + 1) * 64)
            at = pl.ds(p * pair + b * 64, 64)
            part = mw[b * pair : (b + 1) * pair]
            got = dot3(jnp.concatenate([pq[blk], part[:, pair:]], 0), ab)
            qt_ref[0, at, :] = got[:64, :pair]
            ol_ref[0, at, :] = got[:64, pair:] + su[blk]
            keep2 = jnp.concatenate([keep, keep], 1)
            ab = (
                keep2 * ab
                - got[64:]
                + jnp.concatenate([jnp.zeros((pair, pair), F32), part[:, :pair]], 1)
            )
    tr_ref[0] = ab[:, :pair]
    in_ref[0] = ab[:, pair:]


def local_mixer(queries, keys, values, gate, corr, speed, plog):
    rows, width = queries.shape
    heads = gate.shape[0]
    d = width // heads
    by_head = pl.BlockSpec((rows, d), lambda h: (0, h))
    whole = pl.BlockSpec((heads, rows), lambda h: (0, 0))
    return pl.pallas_call(
        local_mixer_kernel,
        grid=(heads,),
        in_specs=[
            by_head,
            by_head,
            by_head,
            whole,
            whole,
            pl.BlockSpec((heads, 1), lambda h: (0, 0)),
            whole,
        ],
        out_specs=[
            pl.BlockSpec((1, rows, d), lambda h: (h, 0, 0)),
            pl.BlockSpec((1, rows, d), lambda h: (h, 0, 0)),
            pl.BlockSpec((1, d, d), lambda h: (h, 0, 0)),
            pl.BlockSpec((1, d, d), lambda h: (h, 0, 0)),
        ],
        out_shape=[
            jax.ShapeDtypeStruct((heads, rows, d), F32),
            jax.ShapeDtypeStruct((heads, rows, d), F32),
            jax.ShapeDtypeStruct((heads, d, d), F32),
            jax.ShapeDtypeStruct((heads, d, d), F32),
        ],
        cost_estimate=pl.CostEstimate(flops=30_000_000_000, bytes_accessed=4_000_000, transcendentals=0),
        name="local_mixer",
    )(queries, keys, values, gate, corr, speed.reshape(heads, 1), plog)


def entry_state_kernel(
    t_ref, i_ref, xn_ref, s_ref, group_ref, send_x, recv_x, keep_x, own, peer, ypack, zpack,
    send_c, recv_c, send_y, recv_y, send_yc, recv_yc,
    send_r, recv_r, send_l, recv_l, send_rc, recv_rc, send_lc, recv_lc,
):
    heads, d, _ = t_ref.shape
    half = d // 2
    nz, ny = zpack.shape[0], ypack.shape[0]
    z, y, c = lax.axis_index("ep_0"), lax.axis_index("ep_1"), lax.axis_index("ep_2")
    other = {"ep_2": 1 - c}
    right, left = {"ep_0": lax.rem(z + 1, nz)}, {"ep_0": lax.rem(z + nz - 1, nz)}
    across = [{"ep_1": lax.rem(y + k, ny)} for k in range(1, ny)]
    members, me = group_ref.shape[0], lax.axis_index("tp")
    fellows = [{"tp": lax.rem(me + k, members)} for k in range(1, members)]

    barrier = pltpu.get_barrier_semaphore()
    for who in (other, right, left, *across, *fellows):
        pl.semaphore_signal(barrier, inc=1, device_id=who, device_id_type=MESH)
    pl.semaphore_wait(barrier, 3 + len(across) + len(fellows))

    def send(src, dst, send_sem, recv_sem, who):
        return pltpu.make_async_remote_copy(
            src_ref=src, dst_ref=dst, send_sem=send_sem, recv_sem=recv_sem,
            device_id=who, device_id_type=MESH,
        )

    def store(ref, h, both):
        both = both.astype(BF16)
        ref[0, h] = both[:half]
        ref[1, h] = both[half:]

    def load(ref, h):
        return jnp.concatenate([ref[0, h], ref[1, h]], 0)

    def after(pack, so_far):
        hi, lo = halves(so_far)
        t = pack[:, :d]
        return mm(jnp.concatenate([t, t], 1), jnp.concatenate([hi, lo], 0))

    def added(pack):
        return pack[:, d:].astype(F32)

    tokens = [
        send(xn_ref, group_ref.at[me], send_x.at[k], recv_x.at[k], who)
        for k, who in enumerate(fellows)
    ]
    kept = pltpu.make_async_copy(xn_ref, group_ref.at[me], keep_x)

    nothing = jnp.zeros((d, d), F32)
    for h in range(heads):
        store(own, h, jnp.concatenate([t_ref[h], i_ref[h]], 1))
    swap = send(own, peer, send_c, recv_c, other)
    swap.start()
    for copy in tokens:
        copy.start()
    kept.start()
    swap.wait()
    for h in range(heads):
        mine, theirs = load(own, h), load(peer, h)
        early = jnp.where(c == 0, mine.astype(F32), theirs.astype(F32)).astype(BF16)
        late = jnp.where(c == 0, theirs.astype(F32), mine.astype(F32)).astype(BF16)
        both = mm(late[:, :d], early) + jnp.concatenate([nothing, added(late)], 1)
        store(ypack.at[y], h, both)

    out = [
        send(ypack.at[y, c], ypack.at[y, c], send_y.at[k - 1], recv_y.at[k - 1], across[k - 1])
        for k in range(1, ny)
    ]
    for copy in out:
        copy.start()
    over = []
    for k in range(1, ny):
        slot = ypack.at[lax.rem(y + ny - k, ny), c]
        out[k - 1].wait_recv()
        over.append(send(slot, slot, send_yc.at[k - 1], recv_yc.at[k - 1], other))
        over[-1].start()
    for copy in out:
        copy.wait_send()
    for copy in over:
        copy.wait()
    for h in range(heads):
        both = load(ypack.at[0], h).astype(F32)
        for k in range(1, ny):
            pack = load(ypack.at[k], h)
            both = after(pack, both) + jnp.concatenate([nothing, added(pack)], 1)
        store(zpack.at[z], h, both)

    def going(r, h, sign, who, send_sem, recv_sem):
        slot = zpack.at[lax.rem(z + nz - sign * (r - 1), nz), c, h]
        return send(slot, slot, send_sem.at[r - 1, h], recv_sem.at[r - 1, h], who)

    def shared_with_other(r, h, sign, send_sem, recv_sem):
        slot = zpack.at[lax.rem(z + nz - sign * r, nz), c, h]
        return send(slot, slot, send_sem.at[r - 1, h], recv_sem.at[r - 1, h], other)

    rings = (
        (nz // 2, 1, right, send_r, recv_r, send_rc, recv_rc),
        ((nz - 1) // 2, -1, left, send_l, recv_l, send_lc, recv_lc),
    )
    pending = []
    for rounds, sign, who, ss, rs, _, _ in rings:
        for h in range(heads):
            if rounds > 0:
                going(1, h, sign, who, ss, rs).start()
    for r in range(1, nz // 2 + 1):
        for h in range(heads):
            for rounds, sign, who, ss, rs, sc, rc in rings:
                if r > rounds:
                    continue
                copy = going(r, h, sign, who, ss, rs)
                copy.wait_recv()
                pending.append((copy, False))
                if r < rounds:
                    going(r + 1, h, sign, who, ss, rs).start()
                hand = shared_with_other(r, h, sign, sc, rc)
                hand.start()
                pending.append((hand, True))
    for copy, both_ways in pending:
        copy.wait_send()
        if both_ways:
            copy.wait_recv()

    for h in range(heads):
        s_ref[h] = nothing
    for k in range(nz - 1):
        for h in range(heads):
            pack = load(zpack.at[k], h)
            s_ref[h] = jnp.where(k < z, after(pack, s_ref[h]) + added(pack), s_ref[h])
    for k in range(ny - 1):
        for h in range(heads):
            pack = load(ypack.at[k], h)
            s_ref[h] = jnp.where(k < y, after(pack, s_ref[h]) + added(pack), s_ref[h])
    for h in range(heads):
        pack = load(peer, h)
        s_ref[h] = jnp.where(c == 1, after(pack, s_ref[h]) + added(pack), s_ref[h])
    kept.wait()
    for copy in tokens:
        copy.wait()


def entry_state(trans, inject, xn):
    heads, d, _ = trans.shape
    nz, ny = lax.axis_size("ep_0"), lax.axis_size("ep_1")
    half = (2, heads, d // 2, 2 * d)
    dma = pltpu.SemaphoreType.DMA
    rounds = max(nz // 2, 1)
    members = lax.axis_size("tp")
    vmem = pl.BlockSpec(memory_space=pltpu.VMEM)
    return pl.pallas_call(
        entry_state_kernel,
        in_specs=[vmem, vmem, pl.BlockSpec(memory_space=pl.ANY)],
        out_specs=[vmem, pl.BlockSpec(memory_space=pl.ANY)],
        out_shape=[
            jax.ShapeDtypeStruct((heads, d, d), F32),
            jax.ShapeDtypeStruct((members, *xn.shape), BF16),
        ],
        scratch_shapes=[
            dma((max(members - 1, 1),)), dma((max(members - 1, 1),)), dma,
            pltpu.VMEM(half, BF16),
            pltpu.VMEM(half, BF16),
            pltpu.VMEM((ny, *half), BF16),
            pltpu.VMEM((nz, *half), BF16),
            dma, dma,
            dma((max(ny - 1, 1),)), dma((max(ny - 1, 1),)), dma((max(ny - 1, 1),)), dma((max(ny - 1, 1),)),
            *[dma((rounds, heads)) for _ in range(8)],
        ],
        compiler_params=pltpu.CompilerParams(collective_id=0, has_side_effects=True),
        cost_estimate=pl.CostEstimate(flops=30_000_000_000, bytes_accessed=4_000_000, transcendentals=0),
        name="entry_state",
    )(trans, inject, xn)


def parts_kernel(
    me_ref, qt_ref, ol_ref, state_ref, gain_ref, w_ref, x_ref, gate_ref, up_ref, down_ref, *out_refs
):
    heads, tile, _ = qt_ref.shape
    normed = []
    for h in range(heads):
        out = dot3(qt_ref[h], state_ref[h]) + ol_ref[h]
        out = out * lax.rsqrt(jnp.mean(out * out, axis=1, keepdims=True) + EPS) * gain_ref[...]
        normed.append(out.astype(BF16))
    mixer = mm(jnp.concatenate(normed, 1), w_ref[...]).astype(BF16)
    x = x_ref[0]
    hidden = gated(mm(x, gate_ref[...]), mm(x, up_ref[...]))
    shared = mm(hidden, down_ref[...]).astype(BF16)
    for r, out_ref in enumerate(out_refs):

        @pl.when(pl.program_id(0) == r)
        def _():
            out_ref[:tile] = mixer
            out_ref[tile:] = shared


def parts_for_peers(me, peers, qt, ol, state, gain, w, group, gate, up, down):
    heads, rows, d = qt.shape
    width = w.shape[1]
    tile = rows // peers

    def whole(x):
        return pl.BlockSpec(x.shape, lambda r, me: (0,) * x.ndim)

    def turn(r, me):
        return lax.rem(me[0] + r, peers)

    gain = gain.reshape(1, d)
    return pl.pallas_call(
        parts_kernel,
        grid_spec=pltpu.PrefetchScalarGridSpec(
            num_scalar_prefetch=1,
            grid=(peers,),
            in_specs=[
                pl.BlockSpec((heads, tile, d), lambda r, me: (0, turn(r, me), 0)),
                pl.BlockSpec((heads, tile, d), lambda r, me: (0, turn(r, me), 0)),
                whole(state),
                whole(gain),
                whole(w),
                pl.BlockSpec((1, tile, group.shape[2]), lambda r, me: (turn(r, me), 0, 0)),
                whole(gate),
                whole(up),
                whole(down),
            ],
            out_specs=[pl.BlockSpec((2 * tile, width), lambda r, me: (0, 0))] * peers,
        ),
        out_shape=[jax.ShapeDtypeStruct((2 * tile, width), BF16)] * peers,
        cost_estimate=pl.CostEstimate(flops=6_000_000_000, bytes_accessed=12_000_000, transcendentals=0),
        name="parts_for_peers",
    )(me, qt, ol, state, gain, w, group, gate, up, down)


def near_experts_kernel(in_ref, *refs):
    shards_ = len(refs) // 3 - 2
    hbm, (x_ref, out_ref, wide, gates, ups, downs) = refs[: 3 * shards_], refs[3 * shards_ : -1]
    sems = refs[-1]
    rows, width = x_ref.shape
    cuts = width // LANES
    tile = 128
    copies = [
        [
            pltpu.make_async_copy(hbm[3 * m + k], held.at[m], sems.at[m, k])
            for k, held in enumerate((gates, ups, downs))
        ]
        for m in range(shards_)
    ]
    for shard in copies:
        for copy in shard:
            copy.start()
    for t in range(rows // tile):
        wide[...] = in_ref[t * tile * cuts : (t + 1) * tile * cuts, :].astype(F32)
        x_ref[t * tile : (t + 1) * tile, :] = gathered(wide, tile, cuts)
    for m in range(shards_):
        for copy in copies[m]:
            copy.wait()

        def one(t, carry):
            at = pl.ds(pl.multiple_of(t * tile, tile), tile)
            x = x_ref[at, :]
            part = mm(gated(mm(x, gates[m]), mm(x, ups[m])), downs[m])
            out_ref[at, :] = part if m == 0 else out_ref[at, :] + part
            return carry

        lax.fori_loop(0, rows // tile, one, 0)


def near_experts(spread_in, shards_):
    weights = [w for shard in shards_ for w in shard]
    width, hidden = shards_[0][0].shape
    rows = spread_in.shape[0] * LANES // width
    count = len(shards_)
    vmem = pl.BlockSpec(memory_space=pltpu.VMEM)
    return pl.pallas_call(
        near_experts_kernel,
        in_specs=[vmem] + [pl.BlockSpec(memory_space=pl.ANY)] * len(weights),
        out_specs=[vmem, vmem],
        out_shape=[
            jax.ShapeDtypeStruct((rows, width), BF16),
            jax.ShapeDtypeStruct((rows, width), F32),
        ],
        scratch_shapes=[
            pltpu.VMEM((128 * width // LANES, LANES), F32),
            pltpu.VMEM((count, width, hidden), BF16),
            pltpu.VMEM((count, width, hidden), BF16),
            pltpu.VMEM((count, hidden, width), BF16),
            pltpu.SemaphoreType.DMA((count, 3)),
        ],
        cost_estimate=pl.CostEstimate(flops=5_000_000_000, bytes_accessed=16_000_000, transcendentals=0),
        name="near_experts",
    )(spread_in, *weights)


def far_expert_kernel(x_ref, near_ref, *refs):
    hbm, (out_ref, wide, near, gate, up, down, sems) = (near_ref, *refs[:4]), refs[4:]
    half = up.shape[0] // 2
    rows, width = x_ref.shape
    cuts = width // LANES
    tile = 128
    spots = (near, gate, up.at[:half], up.at[half:], down)
    copies = [
        pltpu.make_async_copy(src, dst, sems.at[k]) for k, (src, dst) in enumerate(zip(hbm, spots))
    ]
    for k in (1, 2, 3, 4, 0):
        copies[k].start()
    for k in (1, 2, 3, 4, 0):
        copies[k].wait()

    def one(t, carry):
        at = pl.ds(pl.multiple_of(t * tile, tile), tile)
        x = x_ref[at, :]
        total = near[at, :] + mm(gated(mm(x, gate[...]), mm(x, up[...])), down[...])
        spread(wide, tile, 0, total)
        spot = pl.ds(pl.multiple_of(t * (tile * cuts), tile * cuts), tile * cuts)
        out_ref[spot, :] = wide[...].astype(BF16)
        return carry

    lax.fori_loop(0, rows // tile, one, 0)


def far_expert(x, near, gate, up0, up1, down):
    rows, width = x.shape
    hidden = gate.shape[1]
    cuts = width // LANES
    vmem = pl.BlockSpec(memory_space=pltpu.VMEM)
    return pl.pallas_call(
        far_expert_kernel,
        in_specs=[vmem] + [pl.BlockSpec(memory_space=pl.ANY)] * 5,
        out_specs=vmem,
        out_shape=jax.ShapeDtypeStruct((rows * cuts, LANES), BF16),
        scratch_shapes=[
            pltpu.VMEM((128 * cuts, LANES), F32),
            pltpu.VMEM((rows, width), F32),
            pltpu.VMEM((width, hidden), BF16),
            pltpu.VMEM((width, hidden), BF16),
            pltpu.VMEM((hidden, width), BF16),
            pltpu.SemaphoreType.DMA((5,)),
        ],
        cost_estimate=pl.CostEstimate(flops=2_000_000_000, bytes_accessed=12_000_000, transcendentals=0),
        name="far_expert",
    )(x, near, gate, up0, up1, down)


def spread(wide, rows, start, values):
    cuts = values.shape[1] // LANES
    for c in range(cuts):
        wide[pl.ds(start * cuts + c, rows, stride=cuts), :] = values[:, c * LANES : (c + 1) * LANES]


def gathered(wide, rows, cuts):
    return jnp.concatenate(
        [wide[pl.ds(c, rows, stride=cuts), :].astype(BF16) for c in range(cuts)], 1
    )


def dispatch_kernel(capacity, x_ref, gain_ref, routes_ref, weight_ref, xn_ref, out_ref, mix_ref, wide):
    tokens, width = x_ref.shape
    slots = mix_ref.shape[1]
    x = x_ref[...].astype(F32)
    xn = (x * lax.rsqrt(jnp.mean(x * x, axis=1, keepdims=True) + EPS) * gain_ref[...]).astype(BF16)
    xn_ref[...] = xn
    expert = lax.broadcasted_iota(jnp.int32, (LANES, tokens), 0)
    first, second = expert == routes_ref[0:1, :], expert == routes_ref[1:2, :]
    chosen = (first | second).astype(BF16)
    token = lax.broadcasted_iota(jnp.int32, (tokens, tokens), 0)
    later = lax.broadcasted_iota(jnp.int32, (tokens, tokens), 1)
    place = mm(chosen, (token < later).astype(BF16)) + (expert * capacity).astype(F32)
    s0 = jnp.sum(jnp.where(first, place, 0.0), axis=0, keepdims=True)
    s1 = jnp.sum(jnp.where(second, place, 0.0), axis=0, keepdims=True)
    step = 128
    cuts = width // LANES
    for base in range(0, slots, step):
        slot = (lax.broadcasted_iota(jnp.int32, (step, tokens), 0) + base).astype(F32)
        is0, is1 = slot == s0, slot == s1
        spread(wide, step, 0, mm((is0 | is1).astype(BF16), xn))
        out_ref[base * cuts : (base + step) * cuts, :] = wide[...].astype(BF16)
        mix = jnp.where(is0, weight_ref[0:1, :], 0.0) + jnp.where(is1, weight_ref[1:2, :], 0.0)
        mix_ref[:, base : base + step] = mix.T


def dispatch(x, gain, routes, weight, slots, capacity):
    tokens, width = x.shape
    cuts = width // LANES
    return pl.pallas_call(
        functools.partial(dispatch_kernel, capacity),
        out_shape=[
            jax.ShapeDtypeStruct((tokens, width), BF16),
            jax.ShapeDtypeStruct((slots * cuts, LANES), BF16),
            jax.ShapeDtypeStruct((tokens, slots), F32),
        ],
        scratch_shapes=[pltpu.VMEM((128 * cuts, LANES), F32)],
        name="dispatch",
    )(x, gain.reshape(1, width), routes, weight)


def mixer_sum_kernel(*refs):
    *part_refs, out_ref = refs
    total = part_refs[0][...].astype(F32)
    for part in part_refs[1:]:
        total = total + part[...].astype(F32)
    out_ref[...] = total.astype(BF16)


def mixer_sum(parts):
    rows, width = parts[0].shape
    half = pl.BlockSpec((rows // 2, width), lambda c: (0, 0))
    return pl.pallas_call(
        mixer_sum_kernel,
        grid=(1,),
        in_specs=[half] * len(parts),
        out_specs=half,
        out_shape=jax.ShapeDtypeStruct((rows // 2, width), BF16),
        cost_estimate=pl.CostEstimate(flops=1_000_000_000, bytes_accessed=3_000_000, transcendentals=0),
        name="mixer_sum",
    )(*parts)


def combine_kernel(*refs):
    *part_refs, back_ref, mix_ref, out_ref, wide, total = refs
    rows = mix_ref.shape[1]
    cuts = total.shape[1] // LANES
    step = pl.program_id(0)

    @pl.when(step == 0)
    def _():
        shared = part_refs[0][...].astype(F32)
        for part in part_refs[1:]:
            shared = shared + part[...].astype(F32)
        total[...] = shared

    wide[...] = back_ref[...].astype(F32)
    total[...] += dot2(mix_ref[...], gathered(wide, rows, cuts))

    @pl.when(step == pl.num_programs(0) - 1)
    def _():
        out_ref[...] = total[...].astype(BF16)


def combine(parts, back, mix):
    tokens, slots = mix.shape
    width = parts[0].shape[1]
    cuts = width // LANES
    tile = 128
    return pl.pallas_call(
        combine_kernel,
        grid=(slots // tile,),
        in_specs=[pl.BlockSpec((tokens, width), lambda c: (1, 0))] * len(parts)
        + [
            pl.BlockSpec((tile * cuts, LANES), lambda c: (c, 0)),
            pl.BlockSpec((tokens, tile), lambda c: (0, c)),
        ],
        out_specs=pl.BlockSpec((tokens, width), lambda c: (0, 0)),
        out_shape=jax.ShapeDtypeStruct((tokens, width), BF16),
        scratch_shapes=[pltpu.VMEM((tile * cuts, LANES), F32), pltpu.VMEM((tokens, width), F32)],
        name="combine",
    )(*parts, back, mix)


def ring(axis):
    peers = lax.axis_size(axis)
    return (
        [(i, (i + 1) % peers) for i in range(peers)],
        [(i, (i - 1) % peers) for i in range(peers)],
    )


def neighbours_shards(shard, axis):
    right, left = ring(axis)
    from_left = [lax.ppermute(w, axis, right) for w in shard]
    from_right = [lax.ppermute(w, axis, left) for w in shard]
    return from_left, from_right


def far_shard(from_left, from_right, axis):
    right, left = ring(axis)
    half = from_left[1].shape[0] // 2
    return (
        lax.ppermute(from_left[0], axis, right),
        lax.ppermute(from_left[1][:half], axis, right),
        lax.ppermute(from_right[1][half:], axis, left),
        lax.ppermute(from_right[2], axis, left),
    )


def gated(gate_val, up_val):
    return (jax.nn.silu(gate_val) * up_val).astype(BF16)


def shards(
    queries,
    keys,
    values,
    decay_gate_logits,
    correction_logits,
    head_decay_speed,
    position_log_decay,
    head_output_gain,
    mixer_output_weight,
    expert_input_tokens,
    expert_norm_gain,
    routes,
    chosen_expert_weight,
    routed_gate_weight,
    routed_up_weight,
    routed_down_weight,
    common_gate_weight,
    common_up_weight,
    common_down_weight,
):
    experts = lax.axis_size(EP)
    tokens, _ = expert_input_tokens.shape
    own = (routed_gate_weight[0], routed_up_weight[0], routed_down_weight[0])
    from_left, from_right = neighbours_shards(own, "tp")

    capacity = 3 * tokens * routes.shape[1] // (2 * experts)
    xn, outgoing, mix = dispatch(
        expert_input_tokens,
        expert_norm_gain,
        routes.T,
        chosen_expert_weight.T,
        experts * capacity,
        capacity,
    )

    def to_peers(x):
        parts = x.reshape(experts, -1, LANES)
        return lax.all_to_all(parts, EP, split_axis=0, concat_axis=0, tiled=True).reshape(-1, LANES)

    arrived = to_peers(outgoing)

    qt, ol, trans, inject = local_mixer(
        queries,
        keys,
        values,
        decay_gate_logits.T,
        correction_logits.T,
        head_decay_speed,
        position_log_decay.T,
    )
    state, group = entry_state(trans, inject, xn)
    state, from_left, from_right = lax.optimization_barrier((state, from_left, from_right))
    far = far_shard(from_left, from_right, "tp")
    me = lax.axis_index("tp").astype(jnp.int32).reshape(1)
    parts = parts_for_peers(
        me,
        lax.axis_size("tp"),
        qt,
        ol,
        state,
        head_output_gain,
        mixer_output_weight,
        group,
        common_gate_weight,
        common_up_weight,
        common_down_weight,
    )
    rows, near = near_experts(arrived, (own, from_left, from_right))
    parts, near = lax.optimization_barrier((parts, near))
    peers = lax.axis_size("tp")
    got = [parts[0]] + [
        lax.ppermute(parts[r], "tp", [(i, (i + r) % peers) for i in range(peers)])
        for r in range(1, peers)
    ]
    slot_sums = far_expert(rows, near, *far)
    back = to_peers(slot_sums)
    return (mixer_sum(got), combine(got, back, mix))


def solution(mesh):
    finer = Mesh(mesh.devices.reshape(8, 4, 2, mesh.shape["tp"]), ("ep_0", "ep_1", "ep_2", "tp"))
    placed = (
        P(EP, "tp"),
        P(EP, "tp"),
        P(EP, "tp"),
        P(EP, "tp"),
        P(EP, "tp"),
        P("tp"),
        P(EP, "tp"),
        P(),
        P("tp", None),
        P(EP_TP, None),
        P(),
        P(EP_TP, None),
        P(EP_TP, None),
        P(EP, None, "tp"),
        P(EP, None, "tp"),
        P(EP, "tp", None),
        P(None, "tp"),
        P(None, "tp"),
        P("tp", None),
    )
    return jax.shard_map(
        shards,
        mesh=finer,
        in_specs=placed,
        out_specs=(P(EP_TP, None), P(EP_TP, None)),
        check_vma=False,
    )
```

```python
import functools

import jax
import jax.numpy as jnp
from jax import lax
from jax.experimental import pallas as pl
from jax.experimental.pallas import tpu as pltpu
from jax.sharding import Mesh
from jax.sharding import PartitionSpec as P


EP = ("ep_0", "ep_1", "ep_2")
EP_TP = ("ep_0", "ep_1", "ep_2", "tp")


EPS = 1e-06
F32 = jnp.float32
BF16 = jnp.bfloat16
LANES = 128
MESH = pl.DeviceIdType.MESH


def halves(x):
    hi = x.astype(BF16)
    return hi, (x - hi.astype(F32)).astype(BF16)


def thirds(x):
    hi = x.astype(BF16)
    rest = x - hi.astype(F32)
    mid = rest.astype(BF16)
    return hi, mid, (rest - mid.astype(F32)).astype(BF16)


def mm(a, b):
    return jnp.dot(a, b, preferred_element_type=F32)


def dot3(a, b):
    ah, al = halves(a)
    bh, bl = halves(b)
    return mm(jnp.concatenate([ah, ah, al], 1), jnp.concatenate([bh, bl, bh], 0))


def dot2(a, b):
    ah, al = halves(a)
    return mm(jnp.concatenate([ah, al], 1), jnp.concatenate([b, b], 0))


def unit_lower_inverses(lows, row, col):
    eye = (row == col).astype(F32)
    near = (row >> 3) == (col >> 3)
    base = [jnp.where(near, low, 0.0) for low in lows]
    squared = [dot3(x, x) for x in base]
    inv = [eye - x for x in base]
    fourth = [dot3(x, x) for x in squared]
    inv = [x + dot3(x, y) for x, y in zip(inv, squared)]
    inv = [x + dot3(x, y) for x, y in zip(inv, fourth)]
    for bit in (3, 4, 5):
        between = ((row >> (bit + 1)) == (col >> (bit + 1))) & ((row >> bit) != (col >> bit))
        right = [dot3(jnp.where(between, low, 0.0), x) for low, x in zip(lows, inv)]
        inv = [x - dot3(x, y) for x, y in zip(inv, right)]
    return inv


def local_mixer_kernel(
    q_ref, k_ref, v_ref, gate_ref, corr_ref, speed_ref, plog_ref, qt_ref, ol_ref, tr_ref, in_ref,
    su_all, pq_all, mw_all, keep_all,
):
    head = pl.program_id(0)
    heads, rows = gate_ref.shape
    pair = 128
    here = lax.broadcasted_iota(jnp.int32, (heads, rows), 0) == head

    log_gate = (
        -speed_ref[...]
        * (jnp.maximum(gate_ref[...], 0.0) + jnp.log1p(jnp.exp(-jnp.abs(gate_ref[...]))))
        + plog_ref[...]
    )
    beta_all = 1.0 / (1.0 + jnp.exp(-corr_ref[...].astype(F32)))
    g_row = jnp.sum(jnp.where(here, log_gate, 0.0), axis=0, keepdims=True)
    beta_row_all = jnp.sum(jnp.where(here, beta_all, 0.0), axis=0, keepdims=True)

    row = lax.broadcasted_iota(jnp.int32, (pair, pair), 0)
    col = lax.broadcasted_iota(jnp.int32, (pair, pair), 1)
    same = (row >> 6) == (col >> 6)
    causal = same & (row >= col)
    strict = same & (row > col)
    first = col < 64
    ones = (same & (row <= col)).astype(BF16)
    ones = jnp.concatenate([ones, ones, ones], 0)

    pairs = range(rows // pair)
    span = [slice(p * pair, (p + 1) * pair) for p in pairs]
    qb, kb, vb = [[ref[at, :] for at in span] for ref in (q_ref, k_ref, v_ref)]
    gram = [
        lax.dot_general(
            jnp.concatenate([k, q], 0), k, (((1,), (1,)), ((), ())), preferred_element_type=F32
        )
        for k, q in zip(kb, qb)
    ]
    c_row = [
        mm(jnp.concatenate(thirds(jnp.broadcast_to(g_row[:, at], (pair, pair))), 1), ones)
        for at in span
    ]
    c_mat = [c.T for c in c_row]
    qf, kf = [x.astype(F32) for x in qb], [x.astype(F32) for x in kb]
    rq = [
        lax.rsqrt(jnp.sum(x * x, axis=1, keepdims=True) + EPS) * (pair**-0.5) for x in qf
    ]
    rk = [lax.rsqrt(jnp.sum(x * x, axis=1, keepdims=True) + EPS) for x in kf]
    rk_row = [jnp.broadcast_to(x, (pair, pair)).T for x in rk]
    beta_row = [jnp.broadcast_to(beta_row_all[:, at], (pair, pair)) for at in span]
    beta = [x.T for x in beta_row]
    decay = [
        jnp.exp(jnp.where(causal, cm - cr, -jnp.inf)) * r for cm, cr, r in zip(c_mat, c_row, rk_row)
    ]
    low = [
        jnp.where(strict, g[:pair] * d * (b * r), 0.0) for g, d, b, r in zip(gram, decay, beta, rk)
    ]
    scores = [g[pair:] * d * r for g, d, r in zip(gram, decay, rq)]
    inv = unit_lower_inverses(low, row, col)
    scale = [b * x for b, x in zip(beta_row, inv)]
    u = [dot2(x, v) for x, v in zip(scale, vb)]
    w = [dot2(x * (jnp.exp(c) * r), k) for x, c, r, k in zip(scale, c_row, rk_row, kb)]
    uw = [jnp.concatenate([x, y], 1) for x, y in zip(u, w)]
    last = [(c[63:64, :], c[127:128, :]) for c in c_mat]
    kt = [
        k.T * (jnp.exp(jnp.where(first, l[0], l[1]) - c) * r)
        for k, l, c, r in zip(kf, last, c_row, rk_row)
    ]
    suw = [dot3(x, y) for x, y in zip(scores, uw)]
    mw = [
        dot3(jnp.concatenate([jnp.where(first, x, 0.0), jnp.where(first, 0.0, x)], 0), y)
        for x, y in zip(kt, uw)
    ]
    pq = [x * (r * jnp.exp(c)) - y[:, pair:] for x, r, c, y in zip(qf, rq, c_mat, suw)]
    for p in pairs:
        su_all[head, p] = suw[p][:, :pair]
        pq_all[head, p] = pq[p]
        mw_all[head, p] = mw[p]
        keep_all[head, p] = jnp.concatenate([jnp.exp(x) for x in last[p]], 0)

    @pl.when(head == heads - 1)
    def _():
        nothing = jnp.zeros((pair, pair), F32)
        ab = [jnp.concatenate([(row == col).astype(F32), nothing], 1) for _ in range(heads)]
        for p in pairs:
            for b in range(2):
                blk = slice(b * 64, (b + 1) * 64)
                at = pl.ds(p * pair + b * 64, 64)
                part = [mw_all[h, p, b * pair : (b + 1) * pair, :] for h in range(heads)]
                got = [
                    dot3(jnp.concatenate([pq_all[h, p, blk, :], part[h][:, pair:]], 0), ab[h])
                    for h in range(heads)
                ]
                for h in range(heads):
                    qt_ref[h, at, :] = got[h][:64, :pair]
                    ol_ref[h, at, :] = got[h][:64, pair:] + su_all[h, p, blk, :]
                    keep = keep_all[h, p, b : b + 1, :]
                    ab[h] = (
                        jnp.concatenate([keep, keep], 1) * ab[h]
                        - got[h][64:]
                        + jnp.concatenate([nothing, part[h][:, :pair]], 1)
                    )
        for h in range(heads):
            tr_ref[h] = ab[h][:, :pair]
            in_ref[h] = ab[h][:, pair:]


def local_mixer(queries, keys, values, gate, corr, speed, plog):
    rows, width = queries.shape
    heads = gate.shape[0]
    d = width // heads
    by_head = pl.BlockSpec((rows, d), lambda h: (0, h))
    whole = pl.BlockSpec((heads, rows), lambda h: (0, 0))
    return pl.pallas_call(
        local_mixer_kernel,
        grid=(heads,),
        in_specs=[
            by_head,
            by_head,
            by_head,
            whole,
            whole,
            pl.BlockSpec((heads, 1), lambda h: (0, 0)),
            whole,
        ],
        out_specs=[
            pl.BlockSpec((heads, rows, d), lambda h: (0, 0, 0)),
            pl.BlockSpec((heads, rows, d), lambda h: (0, 0, 0)),
            pl.BlockSpec((heads, d, d), lambda h: (0, 0, 0)),
            pl.BlockSpec((heads, d, d), lambda h: (0, 0, 0)),
        ],
        scratch_shapes=[
            pltpu.VMEM((heads, rows // 128, 128, d), F32),
            pltpu.VMEM((heads, rows // 128, 128, d), F32),
            pltpu.VMEM((heads, rows // 128, 2 * d, 2 * d), F32),
            pltpu.VMEM((heads, rows // 128, 2, d), F32),
        ],
        out_shape=[
            jax.ShapeDtypeStruct((heads, rows, d), F32),
            jax.ShapeDtypeStruct((heads, rows, d), F32),
            jax.ShapeDtypeStruct((heads, d, d), F32),
            jax.ShapeDtypeStruct((heads, d, d), F32),
        ],
        cost_estimate=pl.CostEstimate(flops=30_000_000_000, bytes_accessed=4_000_000, transcendentals=0),
        name="local_mixer",
    )(queries, keys, values, gate, corr, speed.reshape(heads, 1), plog)


def entry_state_kernel(
    t_ref, i_ref, s_ref, own, peer, ypack, zpack,
    send_c, recv_c, send_y, recv_y, send_yc, recv_yc,
    send_r, recv_r, send_l, recv_l, send_rc, recv_rc, send_lc, recv_lc,
):
    heads, d, _ = t_ref.shape
    half = d // 2
    nz, ny = zpack.shape[0], ypack.shape[0]
    z, y, c = lax.axis_index("ep_0"), lax.axis_index("ep_1"), lax.axis_index("ep_2")
    other = {"ep_2": 1 - c}
    right, left = {"ep_0": lax.rem(z + 1, nz)}, {"ep_0": lax.rem(z + nz - 1, nz)}
    across = [{"ep_1": lax.rem(y + k, ny)} for k in range(1, ny)]

    barrier = pltpu.get_barrier_semaphore()
    for who in (other, right, left, *across):
        pl.semaphore_signal(barrier, inc=1, device_id=who, device_id_type=MESH)
    pl.semaphore_wait(barrier, 3 + len(across))

    def send(src, dst, send_sem, recv_sem, who):
        return pltpu.make_async_remote_copy(
            src_ref=src, dst_ref=dst, send_sem=send_sem, recv_sem=recv_sem,
            device_id=who, device_id_type=MESH,
        )

    def store(ref, h, both):
        both = both.astype(BF16)
        ref[0, h] = both[:half]
        ref[1, h] = both[half:]

    def load(ref, h):
        return jnp.concatenate([ref[0, h], ref[1, h]], 0)

    def after(pack, so_far):
        hi, lo = halves(so_far)
        t = pack[:, :d]
        return mm(jnp.concatenate([t, t], 1), jnp.concatenate([hi, lo], 0))

    def added(pack):
        return pack[:, d:].astype(F32)

    nothing = jnp.zeros((d, d), F32)
    for h in range(heads):
        store(own, h, jnp.concatenate([t_ref[h], i_ref[h]], 1))
    swap = send(own, peer, send_c, recv_c, other)
    swap.start()
    swap.wait()
    for h in range(heads):
        mine, theirs = load(own, h), load(peer, h)
        early = jnp.where(c == 0, mine.astype(F32), theirs.astype(F32)).astype(BF16)
        late = jnp.where(c == 0, theirs.astype(F32), mine.astype(F32)).astype(BF16)
        both = mm(late[:, :d], early) + jnp.concatenate([nothing, added(late)], 1)
        store(ypack.at[y], h, both)

    out = [
        send(ypack.at[y, c], ypack.at[y, c], send_y.at[k - 1], recv_y.at[k - 1], across[k - 1])
        for k in range(1, ny)
    ]
    for copy in out:
        copy.start()
    over = []
    for k in range(1, ny):
        slot = ypack.at[lax.rem(y + ny - k, ny), c]
        out[k - 1].wait_recv()
        over.append(send(slot, slot, send_yc.at[k - 1], recv_yc.at[k - 1], other))
        over[-1].start()
    for copy in out:
        copy.wait_send()
    for copy in over:
        copy.wait()
    for h in range(heads):
        both = load(ypack.at[0], h).astype(F32)
        for k in range(1, ny):
            pack = load(ypack.at[k], h)
            both = after(pack, both) + jnp.concatenate([nothing, added(pack)], 1)
        store(zpack.at[z], h, both)

    def going(r, h, sign, who, send_sem, recv_sem):
        slot = zpack.at[lax.rem(z + nz - sign * (r - 1), nz), c, h]
        return send(slot, slot, send_sem.at[r - 1, h], recv_sem.at[r - 1, h], who)

    def shared_with_other(r, h, sign, send_sem, recv_sem):
        slot = zpack.at[lax.rem(z + nz - sign * r, nz), c, h]
        return send(slot, slot, send_sem.at[r - 1, h], recv_sem.at[r - 1, h], other)

    rings = (
        (nz // 2, 1, right, send_r, recv_r, send_rc, recv_rc),
        ((nz - 1) // 2, -1, left, send_l, recv_l, send_lc, recv_lc),
    )
    pending = []
    for rounds, sign, who, ss, rs, _, _ in rings:
        for h in range(heads):
            if rounds > 0:
                going(1, h, sign, who, ss, rs).start()
    for r in range(1, nz // 2 + 1):
        for h in range(heads):
            for rounds, sign, who, ss, rs, sc, rc in rings:
                if r > rounds:
                    continue
                copy = going(r, h, sign, who, ss, rs)
                copy.wait_recv()
                pending.append((copy, False))
                if r < rounds:
                    going(r + 1, h, sign, who, ss, rs).start()
                hand = shared_with_other(r, h, sign, sc, rc)
                hand.start()
                pending.append((hand, True))
    for copy, both_ways in pending:
        copy.wait_send()
        if both_ways:
            copy.wait_recv()

    for h in range(heads):
        s_ref[h] = nothing
    for k in range(nz - 1):
        for h in range(heads):
            pack = load(zpack.at[k], h)
            s_ref[h] = jnp.where(k < z, after(pack, s_ref[h]) + added(pack), s_ref[h])
    for k in range(ny - 1):
        for h in range(heads):
            pack = load(ypack.at[k], h)
            s_ref[h] = jnp.where(k < y, after(pack, s_ref[h]) + added(pack), s_ref[h])
    for h in range(heads):
        pack = load(peer, h)
        s_ref[h] = jnp.where(c == 1, after(pack, s_ref[h]) + added(pack), s_ref[h])


def entry_state(trans, inject):
    heads, d, _ = trans.shape
    nz, ny = lax.axis_size("ep_0"), lax.axis_size("ep_1")
    half = (2, heads, d // 2, 2 * d)
    dma = pltpu.SemaphoreType.DMA
    rounds = max(nz // 2, 1)
    vmem = pl.BlockSpec(memory_space=pltpu.VMEM)
    return pl.pallas_call(
        entry_state_kernel,
        in_specs=[vmem, vmem],
        out_specs=vmem,
        out_shape=jax.ShapeDtypeStruct((heads, d, d), F32),
        scratch_shapes=[
            pltpu.VMEM(half, BF16),
            pltpu.VMEM(half, BF16),
            pltpu.VMEM((ny, *half), BF16),
            pltpu.VMEM((nz, *half), BF16),
            dma, dma,
            dma((max(ny - 1, 1),)), dma((max(ny - 1, 1),)), dma((max(ny - 1, 1),)), dma((max(ny - 1, 1),)),
            *[dma((rounds, heads)) for _ in range(8)],
        ],
        compiler_params=pltpu.CompilerParams(collective_id=0, has_side_effects=True),
        cost_estimate=pl.CostEstimate(flops=30_000_000_000, bytes_accessed=4_000_000, transcendentals=0),
        name="entry_state",
    )(trans, inject)


def parts_kernel(peers, me_ref, qt_ref, ol_ref, state_ref, gain_ref, w_ref, *refs):
    hbm, refs = refs[: peers + 3], refs[peers + 3 :]
    out_refs, (x, gate, up, down, sems) = refs[:peers], refs[peers:]
    heads, rows, _ = qt_ref.shape
    tile = rows // peers
    spots = [x.at[r * tile : (r + 1) * tile] for r in range(peers)] + [gate, up, down]
    copies = [
        pltpu.make_async_copy(src, dst, sems.at[k]) for k, (src, dst) in enumerate(zip(hbm, spots))
    ]
    for copy in copies:
        copy.start()
    turns = [
        pl.ds(pl.multiple_of(lax.rem(me_ref[0] + r, peers) * tile, tile), tile)
        for r in range(peers)
    ]
    normed = []
    for h in range(heads):
        qt = jnp.concatenate([qt_ref[h, at, :] for at in turns], 0)
        ol = jnp.concatenate([ol_ref[h, at, :] for at in turns], 0)
        out = dot3(qt, state_ref[h]) + ol
        out = out * lax.rsqrt(jnp.mean(out * out, axis=1, keepdims=True) + EPS) * gain_ref[...]
        normed.append(out.astype(BF16))
    mixer = mm(jnp.concatenate(normed, 1), w_ref[...]).astype(BF16)
    for r in range(peers):
        out_refs[r][:tile] = mixer[r * tile : (r + 1) * tile]
    for copy in copies:
        copy.wait()
    hidden = gated(mm(x[...], gate[...]), mm(x[...], up[...]))
    shared = mm(hidden, down[...]).astype(BF16)
    for r in range(peers):
        out_refs[r][tile:] = shared[r * tile : (r + 1) * tile]


def parts_for_peers(me, qt, ol, state, gain, w, tokens, gate, up, down):
    _, rows, d = qt.shape
    width = w.shape[1]
    peers = len(tokens)
    tile = rows // peers
    vmem = pl.BlockSpec(memory_space=pltpu.VMEM)
    kept = (*tokens, gate, up, down)
    return pl.pallas_call(
        functools.partial(parts_kernel, peers),
        in_specs=[pl.BlockSpec(memory_space=pltpu.SMEM)]
        + [vmem] * 5
        + [pl.BlockSpec(memory_space=pl.ANY)] * len(kept),
        out_specs=[vmem] * peers,
        out_shape=[jax.ShapeDtypeStruct((2 * tile, width), BF16)] * peers,
        scratch_shapes=[
            pltpu.VMEM((rows, width), BF16),
            pltpu.VMEM(gate.shape, BF16),
            pltpu.VMEM(up.shape, BF16),
            pltpu.VMEM(down.shape, BF16),
            pltpu.SemaphoreType.DMA((len(kept),)),
        ],
        cost_estimate=pl.CostEstimate(flops=6_000_000_000, bytes_accessed=12_000_000, transcendentals=0),
        name="parts_for_peers",
    )(me, qt, ol, state, gain.reshape(1, d), w, *kept)


def near_experts_kernel(in_ref, *refs):
    shards_ = len(refs) // 3 - 2
    hbm, (x_ref, out_ref, wide, gates, ups, downs) = refs[: 3 * shards_], refs[3 * shards_ : -1]
    sems = refs[-1]
    rows, width = x_ref.shape
    cuts = width // LANES
    tile = 128
    copies = [
        [
            pltpu.make_async_copy(hbm[3 * m + k], held.at[m], sems.at[m, k])
            for k, held in enumerate((gates, ups, downs))
        ]
        for m in range(shards_)
    ]
    for shard in copies:
        for copy in shard:
            copy.start()
    for t in range(rows // tile):
        wide[...] = in_ref[t * tile * cuts : (t + 1) * tile * cuts, :].astype(F32)
        x_ref[t * tile : (t + 1) * tile, :] = gathered(wide, tile, cuts)
    for m in range(shards_):
        for copy in copies[m]:
            copy.wait()
        x = x_ref[...]
        part = mm(gated(mm(x, gates[m]), mm(x, ups[m])), downs[m])
        out_ref[...] = part if m == 0 else out_ref[...] + part


def near_experts(spread_in, shards_):
    weights = [w for shard in shards_ for w in shard]
    width, hidden = shards_[0][0].shape
    rows = spread_in.shape[0] * LANES // width
    count = len(shards_)
    vmem = pl.BlockSpec(memory_space=pltpu.VMEM)
    return pl.pallas_call(
        near_experts_kernel,
        in_specs=[vmem] + [pl.BlockSpec(memory_space=pl.ANY)] * len(weights),
        out_specs=[vmem, vmem],
        out_shape=[
            jax.ShapeDtypeStruct((rows, width), BF16),
            jax.ShapeDtypeStruct((rows, width), F32),
        ],
        scratch_shapes=[
            pltpu.VMEM((128 * width // LANES, LANES), F32),
            pltpu.VMEM((count, width, hidden), BF16),
            pltpu.VMEM((count, width, hidden), BF16),
            pltpu.VMEM((count, hidden, width), BF16),
            pltpu.SemaphoreType.DMA((count, 3)),
        ],
        cost_estimate=pl.CostEstimate(flops=5_000_000_000, bytes_accessed=16_000_000, transcendentals=0),
        name="near_experts",
    )(spread_in, *weights)


def far_expert_kernel(x_ref, near_ref, *refs):
    hbm, (out_ref, wide, near, gate, up, down, sems) = (near_ref, *refs[:4]), refs[4:]
    half = up.shape[0] // 2
    rows, width = x_ref.shape
    cuts = width // LANES
    tile = 128
    spots = (near, gate, up.at[:half], up.at[half:], down)
    copies = [
        pltpu.make_async_copy(src, dst, sems.at[k]) for k, (src, dst) in enumerate(zip(hbm, spots))
    ]
    for k in (1, 2, 3, 4, 0):
        copies[k].start()
    for k in (1, 2, 3):
        copies[k].wait()
    x = x_ref[...]
    hidden = gated(mm(x, gate[...]), mm(x, up[...]))
    for k in (4, 0):
        copies[k].wait()
    for t in range(rows // tile):
        at = slice(t * tile, (t + 1) * tile)
        spread(wide, tile, 0, near[at, :] + mm(hidden[at], down[...]))
        out_ref[t * tile * cuts : (t + 1) * tile * cuts, :] = wide[...].astype(BF16)


def far_expert(x, near, gate, up0, up1, down):
    rows, width = x.shape
    hidden = gate.shape[1]
    cuts = width // LANES
    vmem = pl.BlockSpec(memory_space=pltpu.VMEM)
    return pl.pallas_call(
        far_expert_kernel,
        in_specs=[vmem] + [pl.BlockSpec(memory_space=pl.ANY)] * 5,
        out_specs=vmem,
        out_shape=jax.ShapeDtypeStruct((rows * cuts, LANES), BF16),
        scratch_shapes=[
            pltpu.VMEM((128 * cuts, LANES), F32),
            pltpu.VMEM((rows, width), F32),
            pltpu.VMEM((width, hidden), BF16),
            pltpu.VMEM((width, hidden), BF16),
            pltpu.VMEM((hidden, width), BF16),
            pltpu.SemaphoreType.DMA((5,)),
        ],
        cost_estimate=pl.CostEstimate(flops=2_000_000_000, bytes_accessed=12_000_000, transcendentals=0),
        name="far_expert",
    )(x, near, gate, up0, up1, down)


def spread(wide, rows, start, values):
    cuts = values.shape[1] // LANES
    for c in range(cuts):
        wide[pl.ds(start * cuts + c, rows, stride=cuts), :] = values[:, c * LANES : (c + 1) * LANES]


def gathered(wide, rows, cuts):
    return jnp.concatenate(
        [wide[pl.ds(c, rows, stride=cuts), :].astype(BF16) for c in range(cuts)], 1
    )


def dispatch_kernel(capacity, x_ref, gain_ref, routes_ref, weight_ref, xn_ref, out_ref, mix_ref, wide):
    tokens, width = x_ref.shape
    slots = mix_ref.shape[1]
    x = x_ref[...].astype(F32)
    xn = (x * lax.rsqrt(jnp.mean(x * x, axis=1, keepdims=True) + EPS) * gain_ref[...]).astype(BF16)
    xn_ref[...] = xn
    expert = lax.broadcasted_iota(jnp.int32, (LANES, tokens), 0)
    first, second = expert == routes_ref[0:1, :], expert == routes_ref[1:2, :]
    chosen = (first | second).astype(BF16)
    token = lax.broadcasted_iota(jnp.int32, (tokens, tokens), 0)
    later = lax.broadcasted_iota(jnp.int32, (tokens, tokens), 1)
    place = mm(chosen, (token < later).astype(BF16)) + (expert * capacity).astype(F32)
    s0 = jnp.sum(jnp.where(first, place, 0.0), axis=0, keepdims=True)
    s1 = jnp.sum(jnp.where(second, place, 0.0), axis=0, keepdims=True)
    step = 128
    cuts = width // LANES
    for base in range(0, slots, step):
        slot = (lax.broadcasted_iota(jnp.int32, (step, tokens), 0) + base).astype(F32)
        is0, is1 = slot == s0, slot == s1
        spread(wide, step, 0, mm((is0 | is1).astype(BF16), xn))
        out_ref[base * cuts : (base + step) * cuts, :] = wide[...].astype(BF16)
        mix = jnp.where(is0, weight_ref[0:1, :], 0.0) + jnp.where(is1, weight_ref[1:2, :], 0.0)
        mix_ref[:, base : base + step] = mix.T


def dispatch(x, gain, routes, weight, slots, capacity):
    tokens, width = x.shape
    cuts = width // LANES
    return pl.pallas_call(
        functools.partial(dispatch_kernel, capacity),
        out_shape=[
            jax.ShapeDtypeStruct((tokens, width), BF16),
            jax.ShapeDtypeStruct((slots * cuts, LANES), BF16),
            jax.ShapeDtypeStruct((tokens, slots), F32),
        ],
        scratch_shapes=[pltpu.VMEM((128 * cuts, LANES), F32)],
        name="dispatch",
    )(x, gain.reshape(1, width), routes, weight)


def mixer_sum_kernel(*refs):
    *part_refs, out_ref = refs
    total = part_refs[0][...].astype(F32)
    for part in part_refs[1:]:
        total = total + part[...].astype(F32)
    out_ref[...] = total.astype(BF16)


def mixer_sum(parts):
    rows, width = parts[0].shape
    half = pl.BlockSpec((rows // 2, width), lambda c: (0, 0))
    return pl.pallas_call(
        mixer_sum_kernel,
        grid=(1,),
        in_specs=[half] * len(parts),
        out_specs=half,
        out_shape=jax.ShapeDtypeStruct((rows // 2, width), BF16),
        cost_estimate=pl.CostEstimate(flops=1_000_000_000, bytes_accessed=3_000_000, transcendentals=0),
        name="mixer_sum",
    )(*parts)


def combine_kernel(*refs):
    *part_refs, back_ref, mix_ref, out_ref, wide, total = refs
    rows = mix_ref.shape[1]
    cuts = total.shape[1] // LANES
    step = pl.program_id(0)

    @pl.when(step == 0)
    def _():
        shared = part_refs[0][...].astype(F32)
        for part in part_refs[1:]:
            shared = shared + part[...].astype(F32)
        total[...] = shared

    wide[...] = back_ref[...].astype(F32)
    total[...] += dot2(mix_ref[...], gathered(wide, rows, cuts))

    @pl.when(step == pl.num_programs(0) - 1)
    def _():
        out_ref[...] = total[...].astype(BF16)


def combine(parts, back, mix):
    tokens, slots = mix.shape
    width = parts[0].shape[1]
    cuts = width // LANES
    tile = 128
    return pl.pallas_call(
        combine_kernel,
        grid=(slots // tile,),
        in_specs=[pl.BlockSpec((tokens, width), lambda c: (1, 0))] * len(parts)
        + [
            pl.BlockSpec((tile * cuts, LANES), lambda c: (c, 0)),
            pl.BlockSpec((tokens, tile), lambda c: (0, c)),
        ],
        out_specs=pl.BlockSpec((tokens, width), lambda c: (0, 0)),
        out_shape=jax.ShapeDtypeStruct((tokens, width), BF16),
        scratch_shapes=[pltpu.VMEM((tile * cuts, LANES), F32), pltpu.VMEM((tokens, width), F32)],
        name="combine",
    )(*parts, back, mix)


def ring(axis):
    peers = lax.axis_size(axis)
    return (
        [(i, (i + 1) % peers) for i in range(peers)],
        [(i, (i - 1) % peers) for i in range(peers)],
    )


def neighbours_shards(shard, axis):
    right, left = ring(axis)
    from_left = [lax.ppermute(w, axis, right) for w in shard]
    from_right = [lax.ppermute(w, axis, left) for w in shard]
    return from_left, from_right


def far_shard(from_left, from_right, axis):
    right, left = ring(axis)
    half = from_left[1].shape[0] // 2
    return (
        lax.ppermute(from_left[0], axis, right),
        lax.ppermute(from_left[1][:half], axis, right),
        lax.ppermute(from_right[1][half:], axis, left),
        lax.ppermute(from_right[2], axis, left),
    )


def gated(gate_val, up_val):
    return (jax.nn.silu(gate_val) * up_val).astype(BF16)


def shards(
    queries,
    keys,
    values,
    decay_gate_logits,
    correction_logits,
    head_decay_speed,
    position_log_decay,
    head_output_gain,
    mixer_output_weight,
    expert_input_tokens,
    expert_norm_gain,
    routes,
    chosen_expert_weight,
    routed_gate_weight,
    routed_up_weight,
    routed_down_weight,
    common_gate_weight,
    common_up_weight,
    common_down_weight,
):
    experts = lax.axis_size(EP)
    tokens, _ = expert_input_tokens.shape
    own = (routed_gate_weight[0], routed_up_weight[0], routed_down_weight[0])
    from_left, from_right = neighbours_shards(own, "tp")

    capacity = 3 * tokens * routes.shape[1] // (2 * experts)
    xn, outgoing, mix = dispatch(
        expert_input_tokens,
        expert_norm_gain,
        routes.T,
        chosen_expert_weight.T,
        experts * capacity,
        capacity,
    )

    def to_peers(x):
        parts = x.reshape(experts, -1, LANES)
        return lax.all_to_all(parts, EP, split_axis=0, concat_axis=0, tiled=True).reshape(-1, LANES)

    peers = lax.axis_size("tp")

    def shift(r):
        return [(i, (i + r) % peers) for i in range(peers)]

    arrived = to_peers(outgoing)
    group = [xn] + [lax.ppermute(xn, "tp", shift(peers - r)) for r in range(1, peers)]

    qt, ol, trans, inject = local_mixer(
        queries,
        keys,
        values,
        decay_gate_logits.T,
        correction_logits.T,
        head_decay_speed,
        position_log_decay.T,
    )
    state = entry_state(trans, inject)
    state, from_left, from_right = lax.optimization_barrier((state, from_left, from_right))
    far = far_shard(from_left, from_right, "tp")
    me = lax.axis_index("tp").astype(jnp.int32).reshape(1)
    parts = parts_for_peers(
        me,
        qt,
        ol,
        state,
        head_output_gain,
        mixer_output_weight,
        group,
        common_gate_weight,
        common_up_weight,
        common_down_weight,
    )
    rows, near = near_experts(arrived, (own, from_left, from_right))
    parts, far, near = lax.optimization_barrier((parts, far, near))
    got = [parts[0]] + [
        lax.ppermute(parts[r], "tp", shift(r)) for r in range(1, peers)
    ]
    slot_sums = far_expert(rows, near, *far)
    back = to_peers(slot_sums)
    return (mixer_sum(got), combine(got, back, mix))


def solution(mesh):
    finer = Mesh(mesh.devices.reshape(8, 4, 2, mesh.shape["tp"]), ("ep_0", "ep_1", "ep_2", "tp"))
    placed = (
        P(EP, "tp"),
        P(EP, "tp"),
        P(EP, "tp"),
        P(EP, "tp"),
        P(EP, "tp"),
        P("tp"),
        P(EP, "tp"),
        P(),
        P("tp", None),
        P(EP_TP, None),
        P(),
        P(EP_TP, None),
        P(EP_TP, None),
        P(EP, None, "tp"),
        P(EP, None, "tp"),
        P(EP, "tp", None),
        P(None, "tp"),
        P(None, "tp"),
        P("tp", None),
    )
    return jax.shard_map(
        shards,
        mesh=finer,
        in_specs=placed,
        out_specs=(P(EP_TP, None), P(EP_TP, None)),
        check_vma=False,
    )
```

```python
import functools

import jax
import jax.numpy as jnp
from jax import lax
from jax.experimental import pallas as pl
from jax.experimental.pallas import tpu as pltpu
from jax.sharding import Mesh
from jax.sharding import PartitionSpec as P


EP = ("ep_0", "ep_1", "ep_2")
EP_TP = ("ep_0", "ep_1", "ep_2", "tp")


EPS = 1e-06
F32 = jnp.float32
BF16 = jnp.bfloat16
LANES = 128
MESH = pl.DeviceIdType.MESH
ALL_VMEM = pltpu.CompilerParams(vmem_limit_bytes=67_043_328)


def halves(x):
    hi = x.astype(BF16)
    return hi, (x - hi.astype(F32)).astype(BF16)


def thirds(x):
    hi = x.astype(BF16)
    rest = x - hi.astype(F32)
    mid = rest.astype(BF16)
    return hi, mid, (rest - mid.astype(F32)).astype(BF16)


def mm(a, b):
    return jnp.dot(a, b, preferred_element_type=F32)


def dot3(a, b):
    ah, al = halves(a)
    bh, bl = halves(b)
    return mm(jnp.concatenate([ah, ah, al], 1), jnp.concatenate([bh, bl, bh], 0))


def dot2(a, b):
    ah, al = halves(a)
    return mm(jnp.concatenate([ah, al], 1), jnp.concatenate([b, b], 0))


def unit_lower_inverses(lows, row, col):
    eye = (row == col).astype(F32)
    near = (row >> 3) == (col >> 3)
    base = [jnp.where(near, low, 0.0) for low in lows]
    squared = [dot3(x, x) for x in base]
    inv = [eye - x for x in base]
    fourth = [dot3(x, x) for x in squared]
    inv = [x + dot3(x, y) for x, y in zip(inv, squared)]
    inv = [x + dot3(x, y) for x, y in zip(inv, fourth)]
    for bit in (3, 4, 5):
        between = ((row >> (bit + 1)) == (col >> (bit + 1))) & ((row >> bit) != (col >> bit))
        right = [dot3(jnp.where(between, low, 0.0), x) for low, x in zip(lows, inv)]
        inv = [x - dot3(x, y) for x, y in zip(inv, right)]
    return inv


def local_mixer_kernel(
    q_ref, k_ref, v_ref, gate_ref, corr_ref, speed_ref, plog_ref, qt_ref, ol_ref, tr_ref, in_ref,
    su_all, pq_all, mw_all, keep_all,
):
    head = pl.program_id(0)
    heads, rows = gate_ref.shape
    pair = 128
    here = lax.broadcasted_iota(jnp.int32, (heads, rows), 0) == head

    log_gate = (
        -speed_ref[...]
        * (jnp.maximum(gate_ref[...], 0.0) + jnp.log1p(jnp.exp(-jnp.abs(gate_ref[...]))))
        + plog_ref[...]
    )
    beta_all = 1.0 / (1.0 + jnp.exp(-corr_ref[...].astype(F32)))
    g_row = jnp.sum(jnp.where(here, log_gate, 0.0), axis=0, keepdims=True)
    beta_row_all = jnp.sum(jnp.where(here, beta_all, 0.0), axis=0, keepdims=True)

    row = lax.broadcasted_iota(jnp.int32, (pair, pair), 0)
    col = lax.broadcasted_iota(jnp.int32, (pair, pair), 1)
    same = (row >> 6) == (col >> 6)
    causal = same & (row >= col)
    strict = same & (row > col)
    first = col < 64
    ones = (same & (row <= col)).astype(BF16)
    ones = jnp.concatenate([ones, ones, ones], 0)

    pairs = range(rows // pair)
    span = [slice(p * pair, (p + 1) * pair) for p in pairs]
    qb, kb, vb = [[ref[at, :] for at in span] for ref in (q_ref, k_ref, v_ref)]
    gram = [
        lax.dot_general(
            jnp.concatenate([k, q], 0), k, (((1,), (1,)), ((), ())), preferred_element_type=F32
        )
        for k, q in zip(kb, qb)
    ]
    c_row = [
        mm(jnp.concatenate(thirds(jnp.broadcast_to(g_row[:, at], (pair, pair))), 1), ones)
        for at in span
    ]
    c_mat = [c.T for c in c_row]
    qf, kf = [x.astype(F32) for x in qb], [x.astype(F32) for x in kb]
    rq = [
        lax.rsqrt(jnp.sum(x * x, axis=1, keepdims=True) + EPS) * (pair**-0.5) for x in qf
    ]
    rk = [lax.rsqrt(jnp.sum(x * x, axis=1, keepdims=True) + EPS) for x in kf]
    rk_row = [jnp.broadcast_to(x, (pair, pair)).T for x in rk]
    beta_row = [jnp.broadcast_to(beta_row_all[:, at], (pair, pair)) for at in span]
    beta = [x.T for x in beta_row]
    decay = [
        jnp.exp(jnp.where(causal, cm - cr, -jnp.inf)) * r for cm, cr, r in zip(c_mat, c_row, rk_row)
    ]
    low = [
        jnp.where(strict, g[:pair] * d * (b * r), 0.0) for g, d, b, r in zip(gram, decay, beta, rk)
    ]
    scores = [g[pair:] * d * r for g, d, r in zip(gram, decay, rq)]
    inv = unit_lower_inverses(low, row, col)
    scale = [b * x for b, x in zip(beta_row, inv)]
    u = [dot2(x, v) for x, v in zip(scale, vb)]
    w = [dot2(x * (jnp.exp(c) * r), k) for x, c, r, k in zip(scale, c_row, rk_row, kb)]
    uw = [jnp.concatenate([x, y], 1) for x, y in zip(u, w)]
    last = [(c[63:64, :], c[127:128, :]) for c in c_mat]
    kt = [
        k.T * (jnp.exp(jnp.where(first, l[0], l[1]) - c) * r)
        for k, l, c, r in zip(kf, last, c_row, rk_row)
    ]
    suw = [dot3(x, y) for x, y in zip(scores, uw)]
    mw = [
        dot3(jnp.concatenate([jnp.where(first, x, 0.0), jnp.where(first, 0.0, x)], 0), y)
        for x, y in zip(kt, uw)
    ]
    pq = [x * (r * jnp.exp(c)) - y[:, pair:] for x, r, c, y in zip(qf, rq, c_mat, suw)]
    for p in pairs:
        su_all[head, p] = suw[p][:, :pair]
        pq_all[head, p] = pq[p]
        mw_all[head, p] = mw[p]
        keep_all[head, p] = jnp.concatenate([jnp.exp(x) for x in last[p]], 0)

    @pl.when(head == heads - 1)
    def _():
        nothing = jnp.zeros((pair, pair), F32)
        ab = [jnp.concatenate([(row == col).astype(F32), nothing], 1) for _ in range(heads)]
        for p in pairs:
            for b in range(2):
                blk = slice(b * 64, (b + 1) * 64)
                at = pl.ds(p * pair + b * 64, 64)
                part = [mw_all[h, p, b * pair : (b + 1) * pair, :] for h in range(heads)]
                got = [
                    dot3(jnp.concatenate([pq_all[h, p, blk, :], part[h][:, pair:]], 0), ab[h])
                    for h in range(heads)
                ]
                for h in range(heads):
                    qt_ref[h, at, :] = got[h][:64, :pair]
                    ol_ref[h, at, :] = got[h][:64, pair:] + su_all[h, p, blk, :]
                    keep = keep_all[h, p, b : b + 1, :]
                    ab[h] = (
                        jnp.concatenate([keep, keep], 1) * ab[h]
                        - got[h][64:]
                        + jnp.concatenate([nothing, part[h][:, :pair]], 1)
                    )
        for h in range(heads):
            tr_ref[h] = ab[h][:, :pair]
            in_ref[h] = ab[h][:, pair:]


def local_mixer(queries, keys, values, gate, corr, speed, plog):
    rows, width = queries.shape
    heads = gate.shape[0]
    d = width // heads
    by_head = pl.BlockSpec((rows, d), lambda h: (0, h))
    whole = pl.BlockSpec((heads, rows), lambda h: (0, 0))
    return pl.pallas_call(
        local_mixer_kernel,
        grid=(heads,),
        in_specs=[
            by_head,
            by_head,
            by_head,
            whole,
            whole,
            pl.BlockSpec((heads, 1), lambda h: (0, 0)),
            whole,
        ],
        out_specs=[
            pl.BlockSpec((heads, rows, d), lambda h: (0, 0, 0)),
            pl.BlockSpec((heads, rows, d), lambda h: (0, 0, 0)),
            pl.BlockSpec((heads, d, d), lambda h: (0, 0, 0)),
            pl.BlockSpec((heads, d, d), lambda h: (0, 0, 0)),
        ],
        scratch_shapes=[
            pltpu.VMEM((heads, rows // 128, 128, d), F32),
            pltpu.VMEM((heads, rows // 128, 128, d), F32),
            pltpu.VMEM((heads, rows // 128, 2 * d, 2 * d), F32),
            pltpu.VMEM((heads, rows // 128, 2, d), F32),
        ],
        out_shape=[
            jax.ShapeDtypeStruct((heads, rows, d), F32),
            jax.ShapeDtypeStruct((heads, rows, d), F32),
            jax.ShapeDtypeStruct((heads, d, d), F32),
            jax.ShapeDtypeStruct((heads, d, d), F32),
        ],
        cost_estimate=pl.CostEstimate(flops=30_000_000_000, bytes_accessed=4_000_000, transcendentals=0),
        compiler_params=ALL_VMEM,
        name="local_mixer",
    )(queries, keys, values, gate, corr, speed.reshape(heads, 1), plog)


def entry_state_kernel(
    t_ref, i_ref, s_ref, own, peer, ypack, zpack,
    send_c, recv_c, send_y, recv_y, send_yc, recv_yc,
    send_r, recv_r, send_l, recv_l, send_rc, recv_rc, send_lc, recv_lc,
):
    heads, d, _ = t_ref.shape
    half = d // 2
    nz, ny = zpack.shape[0], ypack.shape[0]
    z, y, c = lax.axis_index("ep_0"), lax.axis_index("ep_1"), lax.axis_index("ep_2")
    other = {"ep_2": 1 - c}
    right, left = {"ep_0": lax.rem(z + 1, nz)}, {"ep_0": lax.rem(z + nz - 1, nz)}
    across = [{"ep_1": lax.rem(y + k, ny)} for k in range(1, ny)]

    barrier = pltpu.get_barrier_semaphore()
    for who in (other, right, left, *across):
        pl.semaphore_signal(barrier, inc=1, device_id=who, device_id_type=MESH)
    pl.semaphore_wait(barrier, 3 + len(across))

    def send(src, dst, send_sem, recv_sem, who):
        return pltpu.make_async_remote_copy(
            src_ref=src, dst_ref=dst, send_sem=send_sem, recv_sem=recv_sem,
            device_id=who, device_id_type=MESH,
        )

    def store(ref, h, both):
        both = both.astype(BF16)
        ref[0, h] = both[:half]
        ref[1, h] = both[half:]

    def load(ref, h):
        return jnp.concatenate([ref[0, h], ref[1, h]], 0)

    def after(pack, so_far):
        hi, lo = halves(so_far)
        t = pack[:, :d]
        return mm(jnp.concatenate([t, t], 1), jnp.concatenate([hi, lo], 0))

    def added(pack):
        return pack[:, d:].astype(F32)

    nothing = jnp.zeros((d, d), F32)
    for h in range(heads):
        store(own, h, jnp.concatenate([t_ref[h], i_ref[h]], 1))
    swap = send(own, peer, send_c, recv_c, other)
    swap.start()
    swap.wait()
    for h in range(heads):
        mine, theirs = load(own, h), load(peer, h)
        early = jnp.where(c == 0, mine.astype(F32), theirs.astype(F32)).astype(BF16)
        late = jnp.where(c == 0, theirs.astype(F32), mine.astype(F32)).astype(BF16)
        both = mm(late[:, :d], early) + jnp.concatenate([nothing, added(late)], 1)
        store(ypack.at[y], h, both)

    out = [
        send(ypack.at[y, c], ypack.at[y, c], send_y.at[k - 1], recv_y.at[k - 1], across[k - 1])
        for k in range(1, ny)
    ]
    for copy in out:
        copy.start()
    over = []
    for k in range(1, ny):
        slot = ypack.at[lax.rem(y + ny - k, ny), c]
        out[k - 1].wait_recv()
        over.append(send(slot, slot, send_yc.at[k - 1], recv_yc.at[k - 1], other))
        over[-1].start()
    for copy in out:
        copy.wait_send()
    for copy in over:
        copy.wait()
    for h in range(heads):
        both = load(ypack.at[0], h).astype(F32)
        for k in range(1, ny):
            pack = load(ypack.at[k], h)
            both = after(pack, both) + jnp.concatenate([nothing, added(pack)], 1)
        store(zpack.at[z], h, both)

    def going(r, h, sign, who, send_sem, recv_sem):
        slot = zpack.at[lax.rem(z + nz - sign * (r - 1), nz), c, h]
        return send(slot, slot, send_sem.at[r - 1, h], recv_sem.at[r - 1, h], who)

    def shared_with_other(r, h, sign, send_sem, recv_sem):
        slot = zpack.at[lax.rem(z + nz - sign * r, nz), c, h]
        return send(slot, slot, send_sem.at[r - 1, h], recv_sem.at[r - 1, h], other)

    rings = (
        (nz // 2, 1, right, send_r, recv_r, send_rc, recv_rc),
        ((nz - 1) // 2, -1, left, send_l, recv_l, send_lc, recv_lc),
    )
    pending = []
    for rounds, sign, who, ss, rs, _, _ in rings:
        for h in range(heads):
            if rounds > 0:
                going(1, h, sign, who, ss, rs).start()
    for r in range(1, nz // 2 + 1):
        for h in range(heads):
            for rounds, sign, who, ss, rs, sc, rc in rings:
                if r > rounds:
                    continue
                copy = going(r, h, sign, who, ss, rs)
                copy.wait_recv()
                pending.append((copy, False))
                if r < rounds:
                    going(r + 1, h, sign, who, ss, rs).start()
                hand = shared_with_other(r, h, sign, sc, rc)
                hand.start()
                pending.append((hand, True))
    for copy, both_ways in pending:
        copy.wait_send()
        if both_ways:
            copy.wait_recv()

    for h in range(heads):
        s_ref[h] = nothing
    for k in range(nz - 1):
        for h in range(heads):
            pack = load(zpack.at[k], h)
            s_ref[h] = jnp.where(k < z, after(pack, s_ref[h]) + added(pack), s_ref[h])
    for k in range(ny - 1):
        for h in range(heads):
            pack = load(ypack.at[k], h)
            s_ref[h] = jnp.where(k < y, after(pack, s_ref[h]) + added(pack), s_ref[h])
    for h in range(heads):
        pack = load(peer, h)
        s_ref[h] = jnp.where(c == 1, after(pack, s_ref[h]) + added(pack), s_ref[h])


def entry_state(trans, inject):
    heads, d, _ = trans.shape
    nz, ny = lax.axis_size("ep_0"), lax.axis_size("ep_1")
    half = (2, heads, d // 2, 2 * d)
    dma = pltpu.SemaphoreType.DMA
    rounds = max(nz // 2, 1)
    vmem = pl.BlockSpec(memory_space=pltpu.VMEM)
    return pl.pallas_call(
        entry_state_kernel,
        in_specs=[vmem, vmem],
        out_specs=vmem,
        out_shape=jax.ShapeDtypeStruct((heads, d, d), F32),
        scratch_shapes=[
            pltpu.VMEM(half, BF16),
            pltpu.VMEM(half, BF16),
            pltpu.VMEM((ny, *half), BF16),
            pltpu.VMEM((nz, *half), BF16),
            dma, dma,
            dma((max(ny - 1, 1),)), dma((max(ny - 1, 1),)), dma((max(ny - 1, 1),)), dma((max(ny - 1, 1),)),
            *[dma((rounds, heads)) for _ in range(8)],
        ],
        compiler_params=pltpu.CompilerParams(
            collective_id=0, has_side_effects=True, vmem_limit_bytes=67_043_328
        ),
        cost_estimate=pl.CostEstimate(flops=30_000_000_000, bytes_accessed=4_000_000, transcendentals=0),
        name="entry_state",
    )(trans, inject)


def parts_kernel(peers, me_ref, qt_ref, ol_ref, state_ref, gain_ref, w_ref, *refs):
    hbm, refs = refs[: peers + 3], refs[peers + 3 :]
    out_refs, (x, gate, up, down, sems) = refs[:peers], refs[peers:]
    heads, rows, _ = qt_ref.shape
    tile = rows // peers
    spots = [x.at[r * tile : (r + 1) * tile] for r in range(peers)] + [gate, up, down]
    copies = [
        pltpu.make_async_copy(src, dst, sems.at[k]) for k, (src, dst) in enumerate(zip(hbm, spots))
    ]
    for copy in copies:
        copy.start()
    turns = [
        pl.ds(pl.multiple_of(lax.rem(me_ref[0] + r, peers) * tile, tile), tile)
        for r in range(peers)
    ]
    normed = []
    for h in range(heads):
        qt = jnp.concatenate([qt_ref[h, at, :] for at in turns], 0)
        ol = jnp.concatenate([ol_ref[h, at, :] for at in turns], 0)
        out = dot3(qt, state_ref[h]) + ol
        out = out * lax.rsqrt(jnp.mean(out * out, axis=1, keepdims=True) + EPS) * gain_ref[...]
        normed.append(out.astype(BF16))
    mixer = mm(jnp.concatenate(normed, 1), w_ref[...]).astype(BF16)
    for r in range(peers):
        out_refs[r][:tile] = mixer[r * tile : (r + 1) * tile]
    for copy in copies:
        copy.wait()
    hidden = gated(mm(x[...], gate[...]), mm(x[...], up[...]))
    shared = mm(hidden, down[...]).astype(BF16)
    for r in range(peers):
        out_refs[r][tile:] = shared[r * tile : (r + 1) * tile]


def parts_for_peers(me, qt, ol, state, gain, w, tokens, gate, up, down):
    _, rows, d = qt.shape
    width = w.shape[1]
    peers = len(tokens)
    tile = rows // peers
    vmem = pl.BlockSpec(memory_space=pltpu.VMEM)
    kept = (*tokens, gate, up, down)
    return pl.pallas_call(
        functools.partial(parts_kernel, peers),
        in_specs=[pl.BlockSpec(memory_space=pltpu.SMEM)]
        + [vmem] * 5
        + [pl.BlockSpec(memory_space=pl.ANY)] * len(kept),
        out_specs=[vmem] * peers,
        out_shape=[jax.ShapeDtypeStruct((2 * tile, width), BF16)] * peers,
        scratch_shapes=[
            pltpu.VMEM((rows, width), BF16),
            pltpu.VMEM(gate.shape, BF16),
            pltpu.VMEM(up.shape, BF16),
            pltpu.VMEM(down.shape, BF16),
            pltpu.SemaphoreType.DMA((len(kept),)),
        ],
        cost_estimate=pl.CostEstimate(flops=6_000_000_000, bytes_accessed=12_000_000, transcendentals=0),
        compiler_params=ALL_VMEM,
        name="parts_for_peers",
    )(me, qt, ol, state, gain.reshape(1, d), w, *kept)


def near_experts_kernel(in_ref, *refs):
    shards_ = len(refs) // 3 - 2
    hbm, (x_ref, out_ref, gates, ups, downs) = refs[: 3 * shards_], refs[3 * shards_ : -1]
    sems = refs[-1]
    rows, width = x_ref.shape
    cuts = width // LANES
    tile = 128
    copies = [
        [
            pltpu.make_async_copy(hbm[3 * m + k], held.at[m], sems.at[m, k])
            for k, held in enumerate((gates, ups, downs))
        ]
        for m in range(shards_)
    ]
    for shard in copies:
        for copy in shard:
            copy.start()
    for t in range(rows // tile):
        x_ref[t * tile : (t + 1) * tile, :] = gathered(
            in_ref[t * tile * cuts : (t + 1) * tile * cuts, :], cuts
        )
    for m in range(shards_):
        for copy in copies[m]:
            copy.wait()
        x = x_ref[...]
        part = mm(gated(mm(x, gates[m]), mm(x, ups[m])), downs[m])
        out_ref[...] = part if m == 0 else out_ref[...] + part


def near_experts(spread_in, shards_):
    weights = [w for shard in shards_ for w in shard]
    width, hidden = shards_[0][0].shape
    rows = spread_in.shape[0] * LANES // width
    count = len(shards_)
    vmem = pl.BlockSpec(memory_space=pltpu.VMEM)
    return pl.pallas_call(
        near_experts_kernel,
        in_specs=[vmem] + [pl.BlockSpec(memory_space=pl.ANY)] * len(weights),
        out_specs=[vmem, vmem],
        out_shape=[
            jax.ShapeDtypeStruct((rows, width), BF16),
            jax.ShapeDtypeStruct((rows, width), F32),
        ],
        scratch_shapes=[
            pltpu.VMEM((count, width, hidden), BF16),
            pltpu.VMEM((count, width, hidden), BF16),
            pltpu.VMEM((count, hidden, width), BF16),
            pltpu.SemaphoreType.DMA((count, 3)),
        ],
        cost_estimate=pl.CostEstimate(flops=5_000_000_000, bytes_accessed=16_000_000, transcendentals=0),
        compiler_params=ALL_VMEM,
        name="near_experts",
    )(spread_in, *weights)


def far_hidden_kernel(x_ref, gate_ref, up_ref, out_ref):
    x = x_ref[...]
    out_ref[...] = gated(mm(x, gate_ref[...]), mm(x, up_ref[...]))


def far_hidden(x, gate, up):
    vmem = pl.BlockSpec(memory_space=pltpu.VMEM)
    return pl.pallas_call(
        far_hidden_kernel,
        in_specs=[vmem] * 3,
        out_specs=vmem,
        out_shape=jax.ShapeDtypeStruct((x.shape[0], gate.shape[1]), BF16),
        cost_estimate=pl.CostEstimate(flops=1_500_000_000, bytes_accessed=4_000_000, transcendentals=0),
        compiler_params=ALL_VMEM,
        name="far_hidden",
    )(x, gate, up)


def far_out_kernel(hidden_ref, near_ref, down0_ref, down1_ref, out_ref, near, down, ready, sems):
    rows, width = near.shape
    cuts = width // LANES
    half = down.shape[0] // 2
    tile = rows // ready.shape[0]
    spans = [slice(t * tile, (t + 1) * tile) for t in range(ready.shape[0])]
    loads = [
        pltpu.make_async_copy(down0_ref, down.at[:half], sems.at[0]),
        pltpu.make_async_copy(down1_ref, down.at[half:], sems.at[1]),
    ] + [
        pltpu.make_async_copy(near_ref.at[at], near.at[at], sems.at[2 + t])
        for t, at in enumerate(spans)
    ]
    for copy in loads:
        copy.start()
    for copy in loads[:2]:
        copy.wait()
    stores = []
    for t, at in enumerate(spans):
        part = mm(hidden_ref[at, :], down[...])
        loads[2 + t].wait()
        ready[t] = spread(near[at, :] + part)
        stores.append(
            pltpu.make_async_copy(
                ready.at[t],
                out_ref.at[t * tile * cuts : (t + 1) * tile * cuts],
                sems.at[2 + len(spans) + t],
            )
        )
        stores[-1].start()
    for copy in stores:
        copy.wait()


def far_out(hidden, near, down0, down1):
    rows, width = near.shape
    cuts = width // LANES
    tiles = rows // 128
    hbm = pl.BlockSpec(memory_space=pl.ANY)
    return pl.pallas_call(
        far_out_kernel,
        in_specs=[pl.BlockSpec(memory_space=pltpu.VMEM), hbm, hbm, hbm],
        out_specs=hbm,
        out_shape=jax.ShapeDtypeStruct((rows * cuts, LANES), BF16),
        scratch_shapes=[
            pltpu.VMEM((rows, width), F32),
            pltpu.VMEM((2 * down0.shape[0], width), BF16),
            pltpu.VMEM((tiles, 128 * cuts, LANES), BF16),
            pltpu.SemaphoreType.DMA((2 + 2 * tiles,)),
        ],
        cost_estimate=pl.CostEstimate(flops=1_500_000_000, bytes_accessed=8_000_000, transcendentals=0),
        name="far_out",
    )(hidden, near, down0, down1)


def interleaving(cuts, back=False):
    i = lax.broadcasted_iota(jnp.int32, (8 * cuts, 8 * cuts), 1 if back else 0)
    j = lax.broadcasted_iota(jnp.int32, (8 * cuts, 8 * cuts), 0 if back else 1)
    return ((lax.div(i, cuts) == lax.rem(j, 8)) & (lax.rem(i, cuts) == lax.div(j, 8))).astype(BF16)


def spread(values):
    rows, width = values.shape
    cuts = width // LANES
    order = interleaving(cuts)
    blocks = [
        jnp.concatenate(
            [values[g : g + 8, c * LANES : (c + 1) * LANES] for c in range(cuts)], 0
        ).astype(BF16)
        for g in range(0, rows, 8)
    ]
    out = []
    for g in range(0, len(blocks), 2):
        two = mm(order, jnp.concatenate(blocks[g : g + 2], 1)).astype(BF16)
        out += [two[:, :LANES], two[:, LANES:]]
    return jnp.concatenate(out, 0)


def gathered(tall, cuts):
    order = interleaving(cuts, back=True)
    size = 8 * cuts
    blocks = [tall[g : g + size] for g in range(0, tall.shape[0], size)]
    out = []
    for g in range(0, len(blocks), 2):
        two = mm(order, jnp.concatenate(blocks[g : g + 2], 1))
        out += [two[:, :LANES], two[:, LANES:]]
    return jnp.concatenate(
        [jnp.concatenate([x[c * 8 : (c + 1) * 8] for x in out], 0) for c in range(cuts)], 1
    ).astype(BF16)


def dispatch_kernel(capacity, x_ref, gain_ref, routes_ref, weight_ref, xn_ref, out_ref, mix_ref):
    tokens, width = x_ref.shape
    slots = mix_ref.shape[1]
    x = x_ref[...].astype(F32)
    xn = (x * lax.rsqrt(jnp.mean(x * x, axis=1, keepdims=True) + EPS) * gain_ref[...]).astype(BF16)
    xn_ref[...] = xn
    expert = lax.broadcasted_iota(jnp.int32, (LANES, tokens), 0)
    first, second = expert == routes_ref[0:1, :], expert == routes_ref[1:2, :]
    chosen = (first | second).astype(BF16)
    token = lax.broadcasted_iota(jnp.int32, (tokens, tokens), 0)
    later = lax.broadcasted_iota(jnp.int32, (tokens, tokens), 1)
    place = mm(chosen, (token < later).astype(BF16)) + (expert * capacity).astype(F32)
    s0 = jnp.sum(jnp.where(first, place, 0.0), axis=0, keepdims=True)
    s1 = jnp.sum(jnp.where(second, place, 0.0), axis=0, keepdims=True)
    step = 128
    cuts = width // LANES
    for base in range(0, slots, step):
        slot = (lax.broadcasted_iota(jnp.int32, (step, tokens), 0) + base).astype(F32)
        is0, is1 = slot == s0, slot == s1
        out_ref[base * cuts : (base + step) * cuts, :] = spread(mm((is0 | is1).astype(BF16), xn))
        mix = jnp.where(is0, weight_ref[0:1, :], 0.0) + jnp.where(is1, weight_ref[1:2, :], 0.0)
        mix_ref[:, base : base + step] = mix.T


def dispatch(x, gain, routes, weight, slots, capacity):
    tokens, width = x.shape
    cuts = width // LANES
    return pl.pallas_call(
        functools.partial(dispatch_kernel, capacity),
        out_shape=[
            jax.ShapeDtypeStruct((tokens, width), BF16),
            jax.ShapeDtypeStruct((slots * cuts, LANES), BF16),
            jax.ShapeDtypeStruct((tokens, slots), F32),
        ],
        name="dispatch",
    )(x, gain.reshape(1, width), routes, weight)


def sums_kernel(*refs):
    *part_refs, mixer_ref, shared_ref = refs
    tokens = mixer_ref.shape[0]
    mixer, shared = part_refs[0][:tokens].astype(F32), part_refs[0][tokens:].astype(F32)
    for part in part_refs[1:]:
        mixer = mixer + part[:tokens].astype(F32)
        shared = shared + part[tokens:].astype(F32)
    mixer_ref[...] = mixer.astype(BF16)
    shared_ref[...] = shared


def sums_of_parts(parts):
    rows, width = parts[0].shape
    tile = 512
    out = pl.BlockSpec((rows // 2, tile), lambda c: (0, c))
    return pl.pallas_call(
        sums_kernel,
        grid=(width // tile,),
        in_specs=[pl.BlockSpec((rows, tile), lambda c: (0, c))] * len(parts),
        out_specs=[out, out],
        out_shape=[
            jax.ShapeDtypeStruct((rows // 2, width), BF16),
            jax.ShapeDtypeStruct((rows // 2, width), F32),
        ],
        cost_estimate=pl.CostEstimate(flops=1_000_000_000, bytes_accessed=6_000_000, transcendentals=0),
        compiler_params=ALL_VMEM,
        name="sums_of_parts",
    )(*parts)


def combine_kernel(shared_hbm, back_hbm, mix_hbm, out_hbm, shared, back, mix, out, sems):
    tiles = back.shape[0]
    width = shared.shape[1]
    cuts = width // LANES
    tile = back.shape[1] // cuts
    loads = [
        pltpu.make_async_copy(
            back_hbm.at[t * tile * cuts : (t + 1) * tile * cuts], back.at[t], sems.at[t]
        )
        for t in range(tiles)
    ]
    loads.insert(1, pltpu.make_async_copy(mix_hbm, mix, sems.at[tiles]))
    loads.append(pltpu.make_async_copy(shared_hbm, shared, sems.at[tiles + 1]))
    for copy in loads:
        copy.start()
    rows = []
    for t, count in enumerate((2,) + (1,) * (tiles - 1)):
        for _ in range(count):
            loads.pop(0).wait()
        rows.append(gathered(back[t], cuts))
    loads.pop(0).wait()
    rows = jnp.concatenate(rows, 0)
    hi, lo = halves(mix[...])
    both = jnp.concatenate([hi, lo], 1)
    stores = []
    for k in range(2):
        at = slice(k * width // 2, (k + 1) * width // 2)
        part = jnp.concatenate([rows[:, at], rows[:, at]], 0)
        out[:, at] = (shared[:, at] + mm(both, part)).astype(BF16)
        stores.append(pltpu.make_async_copy(out.at[:, at], out_hbm.at[:, at], sems.at[tiles + 2 + k]))
        stores[-1].start()
    for copy in stores:
        copy.wait()


def combine(shared, back, mix):
    tokens, width = shared.shape
    cuts = width // LANES
    tile = 128
    tiles = mix.shape[1] // tile
    hbm = pl.BlockSpec(memory_space=pl.ANY)
    return pl.pallas_call(
        combine_kernel,
        in_specs=[hbm, hbm, hbm],
        out_specs=hbm,
        out_shape=jax.ShapeDtypeStruct((tokens, width), BF16),
        scratch_shapes=[
            pltpu.VMEM((tokens, width), F32),
            pltpu.VMEM((tiles, tile * cuts, LANES), BF16),
            pltpu.VMEM(mix.shape, F32),
            pltpu.VMEM((tokens, width), BF16),
            pltpu.SemaphoreType.DMA((tiles + 4,)),
        ],
        compiler_params=ALL_VMEM,
        name="combine",
    )(shared, back, mix)


def ring(axis):
    peers = lax.axis_size(axis)
    return (
        [(i, (i + 1) % peers) for i in range(peers)],
        [(i, (i - 1) % peers) for i in range(peers)],
    )


def neighbours_shards(shard, axis):
    right, left = ring(axis)
    from_left = [lax.ppermute(w, axis, right) for w in shard]
    from_right = [lax.ppermute(w, axis, left) for w in shard]
    return from_left, from_right


def far_shard(from_left, from_right, axis):
    right, left = ring(axis)
    half = from_left[2].shape[0] // 2
    return (
        lax.ppermute(from_left[0], axis, right),
        lax.ppermute(from_right[1], axis, left),
        lax.ppermute(from_left[2][:half], axis, right),
        lax.ppermute(from_right[2][half:], axis, left),
    )


def gated(gate_val, up_val):
    return (jax.nn.silu(gate_val) * up_val).astype(BF16)


def shards(
    queries,
    keys,
    values,
    decay_gate_logits,
    correction_logits,
    head_decay_speed,
    position_log_decay,
    head_output_gain,
    mixer_output_weight,
    expert_input_tokens,
    expert_norm_gain,
    routes,
    chosen_expert_weight,
    routed_gate_weight,
    routed_up_weight,
    routed_down_weight,
    common_gate_weight,
    common_up_weight,
    common_down_weight,
):
    experts = lax.axis_size(EP)
    tokens, _ = expert_input_tokens.shape
    own = (routed_gate_weight[0], routed_up_weight[0], routed_down_weight[0])
    from_left, from_right = neighbours_shards(own, "tp")

    capacity = 3 * tokens * routes.shape[1] // (2 * experts)
    xn, outgoing, mix = dispatch(
        expert_input_tokens,
        expert_norm_gain,
        routes.T,
        chosen_expert_weight.T,
        experts * capacity,
        capacity,
    )

    def to_peers(x):
        parts = x.reshape(experts, -1, LANES)
        return lax.all_to_all(parts, EP, split_axis=0, concat_axis=0, tiled=True).reshape(-1, LANES)

    peers = lax.axis_size("tp")

    def shift(r):
        return [(i, (i + r) % peers) for i in range(peers)]

    arrived = to_peers(outgoing)
    group = [xn] + [lax.ppermute(xn, "tp", shift(peers - r)) for r in range(1, peers)]

    qt, ol, trans, inject = local_mixer(
        queries,
        keys,
        values,
        decay_gate_logits.T,
        correction_logits.T,
        head_decay_speed,
        position_log_decay.T,
    )
    state = entry_state(trans, inject)
    state, from_left, from_right = lax.optimization_barrier((state, from_left, from_right))
    far = far_shard(from_left, from_right, "tp")
    me = lax.axis_index("tp").astype(jnp.int32).reshape(1)
    parts = parts_for_peers(
        me,
        qt,
        ol,
        state,
        head_output_gain,
        mixer_output_weight,
        group,
        common_gate_weight,
        common_up_weight,
        common_down_weight,
    )
    rows, near = near_experts(arrived, (own, from_left, from_right))
    hidden = far_hidden(rows, *far[:2])
    parts, far, near, hidden = lax.optimization_barrier((parts, far, near, hidden))
    got = [parts[0]] + [
        lax.ppermute(parts[r], "tp", shift(r)) for r in range(1, peers)
    ]
    slot_sums = far_out(hidden, near, *far[2:])
    back = to_peers(slot_sums)
    mixer_out, shared = sums_of_parts(got)
    return (mixer_out, combine(shared, back, mix))


def solution(mesh):
    finer = Mesh(mesh.devices.reshape(8, 4, 2, mesh.shape["tp"]), ("ep_0", "ep_1", "ep_2", "tp"))
    placed = (
        P(EP, "tp"),
        P(EP, "tp"),
        P(EP, "tp"),
        P(EP, "tp"),
        P(EP, "tp"),
        P("tp"),
        P(EP, "tp"),
        P(),
        P("tp", None),
        P(EP_TP, None),
        P(),
        P(EP_TP, None),
        P(EP_TP, None),
        P(EP, None, "tp"),
        P(EP, None, "tp"),
        P(EP, "tp", None),
        P(None, "tp"),
        P(None, "tp"),
        P("tp", None),
    )
    return jax.shard_map(
        shards,
        mesh=finer,
        in_specs=placed,
        out_specs=(P(EP_TP, None), P(EP_TP, None)),
        check_vma=False,
    )
```

```python
import functools

import jax
import jax.numpy as jnp
from jax import lax
from jax.experimental import pallas as pl
from jax.experimental.pallas import tpu as pltpu
from jax.sharding import Mesh
from jax.sharding import PartitionSpec as P


EP = ("ep_0", "ep_1", "ep_2")
EP_TP = ("ep_0", "ep_1", "ep_2", "tp")


EPS = 1e-06
F32 = jnp.float32
BF16 = jnp.bfloat16
LANES = 128
MESH = pl.DeviceIdType.MESH
ALL_VMEM = pltpu.CompilerParams(vmem_limit_bytes=67_043_328)


def halves(x):
    hi = x.astype(BF16)
    return hi, (x - hi.astype(F32)).astype(BF16)


def thirds(x):
    hi = x.astype(BF16)
    rest = x - hi.astype(F32)
    mid = rest.astype(BF16)
    return hi, mid, (rest - mid.astype(F32)).astype(BF16)


def mm(a, b):
    return jnp.dot(a, b, preferred_element_type=F32)


def dot3(a, b):
    ah, al = halves(a)
    bh, bl = halves(b)
    return mm(jnp.concatenate([ah, ah, al], 1), jnp.concatenate([bh, bl, bh], 0))


def dot2(a, b):
    ah, al = halves(a)
    return mm(jnp.concatenate([ah, al], 1), jnp.concatenate([b, b], 0))


def unit_lower_inverses(lows, row, col):
    eye = (row == col).astype(F32)
    near = (row >> 3) == (col >> 3)
    base = [jnp.where(near, low, 0.0) for low in lows]
    squared = [dot3(x, x) for x in base]
    inv = [eye - x for x in base]
    fourth = [dot3(x, x) for x in squared]
    inv = [x + dot3(x, y) for x, y in zip(inv, squared)]
    inv = [x + dot3(x, y) for x, y in zip(inv, fourth)]
    for bit in (3, 4, 5):
        between = ((row >> (bit + 1)) == (col >> (bit + 1))) & ((row >> bit) != (col >> bit))
        right = [dot3(jnp.where(between, low, 0.0), x) for low, x in zip(lows, inv)]
        inv = [x - dot3(x, y) for x, y in zip(inv, right)]
    return inv


def local_mixer_kernel(
    q_ref, k_ref, v_ref, gate_ref, corr_ref, speed_ref, plog_ref, qt_ref, ol_ref, tr_ref, in_ref,
    su_all, pq_all, mw_all, keep_all,
):
    head = pl.program_id(0)
    heads, rows = gate_ref.shape
    pair = 128
    here = lax.broadcasted_iota(jnp.int32, (heads, rows), 0) == head

    log_gate = (
        -speed_ref[...]
        * (jnp.maximum(gate_ref[...], 0.0) + jnp.log1p(jnp.exp(-jnp.abs(gate_ref[...]))))
        + plog_ref[...]
    )
    beta_all = 1.0 / (1.0 + jnp.exp(-corr_ref[...].astype(F32)))
    g_row = jnp.sum(jnp.where(here, log_gate, 0.0), axis=0, keepdims=True)
    beta_row_all = jnp.sum(jnp.where(here, beta_all, 0.0), axis=0, keepdims=True)

    row = lax.broadcasted_iota(jnp.int32, (pair, pair), 0)
    col = lax.broadcasted_iota(jnp.int32, (pair, pair), 1)
    same = (row >> 6) == (col >> 6)
    causal = same & (row >= col)
    strict = same & (row > col)
    first = col < 64
    ones = (same & (row <= col)).astype(BF16)
    ones = jnp.concatenate([ones, ones, ones], 0)

    pairs = range(rows // pair)
    span = [slice(p * pair, (p + 1) * pair) for p in pairs]
    qb, kb, vb = [[ref[at, :] for at in span] for ref in (q_ref, k_ref, v_ref)]
    gram = [
        lax.dot_general(
            jnp.concatenate([k, q], 0), k, (((1,), (1,)), ((), ())), preferred_element_type=F32
        )
        for k, q in zip(kb, qb)
    ]
    c_row = [
        mm(jnp.concatenate(thirds(jnp.broadcast_to(g_row[:, at], (pair, pair))), 1), ones)
        for at in span
    ]
    c_mat = [c.T for c in c_row]
    qf, kf = [x.astype(F32) for x in qb], [x.astype(F32) for x in kb]
    rq = [
        lax.rsqrt(jnp.sum(x * x, axis=1, keepdims=True) + EPS) * (pair**-0.5) for x in qf
    ]
    rk = [lax.rsqrt(jnp.sum(x * x, axis=1, keepdims=True) + EPS) for x in kf]
    rk_row = [jnp.broadcast_to(x, (pair, pair)).T for x in rk]
    beta_row = [jnp.broadcast_to(beta_row_all[:, at], (pair, pair)) for at in span]
    beta = [x.T for x in beta_row]
    decay = [
        jnp.exp(jnp.where(causal, cm - cr, -jnp.inf)) * r for cm, cr, r in zip(c_mat, c_row, rk_row)
    ]
    low = [
        jnp.where(strict, g[:pair] * d * (b * r), 0.0) for g, d, b, r in zip(gram, decay, beta, rk)
    ]
    scores = [g[pair:] * d * r for g, d, r in zip(gram, decay, rq)]
    inv = unit_lower_inverses(low, row, col)
    scale = [b * x for b, x in zip(beta_row, inv)]
    u = [dot2(x, v) for x, v in zip(scale, vb)]
    w = [dot2(x * (jnp.exp(c) * r), k) for x, c, r, k in zip(scale, c_row, rk_row, kb)]
    uw = [jnp.concatenate([x, y], 1) for x, y in zip(u, w)]
    last = [(c[63:64, :], c[127:128, :]) for c in c_mat]
    kt = [
        k.T * (jnp.exp(jnp.where(first, l[0], l[1]) - c) * r)
        for k, l, c, r in zip(kf, last, c_row, rk_row)
    ]
    suw = [dot3(x, y) for x, y in zip(scores, uw)]
    mw = [
        dot3(jnp.concatenate([jnp.where(first, x, 0.0), jnp.where(first, 0.0, x)], 0), y)
        for x, y in zip(kt, uw)
    ]
    pq = [x * (r * jnp.exp(c)) - y[:, pair:] for x, r, c, y in zip(qf, rq, c_mat, suw)]
    for p in pairs:
        su_all[head, p] = suw[p][:, :pair]
        pq_all[head, p] = pq[p]
        mw_all[head, p] = mw[p]
        keep_all[head, p] = jnp.concatenate([jnp.exp(x) for x in last[p]], 0)

    @pl.when(head == heads - 1)
    def _():
        nothing = jnp.zeros((pair, pair), F32)
        ab = [jnp.concatenate([(row == col).astype(F32), nothing], 1) for _ in range(heads)]
        for p in pairs:
            for b in range(2):
                blk = slice(b * 64, (b + 1) * 64)
                at = pl.ds(p * pair + b * 64, 64)
                part = [mw_all[h, p, b * pair : (b + 1) * pair, :] for h in range(heads)]
                got = [
                    dot3(jnp.concatenate([pq_all[h, p, blk, :], part[h][:, pair:]], 0), ab[h])
                    for h in range(heads)
                ]
                for h in range(heads):
                    qt_ref[h, at, :] = got[h][:64, :pair]
                    ol_ref[h, at, :] = got[h][:64, pair:] + su_all[h, p, blk, :]
                    keep = keep_all[h, p, b : b + 1, :]
                    ab[h] = (
                        jnp.concatenate([keep, keep], 1) * ab[h]
                        - got[h][64:]
                        + jnp.concatenate([nothing, part[h][:, :pair]], 1)
                    )
        for h in range(heads):
            tr_ref[h] = ab[h][:, :pair]
            in_ref[h] = ab[h][:, pair:]


def local_mixer(queries, keys, values, gate, corr, speed, plog):
    rows, width = queries.shape
    heads = gate.shape[0]
    d = width // heads
    by_head = pl.BlockSpec((rows, d), lambda h: (0, h))
    whole = pl.BlockSpec((heads, rows), lambda h: (0, 0))
    return pl.pallas_call(
        local_mixer_kernel,
        grid=(heads,),
        in_specs=[
            by_head,
            by_head,
            by_head,
            whole,
            whole,
            pl.BlockSpec((heads, 1), lambda h: (0, 0)),
            whole,
        ],
        out_specs=[
            pl.BlockSpec((heads, rows, d), lambda h: (0, 0, 0)),
            pl.BlockSpec((heads, rows, d), lambda h: (0, 0, 0)),
            pl.BlockSpec((heads, d, d), lambda h: (0, 0, 0)),
            pl.BlockSpec((heads, d, d), lambda h: (0, 0, 0)),
        ],
        scratch_shapes=[
            pltpu.VMEM((heads, rows // 128, 128, d), F32),
            pltpu.VMEM((heads, rows // 128, 128, d), F32),
            pltpu.VMEM((heads, rows // 128, 2 * d, 2 * d), F32),
            pltpu.VMEM((heads, rows // 128, 2, d), F32),
        ],
        out_shape=[
            jax.ShapeDtypeStruct((heads, rows, d), F32),
            jax.ShapeDtypeStruct((heads, rows, d), F32),
            jax.ShapeDtypeStruct((heads, d, d), F32),
            jax.ShapeDtypeStruct((heads, d, d), F32),
        ],
        cost_estimate=pl.CostEstimate(flops=30_000_000_000, bytes_accessed=4_000_000, transcendentals=0),
        compiler_params=ALL_VMEM,
        name="local_mixer",
    )(queries, keys, values, gate, corr, speed.reshape(heads, 1), plog)


def entry_state_kernel(
    t_ref, i_ref, s_ref, own, peer, ypack, zpack,
    send_c, recv_c, send_y, recv_y, send_yc, recv_yc,
    send_r, recv_r, send_l, recv_l, send_rc, recv_rc, send_lc, recv_lc,
):
    heads, d, _ = t_ref.shape
    half = d // 2
    nz, ny = zpack.shape[0], ypack.shape[0]
    z, y, c = lax.axis_index("ep_0"), lax.axis_index("ep_1"), lax.axis_index("ep_2")
    other = {"ep_2": 1 - c}
    right, left = {"ep_0": lax.rem(z + 1, nz)}, {"ep_0": lax.rem(z + nz - 1, nz)}
    across = [{"ep_1": lax.rem(y + k, ny)} for k in range(1, ny)]

    barrier = pltpu.get_barrier_semaphore()
    for who in (other, right, left, *across):
        pl.semaphore_signal(barrier, inc=1, device_id=who, device_id_type=MESH)
    pl.semaphore_wait(barrier, 3 + len(across))

    def send(src, dst, send_sem, recv_sem, who):
        return pltpu.make_async_remote_copy(
            src_ref=src, dst_ref=dst, send_sem=send_sem, recv_sem=recv_sem,
            device_id=who, device_id_type=MESH,
        )

    def store(ref, h, both):
        both = both.astype(BF16)
        ref[0, h] = both[:half]
        ref[1, h] = both[half:]

    def load(ref, h):
        return jnp.concatenate([ref[0, h], ref[1, h]], 0)

    def after(pack, so_far):
        hi, lo = halves(so_far)
        t = pack[:, :d]
        return mm(jnp.concatenate([t, t], 1), jnp.concatenate([hi, lo], 0))

    def added(pack):
        return pack[:, d:].astype(F32)

    nothing = jnp.zeros((d, d), F32)
    for h in range(heads):
        store(own, h, jnp.concatenate([t_ref[h], i_ref[h]], 1))
    swap = send(own, peer, send_c, recv_c, other)
    swap.start()
    swap.wait()
    for h in range(heads):
        mine, theirs = load(own, h), load(peer, h)
        early = jnp.where(c == 0, mine.astype(F32), theirs.astype(F32)).astype(BF16)
        late = jnp.where(c == 0, theirs.astype(F32), mine.astype(F32)).astype(BF16)
        both = mm(late[:, :d], early) + jnp.concatenate([nothing, added(late)], 1)
        store(ypack.at[y], h, both)

    out = [
        send(ypack.at[y, c], ypack.at[y, c], send_y.at[k - 1], recv_y.at[k - 1], across[k - 1])
        for k in range(1, ny)
    ]
    for copy in out:
        copy.start()
    over = []
    for k in range(1, ny):
        slot = ypack.at[lax.rem(y + ny - k, ny), c]
        out[k - 1].wait_recv()
        over.append(send(slot, slot, send_yc.at[k - 1], recv_yc.at[k - 1], other))
        over[-1].start()
    for copy in out:
        copy.wait_send()
    for copy in over:
        copy.wait()
    for h in range(heads):
        both = load(ypack.at[0], h).astype(F32)
        for k in range(1, ny):
            pack = load(ypack.at[k], h)
            both = after(pack, both) + jnp.concatenate([nothing, added(pack)], 1)
        store(zpack.at[z], h, both)

    def going(r, h, sign, who, send_sem, recv_sem):
        slot = zpack.at[lax.rem(z + nz - sign * (r - 1), nz), c, h]
        return send(slot, slot, send_sem.at[r - 1, h], recv_sem.at[r - 1, h], who)

    def shared_with_other(r, h, sign, send_sem, recv_sem):
        slot = zpack.at[lax.rem(z + nz - sign * r, nz), c, h]
        return send(slot, slot, send_sem.at[r - 1, h], recv_sem.at[r - 1, h], other)

    rings = (
        (nz // 2, 1, right, send_r, recv_r, send_rc, recv_rc),
        ((nz - 1) // 2, -1, left, send_l, recv_l, send_lc, recv_lc),
    )
    pending = []
    for rounds, sign, who, ss, rs, _, _ in rings:
        for h in range(heads):
            if rounds > 0:
                going(1, h, sign, who, ss, rs).start()
    for r in range(1, nz // 2 + 1):
        for h in range(heads):
            for rounds, sign, who, ss, rs, sc, rc in rings:
                if r > rounds:
                    continue
                copy = going(r, h, sign, who, ss, rs)
                copy.wait_recv()
                pending.append((copy, False))
                if r < rounds:
                    going(r + 1, h, sign, who, ss, rs).start()
                hand = shared_with_other(r, h, sign, sc, rc)
                hand.start()
                pending.append((hand, True))
    for copy, both_ways in pending:
        copy.wait_send()
        if both_ways:
            copy.wait_recv()

    for h in range(heads):
        s_ref[h] = nothing
    for k in range(nz - 1):
        for h in range(heads):
            pack = load(zpack.at[k], h)
            s_ref[h] = jnp.where(k < z, after(pack, s_ref[h]) + added(pack), s_ref[h])
    for k in range(ny - 1):
        for h in range(heads):
            pack = load(ypack.at[k], h)
            s_ref[h] = jnp.where(k < y, after(pack, s_ref[h]) + added(pack), s_ref[h])
    for h in range(heads):
        pack = load(peer, h)
        s_ref[h] = jnp.where(c == 1, after(pack, s_ref[h]) + added(pack), s_ref[h])


def entry_state(trans, inject):
    heads, d, _ = trans.shape
    nz, ny = lax.axis_size("ep_0"), lax.axis_size("ep_1")
    half = (2, heads, d // 2, 2 * d)
    dma = pltpu.SemaphoreType.DMA
    rounds = max(nz // 2, 1)
    vmem = pl.BlockSpec(memory_space=pltpu.VMEM)
    return pl.pallas_call(
        entry_state_kernel,
        in_specs=[vmem, vmem],
        out_specs=vmem,
        out_shape=jax.ShapeDtypeStruct((heads, d, d), F32),
        scratch_shapes=[
            pltpu.VMEM(half, BF16),
            pltpu.VMEM(half, BF16),
            pltpu.VMEM((ny, *half), BF16),
            pltpu.VMEM((nz, *half), BF16),
            dma, dma,
            dma((max(ny - 1, 1),)), dma((max(ny - 1, 1),)), dma((max(ny - 1, 1),)), dma((max(ny - 1, 1),)),
            *[dma((rounds, heads)) for _ in range(8)],
        ],
        compiler_params=pltpu.CompilerParams(
            collective_id=0, has_side_effects=True, vmem_limit_bytes=67_043_328
        ),
        cost_estimate=pl.CostEstimate(flops=30_000_000_000, bytes_accessed=4_000_000, transcendentals=0),
        name="entry_state",
    )(trans, inject)


def parts_kernel(peers, me_ref, qt_ref, ol_ref, state_ref, gain_ref, w_ref, *refs):
    far = peers // 2
    near = [r for r in range(peers) if r != far]
    count = len(near)
    hbm, refs = refs[: count + 3], refs[count + 3 :]
    out_refs, (x, gate, up, down, sems) = refs[:peers], refs[peers:]
    heads, rows, _ = qt_ref.shape
    tile = rows // peers
    spots = [x.at[r * tile : (r + 1) * tile] for r in range(count)] + [gate, up, down]
    copies = [
        pltpu.make_async_copy(src, dst, sems.at[k]) for k, (src, dst) in enumerate(zip(hbm, spots))
    ]
    for copy in copies:
        copy.start()
    turns = [
        pl.ds(pl.multiple_of(lax.rem(me_ref[0] + r, peers) * tile, tile), tile)
        for r in range(peers)
    ]
    normed = []
    for h in range(heads):
        qt = jnp.concatenate([qt_ref[h, at, :] for at in turns], 0)
        ol = jnp.concatenate([ol_ref[h, at, :] for at in turns], 0)
        out = dot3(qt, state_ref[h]) + ol
        out = out * lax.rsqrt(jnp.mean(out * out, axis=1, keepdims=True) + EPS) * gain_ref[...]
        normed.append(out.astype(BF16))
    mixer = mm(jnp.concatenate(normed, 1), w_ref[...]).astype(BF16)
    for r in range(peers):
        out_refs[r][:tile] = mixer[r * tile : (r + 1) * tile]
    for copy in copies:
        copy.wait()
    hidden = gated(mm(x[...], gate[...]), mm(x[...], up[...]))
    shared = mm(hidden, down[...]).astype(BF16)
    for k, r in enumerate(near):
        out_refs[r][tile:] = shared[k * tile : (k + 1) * tile]


def parts_for_peers(me, qt, ol, state, gain, w, tokens, gate, up, down):
    _, rows, d = qt.shape
    width = w.shape[1]
    peers = len(tokens) + 1
    tile = rows // peers
    vmem = pl.BlockSpec(memory_space=pltpu.VMEM)
    kept = (*tokens, gate, up, down)
    return pl.pallas_call(
        functools.partial(parts_kernel, peers),
        in_specs=[pl.BlockSpec(memory_space=pltpu.SMEM)]
        + [vmem] * 5
        + [pl.BlockSpec(memory_space=pl.ANY)] * len(kept),
        out_specs=[vmem] * peers,
        out_shape=[
            jax.ShapeDtypeStruct((tile if r == peers // 2 else 2 * tile, width), BF16)
            for r in range(peers)
        ],
        scratch_shapes=[
            pltpu.VMEM((len(tokens) * tile, width), BF16),
            pltpu.VMEM(gate.shape, BF16),
            pltpu.VMEM(up.shape, BF16),
            pltpu.VMEM(down.shape, BF16),
            pltpu.SemaphoreType.DMA((len(kept),)),
        ],
        cost_estimate=pl.CostEstimate(flops=6_000_000_000, bytes_accessed=12_000_000, transcendentals=0),
        compiler_params=ALL_VMEM,
        name="parts_for_peers",
    )(me, qt, ol, state, gain.reshape(1, d), w, *kept)


def shared_part_kernel(x_ref, gate_ref, up_ref, down_hbm, out_ref, down, sem):
    load = pltpu.make_async_copy(down_hbm, down, sem)
    load.start()
    x = x_ref[...]
    hidden = gated(mm(x, gate_ref[...]), mm(x, up_ref[...]))
    load.wait()
    out_ref[...] = mm(hidden, down[...]).astype(BF16)


def shared_part(x, gate, up, down):
    vmem = pl.BlockSpec(memory_space=pltpu.VMEM)
    return pl.pallas_call(
        shared_part_kernel,
        in_specs=[vmem] * 3 + [pl.BlockSpec(memory_space=pl.ANY)],
        out_specs=vmem,
        out_shape=jax.ShapeDtypeStruct((x.shape[0], down.shape[1]), BF16),
        scratch_shapes=[pltpu.VMEM(down.shape, BF16), pltpu.SemaphoreType.DMA],
        cost_estimate=pl.CostEstimate(flops=1_000_000_000, bytes_accessed=4_000_000, transcendentals=0),
        compiler_params=ALL_VMEM,
        name="shared_part",
    )(x, gate, up, down)


def near_experts_kernel(in_ref, *refs):
    shards_ = len(refs) // 3 - 2
    hbm, (x_ref, out_ref, gates, ups, downs) = refs[: 3 * shards_], refs[3 * shards_ : -1]
    sems = refs[-1]
    rows, width = x_ref.shape
    cuts = width // LANES
    tile = 128
    copies = [
        [
            pltpu.make_async_copy(hbm[3 * m + k], held.at[m], sems.at[m, k])
            for k, held in enumerate((gates, ups, downs))
        ]
        for m in range(shards_)
    ]
    for shard in copies:
        for copy in shard:
            copy.start()
    for t in range(rows // tile):
        x_ref[t * tile : (t + 1) * tile, :] = gathered(
            in_ref[t * tile * cuts : (t + 1) * tile * cuts, :], cuts
        )
    for m in range(shards_):
        for copy in copies[m]:
            copy.wait()
        x = x_ref[...]
        part = mm(gated(mm(x, gates[m]), mm(x, ups[m])), downs[m])
        out_ref[...] = part if m == 0 else out_ref[...] + part


def near_experts(spread_in, shards_):
    weights = [w for shard in shards_ for w in shard]
    width, hidden = shards_[0][0].shape
    rows = spread_in.shape[0] * LANES // width
    count = len(shards_)
    vmem = pl.BlockSpec(memory_space=pltpu.VMEM)
    return pl.pallas_call(
        near_experts_kernel,
        in_specs=[vmem] + [pl.BlockSpec(memory_space=pl.ANY)] * len(weights),
        out_specs=[vmem, vmem],
        out_shape=[
            jax.ShapeDtypeStruct((rows, width), BF16),
            jax.ShapeDtypeStruct((rows, width), F32),
        ],
        scratch_shapes=[
            pltpu.VMEM((count, width, hidden), BF16),
            pltpu.VMEM((count, width, hidden), BF16),
            pltpu.VMEM((count, hidden, width), BF16),
            pltpu.SemaphoreType.DMA((count, 3)),
        ],
        cost_estimate=pl.CostEstimate(flops=5_000_000_000, bytes_accessed=16_000_000, transcendentals=0),
        compiler_params=ALL_VMEM,
        name="near_experts",
    )(spread_in, *weights)


def far_hidden_kernel(x_ref, gate_ref, up_ref, out_ref):
    x = x_ref[...]
    out_ref[...] = gated(mm(x, gate_ref[...]), mm(x, up_ref[...]))


def far_hidden(x, gate, up):
    vmem = pl.BlockSpec(memory_space=pltpu.VMEM)
    return pl.pallas_call(
        far_hidden_kernel,
        in_specs=[vmem] * 3,
        out_specs=vmem,
        out_shape=jax.ShapeDtypeStruct((x.shape[0], gate.shape[1]), BF16),
        cost_estimate=pl.CostEstimate(flops=1_500_000_000, bytes_accessed=4_000_000, transcendentals=0),
        compiler_params=ALL_VMEM,
        name="far_hidden",
    )(x, gate, up)


def far_out_kernel(hidden_ref, near_ref, down0_ref, down1_ref, out_ref, near, down, ready, sems):
    rows, width = near.shape
    cuts = width // LANES
    half = down.shape[0] // 2
    tile = rows // ready.shape[0]
    spans = [slice(t * tile, (t + 1) * tile) for t in range(ready.shape[0])]
    loads = [
        pltpu.make_async_copy(down0_ref, down.at[:half], sems.at[0]),
        pltpu.make_async_copy(down1_ref, down.at[half:], sems.at[1]),
    ] + [
        pltpu.make_async_copy(near_ref.at[at], near.at[at], sems.at[2 + t])
        for t, at in enumerate(spans)
    ]
    for copy in loads:
        copy.start()
    for copy in loads[:2]:
        copy.wait()
    stores = []
    for t, at in enumerate(spans):
        part = mm(hidden_ref[at, :], down[...])
        loads[2 + t].wait()
        ready[t] = spread(near[at, :] + part)
        stores.append(
            pltpu.make_async_copy(
                ready.at[t],
                out_ref.at[t * tile * cuts : (t + 1) * tile * cuts],
                sems.at[2 + len(spans) + t],
            )
        )
        stores[-1].start()
    for copy in stores:
        copy.wait()


def far_out(hidden, near, down0, down1):
    rows, width = near.shape
    cuts = width // LANES
    tiles = rows // 128
    hbm = pl.BlockSpec(memory_space=pl.ANY)
    return pl.pallas_call(
        far_out_kernel,
        in_specs=[pl.BlockSpec(memory_space=pltpu.VMEM), hbm, hbm, hbm],
        out_specs=hbm,
        out_shape=jax.ShapeDtypeStruct((rows * cuts, LANES), BF16),
        scratch_shapes=[
            pltpu.VMEM((rows, width), F32),
            pltpu.VMEM((2 * down0.shape[0], width), BF16),
            pltpu.VMEM((tiles, 128 * cuts, LANES), BF16),
            pltpu.SemaphoreType.DMA((2 + 2 * tiles,)),
        ],
        cost_estimate=pl.CostEstimate(flops=1_500_000_000, bytes_accessed=8_000_000, transcendentals=0),
        name="far_out",
    )(hidden, near, down0, down1)


def interleaving(cuts, back=False):
    i = lax.broadcasted_iota(jnp.int32, (8 * cuts, 8 * cuts), 1 if back else 0)
    j = lax.broadcasted_iota(jnp.int32, (8 * cuts, 8 * cuts), 0 if back else 1)
    return ((lax.div(i, cuts) == lax.rem(j, 8)) & (lax.rem(i, cuts) == lax.div(j, 8))).astype(BF16)


def spread(values):
    rows, width = values.shape
    cuts = width // LANES
    order = interleaving(cuts)
    blocks = [
        jnp.concatenate(
            [values[g : g + 8, c * LANES : (c + 1) * LANES] for c in range(cuts)], 0
        ).astype(BF16)
        for g in range(0, rows, 8)
    ]
    out = []
    for g in range(0, len(blocks), 2):
        two = mm(order, jnp.concatenate(blocks[g : g + 2], 1)).astype(BF16)
        out += [two[:, :LANES], two[:, LANES:]]
    return jnp.concatenate(out, 0)


def gathered(tall, cuts):
    order = interleaving(cuts, back=True)
    size = 8 * cuts
    blocks = [tall[g : g + size] for g in range(0, tall.shape[0], size)]
    out = []
    for g in range(0, len(blocks), 2):
        two = mm(order, jnp.concatenate(blocks[g : g + 2], 1))
        out += [two[:, :LANES], two[:, LANES:]]
    return jnp.concatenate(
        [jnp.concatenate([x[c * 8 : (c + 1) * 8] for x in out], 0) for c in range(cuts)], 1
    ).astype(BF16)


def dispatch_kernel(capacity, x_ref, gain_ref, routes_ref, weight_ref, xn_ref, out_ref, mix_ref):
    tokens, width = x_ref.shape
    slots = mix_ref.shape[1]
    x = x_ref[...].astype(F32)
    xn = (x * lax.rsqrt(jnp.mean(x * x, axis=1, keepdims=True) + EPS) * gain_ref[...]).astype(BF16)
    xn_ref[...] = xn
    expert = lax.broadcasted_iota(jnp.int32, (LANES, tokens), 0)
    first, second = expert == routes_ref[0:1, :], expert == routes_ref[1:2, :]
    chosen = (first | second).astype(BF16)
    token = lax.broadcasted_iota(jnp.int32, (tokens, tokens), 0)
    later = lax.broadcasted_iota(jnp.int32, (tokens, tokens), 1)
    place = mm(chosen, (token < later).astype(BF16)) + (expert * capacity).astype(F32)
    s0 = jnp.sum(jnp.where(first, place, 0.0), axis=0, keepdims=True)
    s1 = jnp.sum(jnp.where(second, place, 0.0), axis=0, keepdims=True)
    step = 128
    cuts = width // LANES
    for base in range(0, slots, step):
        slot = (lax.broadcasted_iota(jnp.int32, (step, tokens), 0) + base).astype(F32)
        is0, is1 = slot == s0, slot == s1
        out_ref[base * cuts : (base + step) * cuts, :] = spread(mm((is0 | is1).astype(BF16), xn))
        mix = jnp.where(is0, weight_ref[0:1, :], 0.0) + jnp.where(is1, weight_ref[1:2, :], 0.0)
        mix_ref[:, base : base + step] = mix.T


def dispatch(x, gain, routes, weight, slots, capacity):
    tokens, width = x.shape
    cuts = width // LANES
    return pl.pallas_call(
        functools.partial(dispatch_kernel, capacity),
        out_shape=[
            jax.ShapeDtypeStruct((tokens, width), BF16),
            jax.ShapeDtypeStruct((slots * cuts, LANES), BF16),
            jax.ShapeDtypeStruct((tokens, slots), F32),
        ],
        name="dispatch",
    )(x, gain.reshape(1, width), routes, weight)


def sums_kernel(*refs):
    *part_refs, far_mixer_ref, far_shared_ref, mixer_ref, shared_ref = refs
    tokens = mixer_ref.shape[0]
    mixer, shared = far_mixer_ref[...].astype(F32), far_shared_ref[...].astype(F32)
    for part in part_refs:
        mixer = mixer + part[:tokens].astype(F32)
        shared = shared + part[tokens:].astype(F32)
    mixer_ref[...] = mixer.astype(BF16)
    shared_ref[...] = shared


def sums_of_parts(parts, far_mixer, far_shared):
    tokens, width = far_mixer.shape
    tile = 512
    out = pl.BlockSpec((tokens, tile), lambda c: (0, c))
    return pl.pallas_call(
        sums_kernel,
        grid=(width // tile,),
        in_specs=[pl.BlockSpec((2 * tokens, tile), lambda c: (0, c))] * len(parts) + [out, out],
        out_specs=[out, out],
        out_shape=[
            jax.ShapeDtypeStruct((tokens, width), BF16),
            jax.ShapeDtypeStruct((tokens, width), F32),
        ],
        cost_estimate=pl.CostEstimate(flops=1_000_000_000, bytes_accessed=6_000_000, transcendentals=0),
        compiler_params=ALL_VMEM,
        name="sums_of_parts",
    )(*parts, far_mixer, far_shared)


def combine_kernel(shared_hbm, back_hbm, mix_hbm, out_hbm, shared, back, mix, out, sems):
    tiles = back.shape[0]
    width = shared.shape[1]
    cuts = width // LANES
    tile = back.shape[1] // cuts
    loads = [
        pltpu.make_async_copy(
            back_hbm.at[t * tile * cuts : (t + 1) * tile * cuts], back.at[t], sems.at[t]
        )
        for t in range(tiles)
    ]
    loads.insert(1, pltpu.make_async_copy(mix_hbm, mix, sems.at[tiles]))
    loads.append(pltpu.make_async_copy(shared_hbm, shared, sems.at[tiles + 1]))
    for copy in loads:
        copy.start()
    rows = []
    for t, count in enumerate((2,) + (1,) * (tiles - 1)):
        for _ in range(count):
            loads.pop(0).wait()
        rows.append(gathered(back[t], cuts))
    loads.pop(0).wait()
    rows = jnp.concatenate(rows, 0)
    hi, lo = halves(mix[...])
    both = jnp.concatenate([hi, lo], 1)
    stores = []
    for k in range(2):
        at = slice(k * width // 2, (k + 1) * width // 2)
        part = jnp.concatenate([rows[:, at], rows[:, at]], 0)
        out[:, at] = (shared[:, at] + mm(both, part)).astype(BF16)
        stores.append(pltpu.make_async_copy(out.at[:, at], out_hbm.at[:, at], sems.at[tiles + 2 + k]))
        stores[-1].start()
    for copy in stores:
        copy.wait()


def combine(shared, back, mix):
    tokens, width = shared.shape
    cuts = width // LANES
    tile = 128
    tiles = mix.shape[1] // tile
    hbm = pl.BlockSpec(memory_space=pl.ANY)
    return pl.pallas_call(
        combine_kernel,
        in_specs=[hbm, hbm, hbm],
        out_specs=hbm,
        out_shape=jax.ShapeDtypeStruct((tokens, width), BF16),
        scratch_shapes=[
            pltpu.VMEM((tokens, width), F32),
            pltpu.VMEM((tiles, tile * cuts, LANES), BF16),
            pltpu.VMEM(mix.shape, F32),
            pltpu.VMEM((tokens, width), BF16),
            pltpu.SemaphoreType.DMA((tiles + 4,)),
        ],
        compiler_params=ALL_VMEM,
        name="combine",
    )(shared, back, mix)


def ring(axis):
    peers = lax.axis_size(axis)
    return (
        [(i, (i + 1) % peers) for i in range(peers)],
        [(i, (i - 1) % peers) for i in range(peers)],
    )


def neighbours_shards(shard, axis):
    right, left = ring(axis)
    from_left = [lax.ppermute(w, axis, right) for w in shard]
    from_right = [lax.ppermute(w, axis, left) for w in shard]
    return from_left, from_right


def far_shard(from_left, from_right, axis):
    right, left = ring(axis)
    half = from_left[2].shape[0] // 2
    return (
        lax.ppermute(from_left[0], axis, right),
        lax.ppermute(from_right[1], axis, left),
        lax.ppermute(from_left[2][:half], axis, right),
        lax.ppermute(from_right[2][half:], axis, left),
    )


def gated(gate_val, up_val):
    return (jax.nn.silu(gate_val) * up_val).astype(BF16)


def shards(
    queries,
    keys,
    values,
    decay_gate_logits,
    correction_logits,
    head_decay_speed,
    position_log_decay,
    head_output_gain,
    mixer_output_weight,
    expert_input_tokens,
    expert_norm_gain,
    routes,
    chosen_expert_weight,
    routed_gate_weight,
    routed_up_weight,
    routed_down_weight,
    common_gate_weight,
    common_up_weight,
    common_down_weight,
):
    experts = lax.axis_size(EP)
    tokens, _ = expert_input_tokens.shape
    own = (routed_gate_weight[0], routed_up_weight[0], routed_down_weight[0])
    from_left, from_right = neighbours_shards(own, "tp")

    capacity = 3 * tokens * routes.shape[1] // (2 * experts)
    xn, outgoing, mix = dispatch(
        expert_input_tokens,
        expert_norm_gain,
        routes.T,
        chosen_expert_weight.T,
        experts * capacity,
        capacity,
    )

    def to_peers(x):
        parts = x.reshape(experts, -1, LANES)
        return lax.all_to_all(parts, EP, split_axis=0, concat_axis=0, tiled=True).reshape(-1, LANES)

    peers = lax.axis_size("tp")

    def shift(r):
        return [(i, (i + r) % peers) for i in range(peers)]

    arrived = to_peers(outgoing)
    opposite = peers // 2
    near_peers = [r for r in range(1, peers) if r != opposite]
    group = [xn] + [lax.ppermute(xn, "tp", shift(peers - r)) for r in near_peers]

    qt, ol, trans, inject = local_mixer(
        queries,
        keys,
        values,
        decay_gate_logits.T,
        correction_logits.T,
        head_decay_speed,
        position_log_decay.T,
    )
    state = entry_state(trans, inject)
    state, from_left, from_right = lax.optimization_barrier((state, from_left, from_right))
    far = far_shard(from_left, from_right, "tp")
    me = lax.axis_index("tp").astype(jnp.int32).reshape(1)
    parts = parts_for_peers(
        me,
        qt,
        ol,
        state,
        head_output_gain,
        mixer_output_weight,
        group,
        common_gate_weight,
        common_up_weight,
        common_down_weight,
    )
    rows, near = near_experts(arrived, (own, from_left, from_right))
    hidden = far_hidden(rows, *far[:2])
    parts, far, near, hidden, xn = lax.optimization_barrier((parts, far, near, hidden, xn))
    far_xn = lax.ppermute(xn, "tp", shift(opposite))
    got = [parts[0]] + [lax.ppermute(parts[r], "tp", shift(r)) for r in near_peers]
    far_mixer = lax.ppermute(parts[opposite], "tp", shift(opposite))
    slot_sums = far_out(hidden, near, *far[2:])
    back = to_peers(slot_sums)
    far_xn, slot_sums = lax.optimization_barrier((far_xn, slot_sums))
    late = shared_part(far_xn, common_gate_weight, common_up_weight, common_down_weight)
    far_shared = lax.ppermute(late, "tp", shift(opposite))
    mixer_out, shared = sums_of_parts(got, far_mixer, far_shared)
    return (mixer_out, combine(shared, back, mix))


def solution(mesh):
    finer = Mesh(mesh.devices.reshape(8, 4, 2, mesh.shape["tp"]), ("ep_0", "ep_1", "ep_2", "tp"))
    placed = (
        P(EP, "tp"),
        P(EP, "tp"),
        P(EP, "tp"),
        P(EP, "tp"),
        P(EP, "tp"),
        P("tp"),
        P(EP, "tp"),
        P(),
        P("tp", None),
        P(EP_TP, None),
        P(),
        P(EP_TP, None),
        P(EP_TP, None),
        P(EP, None, "tp"),
        P(EP, None, "tp"),
        P(EP, "tp", None),
        P(None, "tp"),
        P(None, "tp"),
        P("tp", None),
    )
    return jax.shard_map(
        shards,
        mesh=finer,
        in_specs=placed,
        out_specs=(P(EP_TP, None), P(EP_TP, None)),
        check_vma=False,
    )
```

```python
import functools

import jax
import jax.numpy as jnp
from jax import lax
from jax.experimental import pallas as pl
from jax.experimental.pallas import tpu as pltpu
from jax.sharding import Mesh
from jax.sharding import PartitionSpec as P


EP = ("ep_0", "ep_1", "ep_2")
EP_TP = ("ep_0", "ep_1", "ep_2", "tp")


EPS = 1e-06
F32 = jnp.float32
BF16 = jnp.bfloat16
LANES = 128
MESH = pl.DeviceIdType.MESH
ALL_VMEM = pltpu.CompilerParams(vmem_limit_bytes=67_043_328)


def halves(x):
    hi = x.astype(BF16)
    return hi, (x - hi.astype(F32)).astype(BF16)


def thirds(x):
    hi = x.astype(BF16)
    rest = x - hi.astype(F32)
    mid = rest.astype(BF16)
    return hi, mid, (rest - mid.astype(F32)).astype(BF16)


def mm(a, b):
    return jnp.dot(a, b, preferred_element_type=F32)


def dot3(a, b):
    ah, al = halves(a)
    bh, bl = halves(b)
    return mm(jnp.concatenate([ah, ah, al], 1), jnp.concatenate([bh, bl, bh], 0))


def dot2(a, b):
    ah, al = halves(a)
    return mm(jnp.concatenate([ah, al], 1), jnp.concatenate([b, b], 0))


def unit_lower_inverses(lows, row, col):
    eye = (row == col).astype(F32)
    near = (row >> 3) == (col >> 3)
    base = [jnp.where(near, low, 0.0) for low in lows]
    squared = [dot3(x, x) for x in base]
    inv = [eye - x for x in base]
    fourth = [dot3(x, x) for x in squared]
    inv = [x + dot3(x, y) for x, y in zip(inv, squared)]
    inv = [x + dot3(x, y) for x, y in zip(inv, fourth)]
    for bit in (3, 4, 5):
        between = ((row >> (bit + 1)) == (col >> (bit + 1))) & ((row >> bit) != (col >> bit))
        right = [dot3(jnp.where(between, low, 0.0), x) for low, x in zip(lows, inv)]
        inv = [x - dot3(x, y) for x, y in zip(inv, right)]
    return inv


def local_mixer_kernel(
    q_ref, k_ref, v_ref, gate_ref, corr_ref, speed_ref, plog_ref, qt_ref, ol_ref, tr_ref, in_ref,
    su_all, pq_all, mw_all, keep_all,
):
    head = pl.program_id(0)
    heads, rows = gate_ref.shape
    pair = 128
    here = lax.broadcasted_iota(jnp.int32, (heads, rows), 0) == head

    log_gate = (
        -speed_ref[...]
        * (jnp.maximum(gate_ref[...], 0.0) + jnp.log1p(jnp.exp(-jnp.abs(gate_ref[...]))))
        + plog_ref[...]
    )
    beta_all = 1.0 / (1.0 + jnp.exp(-corr_ref[...].astype(F32)))
    g_row = jnp.sum(jnp.where(here, log_gate, 0.0), axis=0, keepdims=True)
    beta_row_all = jnp.sum(jnp.where(here, beta_all, 0.0), axis=0, keepdims=True)

    row = lax.broadcasted_iota(jnp.int32, (pair, pair), 0)
    col = lax.broadcasted_iota(jnp.int32, (pair, pair), 1)
    same = (row >> 6) == (col >> 6)
    causal = same & (row >= col)
    strict = same & (row > col)
    first = col < 64
    ones = (same & (row <= col)).astype(BF16)
    ones = jnp.concatenate([ones, ones, ones], 0)

    pairs = range(rows // pair)
    span = [slice(p * pair, (p + 1) * pair) for p in pairs]
    qb, kb, vb = [[ref[at, :] for at in span] for ref in (q_ref, k_ref, v_ref)]
    gram = [
        lax.dot_general(
            jnp.concatenate([k, q], 0), k, (((1,), (1,)), ((), ())), preferred_element_type=F32
        )
        for k, q in zip(kb, qb)
    ]
    c_row = [
        mm(jnp.concatenate(thirds(jnp.broadcast_to(g_row[:, at], (pair, pair))), 1), ones)
        for at in span
    ]
    c_mat = [c.T for c in c_row]
    qf, kf = [x.astype(F32) for x in qb], [x.astype(F32) for x in kb]
    rq = [
        lax.rsqrt(jnp.sum(x * x, axis=1, keepdims=True) + EPS) * (pair**-0.5) for x in qf
    ]
    rk = [lax.rsqrt(jnp.sum(x * x, axis=1, keepdims=True) + EPS) for x in kf]
    rk_row = [jnp.broadcast_to(x, (pair, pair)).T for x in rk]
    beta_row = [jnp.broadcast_to(beta_row_all[:, at], (pair, pair)) for at in span]
    beta = [x.T for x in beta_row]
    decay = [
        jnp.exp(jnp.where(causal, cm - cr, -jnp.inf)) * r for cm, cr, r in zip(c_mat, c_row, rk_row)
    ]
    low = [
        jnp.where(strict, g[:pair] * d * (b * r), 0.0) for g, d, b, r in zip(gram, decay, beta, rk)
    ]
    scores = [g[pair:] * d * r for g, d, r in zip(gram, decay, rq)]
    inv = unit_lower_inverses(low, row, col)
    scale = [b * x for b, x in zip(beta_row, inv)]
    u = [dot2(x, v) for x, v in zip(scale, vb)]
    w = [dot2(x * (jnp.exp(c) * r), k) for x, c, r, k in zip(scale, c_row, rk_row, kb)]
    uw = [jnp.concatenate([x, y], 1) for x, y in zip(u, w)]
    last = [(c[63:64, :], c[127:128, :]) for c in c_mat]
    kt = [
        k.T * (jnp.exp(jnp.where(first, l[0], l[1]) - c) * r)
        for k, l, c, r in zip(kf, last, c_row, rk_row)
    ]
    suw = [dot3(x, y) for x, y in zip(scores, uw)]
    mw = [
        dot3(jnp.concatenate([jnp.where(first, x, 0.0), jnp.where(first, 0.0, x)], 0), y)
        for x, y in zip(kt, uw)
    ]
    pq = [x * (r * jnp.exp(c)) - y[:, pair:] for x, r, c, y in zip(qf, rq, c_mat, suw)]
    for p in pairs:
        su_all[head, p] = suw[p][:, :pair]
        pq_all[head, p] = pq[p]
        mw_all[head, p] = mw[p]
        keep_all[head, p] = jnp.concatenate([jnp.exp(x) for x in last[p]], 0)

    @pl.when(head == heads - 1)
    def _():
        nothing = jnp.zeros((pair, pair), F32)
        ab = [jnp.concatenate([(row == col).astype(F32), nothing], 1) for _ in range(heads)]
        for p in pairs:
            for b in range(2):
                blk = slice(b * 64, (b + 1) * 64)
                at = pl.ds(p * pair + b * 64, 64)
                part = [mw_all[h, p, b * pair : (b + 1) * pair, :] for h in range(heads)]
                got = [
                    dot3(jnp.concatenate([pq_all[h, p, blk, :], part[h][:, pair:]], 0), ab[h])
                    for h in range(heads)
                ]
                for h in range(heads):
                    qt_ref[h, at, :] = got[h][:64, :pair]
                    ol_ref[h, at, :] = got[h][:64, pair:] + su_all[h, p, blk, :]
                    keep = keep_all[h, p, b : b + 1, :]
                    ab[h] = (
                        jnp.concatenate([keep, keep], 1) * ab[h]
                        - got[h][64:]
                        + jnp.concatenate([nothing, part[h][:, :pair]], 1)
                    )
        for h in range(heads):
            tr_ref[h] = ab[h][:, :pair]
            in_ref[h] = ab[h][:, pair:]


def local_mixer(queries, keys, values, gate, corr, speed, plog):
    rows, width = queries.shape
    heads = gate.shape[0]
    d = width // heads
    by_head = pl.BlockSpec((rows, d), lambda h: (0, h))
    whole = pl.BlockSpec((heads, rows), lambda h: (0, 0))
    return pl.pallas_call(
        local_mixer_kernel,
        grid=(heads,),
        in_specs=[
            by_head,
            by_head,
            by_head,
            whole,
            whole,
            pl.BlockSpec((heads, 1), lambda h: (0, 0)),
            whole,
        ],
        out_specs=[
            pl.BlockSpec((heads, rows, d), lambda h: (0, 0, 0)),
            pl.BlockSpec((heads, rows, d), lambda h: (0, 0, 0)),
            pl.BlockSpec((heads, d, d), lambda h: (0, 0, 0)),
            pl.BlockSpec((heads, d, d), lambda h: (0, 0, 0)),
        ],
        scratch_shapes=[
            pltpu.VMEM((heads, rows // 128, 128, d), F32),
            pltpu.VMEM((heads, rows // 128, 128, d), F32),
            pltpu.VMEM((heads, rows // 128, 2 * d, 2 * d), F32),
            pltpu.VMEM((heads, rows // 128, 2, d), F32),
        ],
        out_shape=[
            jax.ShapeDtypeStruct((heads, rows, d), F32),
            jax.ShapeDtypeStruct((heads, rows, d), F32),
            jax.ShapeDtypeStruct((heads, d, d), F32),
            jax.ShapeDtypeStruct((heads, d, d), F32),
        ],
        cost_estimate=pl.CostEstimate(flops=30_000_000_000, bytes_accessed=4_000_000, transcendentals=0),
        compiler_params=ALL_VMEM,
        name="local_mixer",
    )(queries, keys, values, gate, corr, speed.reshape(heads, 1), plog)


def entry_state_kernel(
    t_ref, i_ref, s_ref, own, peer, ypack, zpack,
    send_c, recv_c, send_y, recv_y, send_yc, recv_yc,
    send_r, recv_r, send_l, recv_l, send_rc, recv_rc, send_lc, recv_lc,
):
    heads, d, _ = t_ref.shape
    half = d // 2
    nz, ny = zpack.shape[0], ypack.shape[0]
    z, y, c = lax.axis_index("ep_0"), lax.axis_index("ep_1"), lax.axis_index("ep_2")
    other = {"ep_2": 1 - c}
    right, left = {"ep_0": lax.rem(z + 1, nz)}, {"ep_0": lax.rem(z + nz - 1, nz)}
    across = [{"ep_1": lax.rem(y + k, ny)} for k in range(1, ny)]

    barrier = pltpu.get_barrier_semaphore()
    for who in (other, right, left, *across):
        pl.semaphore_signal(barrier, inc=1, device_id=who, device_id_type=MESH)
    pl.semaphore_wait(barrier, 3 + len(across))

    def send(src, dst, send_sem, recv_sem, who):
        return pltpu.make_async_remote_copy(
            src_ref=src, dst_ref=dst, send_sem=send_sem, recv_sem=recv_sem,
            device_id=who, device_id_type=MESH,
        )

    def store(ref, h, both):
        both = both.astype(BF16)
        ref[0, h] = both[:half]
        ref[1, h] = both[half:]

    def load(ref, h):
        return jnp.concatenate([ref[0, h], ref[1, h]], 0)

    def after(pack, so_far):
        hi, lo = halves(so_far)
        t = pack[:, :d]
        return mm(jnp.concatenate([t, t], 1), jnp.concatenate([hi, lo], 0))

    def added(pack):
        return pack[:, d:].astype(F32)

    nothing = jnp.zeros((d, d), F32)
    for h in range(heads):
        store(own, h, jnp.concatenate([t_ref[h], i_ref[h]], 1))
    swap = send(own, peer, send_c, recv_c, other)
    swap.start()
    swap.wait()
    for h in range(heads):
        mine, theirs = load(own, h), load(peer, h)
        early = jnp.where(c == 0, mine.astype(F32), theirs.astype(F32)).astype(BF16)
        late = jnp.where(c == 0, theirs.astype(F32), mine.astype(F32)).astype(BF16)
        both = mm(late[:, :d], early) + jnp.concatenate([nothing, added(late)], 1)
        store(ypack.at[y], h, both)

    out = [
        send(ypack.at[y, c], ypack.at[y, c], send_y.at[k - 1], recv_y.at[k - 1], across[k - 1])
        for k in range(1, ny)
    ]
    for copy in out:
        copy.start()
    over = []
    for k in range(1, ny):
        slot = ypack.at[lax.rem(y + ny - k, ny), c]
        out[k - 1].wait_recv()
        over.append(send(slot, slot, send_yc.at[k - 1], recv_yc.at[k - 1], other))
        over[-1].start()
    for copy in out:
        copy.wait_send()
    for copy in over:
        copy.wait()
    for h in range(heads):
        both = load(ypack.at[0], h).astype(F32)
        for k in range(1, ny):
            pack = load(ypack.at[k], h)
            both = after(pack, both) + jnp.concatenate([nothing, added(pack)], 1)
        store(zpack.at[z], h, both)

    def going(r, h, sign, who, send_sem, recv_sem):
        slot = zpack.at[lax.rem(z + nz - sign * (r - 1), nz), c, h]
        return send(slot, slot, send_sem.at[r - 1, h], recv_sem.at[r - 1, h], who)

    def shared_with_other(r, h, sign, send_sem, recv_sem):
        slot = zpack.at[lax.rem(z + nz - sign * r, nz), c, h]
        return send(slot, slot, send_sem.at[r - 1, h], recv_sem.at[r - 1, h], other)

    rings = (
        (nz // 2, 1, right, send_r, recv_r, send_rc, recv_rc),
        ((nz - 1) // 2, -1, left, send_l, recv_l, send_lc, recv_lc),
    )
    pending = []
    for rounds, sign, who, ss, rs, _, _ in rings:
        for h in range(heads):
            if rounds > 0:
                going(1, h, sign, who, ss, rs).start()
    for r in range(1, nz // 2 + 1):
        for h in range(heads):
            for rounds, sign, who, ss, rs, sc, rc in rings:
                if r > rounds:
                    continue
                copy = going(r, h, sign, who, ss, rs)
                copy.wait_recv()
                pending.append((copy, False))
                if r < rounds:
                    going(r + 1, h, sign, who, ss, rs).start()
                hand = shared_with_other(r, h, sign, sc, rc)
                hand.start()
                pending.append((hand, True))
    for copy, both_ways in pending:
        copy.wait_send()
        if both_ways:
            copy.wait_recv()

    for h in range(heads):
        s_ref[h] = nothing
    for k in range(nz - 1):
        for h in range(heads):
            pack = load(zpack.at[k], h)
            s_ref[h] = jnp.where(k < z, after(pack, s_ref[h]) + added(pack), s_ref[h])
    for k in range(ny - 1):
        for h in range(heads):
            pack = load(ypack.at[k], h)
            s_ref[h] = jnp.where(k < y, after(pack, s_ref[h]) + added(pack), s_ref[h])
    for h in range(heads):
        pack = load(peer, h)
        s_ref[h] = jnp.where(c == 1, after(pack, s_ref[h]) + added(pack), s_ref[h])


def entry_state(trans, inject):
    heads, d, _ = trans.shape
    nz, ny = lax.axis_size("ep_0"), lax.axis_size("ep_1")
    half = (2, heads, d // 2, 2 * d)
    dma = pltpu.SemaphoreType.DMA
    rounds = max(nz // 2, 1)
    vmem = pl.BlockSpec(memory_space=pltpu.VMEM)
    return pl.pallas_call(
        entry_state_kernel,
        in_specs=[vmem, vmem],
        out_specs=vmem,
        out_shape=jax.ShapeDtypeStruct((heads, d, d), F32),
        scratch_shapes=[
            pltpu.VMEM(half, BF16),
            pltpu.VMEM(half, BF16),
            pltpu.VMEM((ny, *half), BF16),
            pltpu.VMEM((nz, *half), BF16),
            dma, dma,
            dma((max(ny - 1, 1),)), dma((max(ny - 1, 1),)), dma((max(ny - 1, 1),)), dma((max(ny - 1, 1),)),
            *[dma((rounds, heads)) for _ in range(8)],
        ],
        compiler_params=pltpu.CompilerParams(
            collective_id=0, has_side_effects=True, vmem_limit_bytes=67_043_328
        ),
        cost_estimate=pl.CostEstimate(flops=30_000_000_000, bytes_accessed=4_000_000, transcendentals=0),
        name="entry_state",
    )(trans, inject)


def parts_kernel(peers, me_ref, qt_ref, ol_ref, state_ref, gain_ref, w_ref, *refs):
    far = peers // 2
    near = [r for r in range(peers) if r != far]
    count = len(near)
    hbm, refs = refs[: count + 3], refs[count + 3 :]
    out_refs, (x, gate, up, down, sems) = refs[:peers], refs[peers:]
    heads, rows, _ = qt_ref.shape
    tile = rows // peers
    spots = [x.at[r * tile : (r + 1) * tile] for r in range(count)] + [gate, up, down]
    copies = [
        pltpu.make_async_copy(src, dst, sems.at[k]) for k, (src, dst) in enumerate(zip(hbm, spots))
    ]
    for copy in copies:
        copy.start()
    turns = [
        pl.ds(pl.multiple_of(lax.rem(me_ref[0] + r, peers) * tile, tile), tile)
        for r in range(peers)
    ]
    normed = []
    for h in range(heads):
        qt = jnp.concatenate([qt_ref[h, at, :] for at in turns], 0)
        ol = jnp.concatenate([ol_ref[h, at, :] for at in turns], 0)
        out = dot3(qt, state_ref[h]) + ol
        out = out * lax.rsqrt(jnp.mean(out * out, axis=1, keepdims=True) + EPS) * gain_ref[...]
        normed.append(out.astype(BF16))
    mixer = mm(jnp.concatenate(normed, 1), w_ref[...]).astype(BF16)
    for r in range(peers):
        out_refs[r][:tile] = mixer[r * tile : (r + 1) * tile]
    for copy in copies:
        copy.wait()
    hidden = gated(mm(x[...], gate[...]), mm(x[...], up[...]))
    shared = mm(hidden, down[...]).astype(BF16)
    for k, r in enumerate(near):
        out_refs[r][tile:] = shared[k * tile : (k + 1) * tile]


def parts_for_peers(me, qt, ol, state, gain, w, tokens, gate, up, down):
    _, rows, d = qt.shape
    width = w.shape[1]
    peers = len(tokens) + 1
    tile = rows // peers
    vmem = pl.BlockSpec(memory_space=pltpu.VMEM)
    kept = (*tokens, gate, up, down)
    return pl.pallas_call(
        functools.partial(parts_kernel, peers),
        in_specs=[pl.BlockSpec(memory_space=pltpu.SMEM)]
        + [vmem] * 5
        + [pl.BlockSpec(memory_space=pl.ANY)] * len(kept),
        out_specs=[vmem] * peers,
        out_shape=[
            jax.ShapeDtypeStruct((tile if r == peers // 2 else 2 * tile, width), BF16)
            for r in range(peers)
        ],
        scratch_shapes=[
            pltpu.VMEM((len(tokens) * tile, width), BF16),
            pltpu.VMEM(gate.shape, BF16),
            pltpu.VMEM(up.shape, BF16),
            pltpu.VMEM(down.shape, BF16),
            pltpu.SemaphoreType.DMA((len(kept),)),
        ],
        cost_estimate=pl.CostEstimate(flops=6_000_000_000, bytes_accessed=12_000_000, transcendentals=0),
        compiler_params=ALL_VMEM,
        name="parts_for_peers",
    )(me, qt, ol, state, gain.reshape(1, d), w, *kept)


def shared_part_kernel(x_ref, gate_ref, up_ref, down_hbm, out_ref, down, sem):
    load = pltpu.make_async_copy(down_hbm, down, sem)
    load.start()
    x = x_ref[...]
    hidden = gated(mm(x, gate_ref[...]), mm(x, up_ref[...]))
    load.wait()
    out_ref[...] = mm(hidden, down[...]).astype(BF16)


def shared_part(x, gate, up, down):
    vmem = pl.BlockSpec(memory_space=pltpu.VMEM)
    return pl.pallas_call(
        shared_part_kernel,
        in_specs=[vmem] * 3 + [pl.BlockSpec(memory_space=pl.ANY)],
        out_specs=vmem,
        out_shape=jax.ShapeDtypeStruct((x.shape[0], down.shape[1]), BF16),
        scratch_shapes=[pltpu.VMEM(down.shape, BF16), pltpu.SemaphoreType.DMA],
        cost_estimate=pl.CostEstimate(flops=1_000_000_000, bytes_accessed=4_000_000, transcendentals=0),
        compiler_params=ALL_VMEM,
        name="shared_part",
    )(x, gate, up, down)


def near_experts_kernel(in_ref, *refs):
    shards_ = len(refs) // 3 - 2
    hbm, (x_ref, out_ref, gates, ups, downs) = refs[: 3 * shards_], refs[3 * shards_ : -1]
    sems = refs[-1]
    rows, width = x_ref.shape
    cuts = width // LANES
    tile = 128
    copies = [
        [
            pltpu.make_async_copy(hbm[3 * m + k], held.at[m], sems.at[m, k])
            for k, held in enumerate((gates, ups, downs))
        ]
        for m in range(shards_)
    ]
    for shard in copies:
        for copy in shard:
            copy.start()
    for t in range(rows // tile):
        x_ref[t * tile : (t + 1) * tile, :] = gathered(
            in_ref[t * tile * cuts : (t + 1) * tile * cuts, :], cuts
        )
    for m in range(shards_):
        for copy in copies[m]:
            copy.wait()
        x = x_ref[...]
        part = mm(gated(mm(x, gates[m]), mm(x, ups[m])), downs[m])
        out_ref[...] = part if m == 0 else out_ref[...] + part


def near_experts(spread_in, shards_):
    weights = [w for shard in shards_ for w in shard]
    width, hidden = shards_[0][0].shape
    rows = spread_in.shape[0] * LANES // width
    count = len(shards_)
    vmem = pl.BlockSpec(memory_space=pltpu.VMEM)
    return pl.pallas_call(
        near_experts_kernel,
        in_specs=[vmem] + [pl.BlockSpec(memory_space=pl.ANY)] * len(weights),
        out_specs=[vmem, vmem],
        out_shape=[
            jax.ShapeDtypeStruct((rows, width), BF16),
            jax.ShapeDtypeStruct((rows, width), F32),
        ],
        scratch_shapes=[
            pltpu.VMEM((count, width, hidden), BF16),
            pltpu.VMEM((count, width, hidden), BF16),
            pltpu.VMEM((count, hidden, width), BF16),
            pltpu.SemaphoreType.DMA((count, 3)),
        ],
        cost_estimate=pl.CostEstimate(flops=5_000_000_000, bytes_accessed=16_000_000, transcendentals=0),
        compiler_params=ALL_VMEM,
        name="near_experts",
    )(spread_in, *weights)


def far_hidden_kernel(x_ref, gate_ref, up_ref, out_ref):
    x = x_ref[...]
    out_ref[...] = gated(mm(x, gate_ref[...]), mm(x, up_ref[...]))


def far_hidden(x, gate, up):
    vmem = pl.BlockSpec(memory_space=pltpu.VMEM)
    return pl.pallas_call(
        far_hidden_kernel,
        in_specs=[vmem] * 3,
        out_specs=vmem,
        out_shape=jax.ShapeDtypeStruct((x.shape[0], gate.shape[1]), BF16),
        cost_estimate=pl.CostEstimate(flops=1_500_000_000, bytes_accessed=4_000_000, transcendentals=0),
        compiler_params=ALL_VMEM,
        name="far_hidden",
    )(x, gate, up)


def far_out_kernel(hidden_ref, near_ref, down0_ref, down1_ref, out_ref, near, down, ready, sems):
    rows, width = near.shape
    cuts = width // LANES
    half = down.shape[0] // 2
    tile = rows // ready.shape[0]
    spans = [slice(t * tile, (t + 1) * tile) for t in range(ready.shape[0])]
    loads = [
        pltpu.make_async_copy(down0_ref, down.at[:half], sems.at[0]),
        pltpu.make_async_copy(down1_ref, down.at[half:], sems.at[1]),
    ] + [
        pltpu.make_async_copy(near_ref.at[at], near.at[at], sems.at[2 + t])
        for t, at in enumerate(spans)
    ]
    for copy in loads:
        copy.start()
    for copy in loads[:2]:
        copy.wait()
    stores = []
    for t, at in enumerate(spans):
        part = mm(hidden_ref[at, :], down[...])
        loads[2 + t].wait()
        ready[t] = spread(near[at, :] + part)
        stores.append(
            pltpu.make_async_copy(
                ready.at[t],
                out_ref.at[t * tile * cuts : (t + 1) * tile * cuts],
                sems.at[2 + len(spans) + t],
            )
        )
        stores[-1].start()
    for copy in stores:
        copy.wait()


def far_out(hidden, near, down0, down1):
    rows, width = near.shape
    cuts = width // LANES
    tiles = rows // 128
    hbm = pl.BlockSpec(memory_space=pl.ANY)
    return pl.pallas_call(
        far_out_kernel,
        in_specs=[pl.BlockSpec(memory_space=pltpu.VMEM), hbm, hbm, hbm],
        out_specs=hbm,
        out_shape=jax.ShapeDtypeStruct((rows * cuts, LANES), BF16),
        scratch_shapes=[
            pltpu.VMEM((rows, width), F32),
            pltpu.VMEM((2 * down0.shape[0], width), BF16),
            pltpu.VMEM((tiles, 128 * cuts, LANES), BF16),
            pltpu.SemaphoreType.DMA((2 + 2 * tiles,)),
        ],
        cost_estimate=pl.CostEstimate(flops=1_500_000_000, bytes_accessed=8_000_000, transcendentals=0),
        name="far_out",
    )(hidden, near, down0, down1)


def interleaving(cuts, back=False):
    i = lax.broadcasted_iota(jnp.int32, (8 * cuts, 8 * cuts), 1 if back else 0)
    j = lax.broadcasted_iota(jnp.int32, (8 * cuts, 8 * cuts), 0 if back else 1)
    return ((lax.div(i, cuts) == lax.rem(j, 8)) & (lax.rem(i, cuts) == lax.div(j, 8))).astype(BF16)


def spread(values):
    rows, width = values.shape
    cuts = width // LANES
    order = interleaving(cuts)
    blocks = [
        jnp.concatenate(
            [values[g : g + 8, c * LANES : (c + 1) * LANES] for c in range(cuts)], 0
        ).astype(BF16)
        for g in range(0, rows, 8)
    ]
    out = []
    for g in range(0, len(blocks), 2):
        two = mm(order, jnp.concatenate(blocks[g : g + 2], 1)).astype(BF16)
        out += [two[:, :LANES], two[:, LANES:]]
    return jnp.concatenate(out, 0)


def gathered(tall, cuts):
    order = interleaving(cuts, back=True)
    size = 8 * cuts
    blocks = [tall[g : g + size] for g in range(0, tall.shape[0], size)]
    out = []
    for g in range(0, len(blocks), 2):
        two = mm(order, jnp.concatenate(blocks[g : g + 2], 1))
        out += [two[:, :LANES], two[:, LANES:]]
    return jnp.concatenate(
        [jnp.concatenate([x[c * 8 : (c + 1) * 8] for x in out], 0) for c in range(cuts)], 1
    ).astype(BF16)


def dispatch_kernel(capacity, x_ref, gain_ref, routes_ref, weight_ref, xn_ref, out_ref, mix_ref):
    tokens, width = x_ref.shape
    slots = mix_ref.shape[1]
    x = x_ref[...].astype(F32)
    xn = (x * lax.rsqrt(jnp.mean(x * x, axis=1, keepdims=True) + EPS) * gain_ref[...]).astype(BF16)
    xn_ref[...] = xn
    expert = lax.broadcasted_iota(jnp.int32, (LANES, tokens), 0)
    first, second = expert == routes_ref[0:1, :], expert == routes_ref[1:2, :]
    chosen = (first | second).astype(BF16)
    token = lax.broadcasted_iota(jnp.int32, (tokens, tokens), 0)
    later = lax.broadcasted_iota(jnp.int32, (tokens, tokens), 1)
    place = mm(chosen, (token < later).astype(BF16)) + (expert * capacity).astype(F32)
    s0 = jnp.sum(jnp.where(first, place, 0.0), axis=0, keepdims=True)
    s1 = jnp.sum(jnp.where(second, place, 0.0), axis=0, keepdims=True)
    step = 128
    cuts = width // LANES
    for base in range(0, slots, step):
        slot = (lax.broadcasted_iota(jnp.int32, (step, tokens), 0) + base).astype(F32)
        is0, is1 = slot == s0, slot == s1
        out_ref[base * cuts : (base + step) * cuts, :] = spread(mm((is0 | is1).astype(BF16), xn))
        mix = jnp.where(is0, weight_ref[0:1, :], 0.0) + jnp.where(is1, weight_ref[1:2, :], 0.0)
        mix_ref[:, base : base + step] = mix.T


def dispatch(x, gain, routes, weight, slots, capacity):
    tokens, width = x.shape
    cuts = width // LANES
    return pl.pallas_call(
        functools.partial(dispatch_kernel, capacity),
        out_shape=[
            jax.ShapeDtypeStruct((tokens, width), BF16),
            jax.ShapeDtypeStruct((slots * cuts, LANES), BF16),
            jax.ShapeDtypeStruct((tokens, slots), F32),
        ],
        name="dispatch",
    )(x, gain.reshape(1, width), routes, weight)


def sums_kernel(*refs):
    *part_refs, far_mixer_ref, mixer_ref, shared_ref = refs
    tokens = mixer_ref.shape[0]
    mixer, shared = far_mixer_ref[...].astype(F32), None
    for part in part_refs:
        mixer = mixer + part[:tokens].astype(F32)
        term = part[tokens:].astype(F32)
        shared = term if shared is None else shared + term
    mixer_ref[...] = mixer.astype(BF16)
    shared_ref[...] = shared


def sums_of_parts(parts, far_mixer):
    tokens, width = far_mixer.shape
    tile = 512
    out = pl.BlockSpec((tokens, tile), lambda c: (0, c))
    return pl.pallas_call(
        sums_kernel,
        grid=(width // tile,),
        in_specs=[pl.BlockSpec((2 * tokens, tile), lambda c: (0, c))] * len(parts) + [out],
        out_specs=[out, out],
        out_shape=[
            jax.ShapeDtypeStruct((tokens, width), BF16),
            jax.ShapeDtypeStruct((tokens, width), F32),
        ],
        cost_estimate=pl.CostEstimate(flops=1_000_000_000, bytes_accessed=6_000_000, transcendentals=0),
        compiler_params=ALL_VMEM,
        name="sums_of_parts",
    )(*parts, far_mixer)


def combine_kernel(
    shared_hbm, late_hbm, back_hbm, mix_hbm, out_hbm, shared, late, back, mix, out, sems
):
    tiles = back.shape[0]
    width = shared.shape[1]
    cuts = width // LANES
    tile = back.shape[1] // cuts
    loads = [
        pltpu.make_async_copy(
            back_hbm.at[t * tile * cuts : (t + 1) * tile * cuts], back.at[t], sems.at[t]
        )
        for t in range(tiles)
    ]
    loads.insert(1, pltpu.make_async_copy(mix_hbm, mix, sems.at[tiles]))
    loads.append(pltpu.make_async_copy(shared_hbm, shared, sems.at[tiles + 1]))
    loads.append(pltpu.make_async_copy(late_hbm, late, sems.at[tiles + 2]))
    for copy in loads:
        copy.start()
    rows = []
    for t, count in enumerate((2,) + (1,) * (tiles - 1)):
        for _ in range(count):
            loads.pop(0).wait()
        rows.append(gathered(back[t], cuts))
    for copy in loads:
        copy.wait()
    rows = jnp.concatenate(rows, 0)
    hi, lo = halves(mix[...])
    both = jnp.concatenate([hi, lo], 1)
    stores = []
    for k in range(2):
        at = slice(k * width // 2, (k + 1) * width // 2)
        part = jnp.concatenate([rows[:, at], rows[:, at]], 0)
        total = shared[:, at] + late[:, at].astype(F32)
        out[:, at] = (total + mm(both, part)).astype(BF16)
        stores.append(pltpu.make_async_copy(out.at[:, at], out_hbm.at[:, at], sems.at[tiles + 3 + k]))
        stores[-1].start()
    for copy in stores:
        copy.wait()


def combine(shared, late, back, mix):
    tokens, width = shared.shape
    cuts = width // LANES
    tile = 128
    tiles = mix.shape[1] // tile
    hbm = pl.BlockSpec(memory_space=pl.ANY)
    return pl.pallas_call(
        combine_kernel,
        in_specs=[hbm] * 4,
        out_specs=hbm,
        out_shape=jax.ShapeDtypeStruct((tokens, width), BF16),
        scratch_shapes=[
            pltpu.VMEM((tokens, width), F32),
            pltpu.VMEM((tokens, width), BF16),
            pltpu.VMEM((tiles, tile * cuts, LANES), BF16),
            pltpu.VMEM(mix.shape, F32),
            pltpu.VMEM((tokens, width), BF16),
            pltpu.SemaphoreType.DMA((tiles + 5,)),
        ],
        compiler_params=ALL_VMEM,
        name="combine",
    )(shared, late, back, mix)


def ring(axis):
    peers = lax.axis_size(axis)
    return (
        [(i, (i + 1) % peers) for i in range(peers)],
        [(i, (i - 1) % peers) for i in range(peers)],
    )


def neighbours_shards(shard, axis):
    right, left = ring(axis)
    from_left = [lax.ppermute(w, axis, right) for w in shard]
    from_right = [lax.ppermute(w, axis, left) for w in shard]
    return from_left, from_right


def far_shard(from_left, from_right, axis):
    right, left = ring(axis)
    half = from_left[2].shape[0] // 2
    return (
        lax.ppermute(from_left[0], axis, right),
        lax.ppermute(from_right[1], axis, left),
        lax.ppermute(from_left[2][:half], axis, right),
        lax.ppermute(from_right[2][half:], axis, left),
    )


def gated(gate_val, up_val):
    return (jax.nn.silu(gate_val) * up_val).astype(BF16)


def shards(
    queries,
    keys,
    values,
    decay_gate_logits,
    correction_logits,
    head_decay_speed,
    position_log_decay,
    head_output_gain,
    mixer_output_weight,
    expert_input_tokens,
    expert_norm_gain,
    routes,
    chosen_expert_weight,
    routed_gate_weight,
    routed_up_weight,
    routed_down_weight,
    common_gate_weight,
    common_up_weight,
    common_down_weight,
):
    experts = lax.axis_size(EP)
    tokens, _ = expert_input_tokens.shape
    own = (routed_gate_weight[0], routed_up_weight[0], routed_down_weight[0])
    from_left, from_right = neighbours_shards(own, "tp")

    capacity = 3 * tokens * routes.shape[1] // (2 * experts)
    xn, outgoing, mix = dispatch(
        expert_input_tokens,
        expert_norm_gain,
        routes.T,
        chosen_expert_weight.T,
        experts * capacity,
        capacity,
    )

    def to_peers(x):
        parts = x.reshape(experts, -1, LANES)
        return lax.all_to_all(parts, EP, split_axis=0, concat_axis=0, tiled=True).reshape(-1, LANES)

    peers = lax.axis_size("tp")

    def shift(r):
        return [(i, (i + r) % peers) for i in range(peers)]

    arrived = to_peers(outgoing)
    opposite = peers // 2
    near_peers = [r for r in range(1, peers) if r != opposite]
    group = [xn] + [lax.ppermute(xn, "tp", shift(peers - r)) for r in near_peers]

    qt, ol, trans, inject = local_mixer(
        queries,
        keys,
        values,
        decay_gate_logits.T,
        correction_logits.T,
        head_decay_speed,
        position_log_decay.T,
    )
    state = entry_state(trans, inject)
    state, from_left, from_right = lax.optimization_barrier((state, from_left, from_right))
    far = far_shard(from_left, from_right, "tp")
    me = lax.axis_index("tp").astype(jnp.int32).reshape(1)
    parts = parts_for_peers(
        me,
        qt,
        ol,
        state,
        head_output_gain,
        mixer_output_weight,
        group,
        common_gate_weight,
        common_up_weight,
        common_down_weight,
    )
    rows, near = near_experts(arrived, (own, from_left, from_right))
    hidden = far_hidden(rows, *far[:2])
    parts, far, near, hidden, xn = lax.optimization_barrier((parts, far, near, hidden, xn))
    far_xn = lax.ppermute(xn, "tp", shift(opposite))
    far_mixer = lax.ppermute(parts[opposite], "tp", shift(opposite))
    slot_sums = far_out(hidden, near, *far[2:])
    back = to_peers(slot_sums)
    got = [parts[0]] + [lax.ppermute(parts[r], "tp", shift(r)) for r in near_peers]
    far_xn, slot_sums = lax.optimization_barrier((far_xn, slot_sums))
    late = shared_part(far_xn, common_gate_weight, common_up_weight, common_down_weight)
    far_shared = lax.ppermute(late, "tp", shift(opposite))
    mixer_out, shared = sums_of_parts(got, far_mixer)
    return (mixer_out, combine(shared, far_shared, back, mix))


def solution(mesh):
    finer = Mesh(mesh.devices.reshape(8, 4, 2, mesh.shape["tp"]), ("ep_0", "ep_1", "ep_2", "tp"))
    placed = (
        P(EP, "tp"),
        P(EP, "tp"),
        P(EP, "tp"),
        P(EP, "tp"),
        P(EP, "tp"),
        P("tp"),
        P(EP, "tp"),
        P(),
        P("tp", None),
        P(EP_TP, None),
        P(),
        P(EP_TP, None),
        P(EP_TP, None),
        P(EP, None, "tp"),
        P(EP, None, "tp"),
        P(EP, "tp", None),
        P(None, "tp"),
        P(None, "tp"),
        P("tp", None),
    )
    return jax.shard_map(
        shards,
        mesh=finer,
        in_specs=placed,
        out_specs=(P(EP_TP, None), P(EP_TP, None)),
        check_vma=False,
    )
```

```python
import functools

import jax
import jax.numpy as jnp
from jax import lax
from jax.experimental import pallas as pl
from jax.experimental.pallas import tpu as pltpu
from jax.sharding import Mesh
from jax.sharding import PartitionSpec as P


EP = ("ep_0", "ep_1", "ep_2")
EP_TP = ("ep_0", "ep_1", "ep_2", "tp")


EPS = 1e-06
F32 = jnp.float32
BF16 = jnp.bfloat16
LANES = 128
MESH = pl.DeviceIdType.MESH
ALL_VMEM = pltpu.CompilerParams(vmem_limit_bytes=67_043_328)


def halves(x):
    hi = x.astype(BF16)
    return hi, (x - hi.astype(F32)).astype(BF16)


def thirds(x):
    hi = x.astype(BF16)
    rest = x - hi.astype(F32)
    mid = rest.astype(BF16)
    return hi, mid, (rest - mid.astype(F32)).astype(BF16)


def mm(a, b):
    return jnp.dot(a, b, preferred_element_type=F32)


def dot3(a, b):
    ah, al = halves(a)
    bh, bl = halves(b)
    return mm(jnp.concatenate([ah, ah, al], 1), jnp.concatenate([bh, bl, bh], 0))


def dot2(a, b):
    ah, al = halves(a)
    return mm(jnp.concatenate([ah, al], 1), jnp.concatenate([b, b], 0))


def unit_lower_inverses(lows, row, col):
    eye = (row == col).astype(F32)
    near = (row >> 3) == (col >> 3)
    base = [jnp.where(near, low, 0.0) for low in lows]
    squared = [dot3(x, x) for x in base]
    inv = [eye - x for x in base]
    fourth = [dot3(x, x) for x in squared]
    inv = [x + dot3(x, y) for x, y in zip(inv, squared)]
    inv = [x + dot3(x, y) for x, y in zip(inv, fourth)]
    for bit in (3, 4, 5):
        between = ((row >> (bit + 1)) == (col >> (bit + 1))) & ((row >> bit) != (col >> bit))
        right = [dot3(jnp.where(between, low, 0.0), x) for low, x in zip(lows, inv)]
        inv = [x - dot3(x, y) for x, y in zip(inv, right)]
    return inv


def local_mixer_kernel(
    q_ref, k_ref, v_ref, gate_ref, corr_ref, speed_ref, plog_ref, qt_ref, ol_ref, tr_ref, in_ref,
    su_all, pq_all, mw_all, keep_all,
):
    head = pl.program_id(0)
    heads, rows = gate_ref.shape
    pair = 128
    here = lax.broadcasted_iota(jnp.int32, (heads, rows), 0) == head

    log_gate = (
        -speed_ref[...]
        * (jnp.maximum(gate_ref[...], 0.0) + jnp.log1p(jnp.exp(-jnp.abs(gate_ref[...]))))
        + plog_ref[...]
    )
    beta_all = 1.0 / (1.0 + jnp.exp(-corr_ref[...].astype(F32)))
    g_row = jnp.sum(jnp.where(here, log_gate, 0.0), axis=0, keepdims=True)
    beta_row_all = jnp.sum(jnp.where(here, beta_all, 0.0), axis=0, keepdims=True)

    row = lax.broadcasted_iota(jnp.int32, (pair, pair), 0)
    col = lax.broadcasted_iota(jnp.int32, (pair, pair), 1)
    same = (row >> 6) == (col >> 6)
    causal = same & (row >= col)
    strict = same & (row > col)
    first = col < 64
    ones = (same & (row <= col)).astype(BF16)
    ones = jnp.concatenate([ones, ones, ones], 0)

    pairs = range(rows // pair)
    span = [slice(p * pair, (p + 1) * pair) for p in pairs]
    qb, kb, vb = [[ref[at, :] for at in span] for ref in (q_ref, k_ref, v_ref)]
    gram = [
        lax.dot_general(
            jnp.concatenate([k, q], 0), k, (((1,), (1,)), ((), ())), preferred_element_type=F32
        )
        for k, q in zip(kb, qb)
    ]
    c_row = [
        mm(jnp.concatenate(thirds(jnp.broadcast_to(g_row[:, at], (pair, pair))), 1), ones)
        for at in span
    ]
    c_mat = [c.T for c in c_row]
    qf, kf = [x.astype(F32) for x in qb], [x.astype(F32) for x in kb]
    rq = [
        lax.rsqrt(jnp.sum(x * x, axis=1, keepdims=True) + EPS) * (pair**-0.5) for x in qf
    ]
    rk = [lax.rsqrt(jnp.sum(x * x, axis=1, keepdims=True) + EPS) for x in kf]
    rk_row = [jnp.broadcast_to(x, (pair, pair)).T for x in rk]
    beta_row = [jnp.broadcast_to(beta_row_all[:, at], (pair, pair)) for at in span]
    beta = [x.T for x in beta_row]
    decay = [
        jnp.exp(jnp.where(causal, cm - cr, -jnp.inf)) * r for cm, cr, r in zip(c_mat, c_row, rk_row)
    ]
    low = [
        jnp.where(strict, g[:pair] * d * (b * r), 0.0) for g, d, b, r in zip(gram, decay, beta, rk)
    ]
    scores = [g[pair:] * d * r for g, d, r in zip(gram, decay, rq)]
    inv = unit_lower_inverses(low, row, col)
    scale = [b * x for b, x in zip(beta_row, inv)]
    u = [dot2(x, v) for x, v in zip(scale, vb)]
    w = [dot2(x * (jnp.exp(c) * r), k) for x, c, r, k in zip(scale, c_row, rk_row, kb)]
    uw = [jnp.concatenate([x, y], 1) for x, y in zip(u, w)]
    last = [(c[63:64, :], c[127:128, :]) for c in c_mat]
    kt = [
        k.T * (jnp.exp(jnp.where(first, l[0], l[1]) - c) * r)
        for k, l, c, r in zip(kf, last, c_row, rk_row)
    ]
    suw = [dot3(x, y) for x, y in zip(scores, uw)]
    mw = [
        dot3(jnp.concatenate([jnp.where(first, x, 0.0), jnp.where(first, 0.0, x)], 0), y)
        for x, y in zip(kt, uw)
    ]
    pq = [x * (r * jnp.exp(c)) - y[:, pair:] for x, r, c, y in zip(qf, rq, c_mat, suw)]
    for p in pairs:
        su_all[head, p] = suw[p][:, :pair]
        pq_all[head, p] = pq[p]
        mw_all[head, p] = mw[p]
        keep_all[head, p] = jnp.concatenate([jnp.exp(x) for x in last[p]], 0)

    @pl.when(head == heads - 1)
    def _():
        nothing = jnp.zeros((pair, pair), F32)
        ab = [jnp.concatenate([(row == col).astype(F32), nothing], 1) for _ in range(heads)]
        for p in pairs:
            for b in range(2):
                blk = slice(b * 64, (b + 1) * 64)
                at = pl.ds(p * pair + b * 64, 64)
                part = [mw_all[h, p, b * pair : (b + 1) * pair, :] for h in range(heads)]
                got = [
                    dot3(jnp.concatenate([pq_all[h, p, blk, :], part[h][:, pair:]], 0), ab[h])
                    for h in range(heads)
                ]
                for h in range(heads):
                    qt_ref[h, at, :] = got[h][:64, :pair]
                    ol_ref[h, at, :] = got[h][:64, pair:] + su_all[h, p, blk, :]
                    keep = keep_all[h, p, b : b + 1, :]
                    ab[h] = (
                        jnp.concatenate([keep, keep], 1) * ab[h]
                        - got[h][64:]
                        + jnp.concatenate([nothing, part[h][:, :pair]], 1)
                    )
        for h in range(heads):
            tr_ref[h] = ab[h][:, :pair]
            in_ref[h] = ab[h][:, pair:]


def local_mixer(queries, keys, values, gate, corr, speed, plog):
    rows, width = queries.shape
    heads = gate.shape[0]
    d = width // heads
    by_head = pl.BlockSpec((rows, d), lambda h: (0, h))
    whole = pl.BlockSpec((heads, rows), lambda h: (0, 0))
    return pl.pallas_call(
        local_mixer_kernel,
        grid=(heads,),
        in_specs=[
            by_head,
            by_head,
            by_head,
            whole,
            whole,
            pl.BlockSpec((heads, 1), lambda h: (0, 0)),
            whole,
        ],
        out_specs=[
            pl.BlockSpec((heads, rows, d), lambda h: (0, 0, 0)),
            pl.BlockSpec((heads, rows, d), lambda h: (0, 0, 0)),
            pl.BlockSpec((heads, d, d), lambda h: (0, 0, 0)),
            pl.BlockSpec((heads, d, d), lambda h: (0, 0, 0)),
        ],
        scratch_shapes=[
            pltpu.VMEM((heads, rows // 128, 128, d), F32),
            pltpu.VMEM((heads, rows // 128, 128, d), F32),
            pltpu.VMEM((heads, rows // 128, 2 * d, 2 * d), F32),
            pltpu.VMEM((heads, rows // 128, 2, d), F32),
        ],
        out_shape=[
            jax.ShapeDtypeStruct((heads, rows, d), F32),
            jax.ShapeDtypeStruct((heads, rows, d), F32),
            jax.ShapeDtypeStruct((heads, d, d), F32),
            jax.ShapeDtypeStruct((heads, d, d), F32),
        ],
        cost_estimate=pl.CostEstimate(flops=30_000_000_000, bytes_accessed=4_000_000, transcendentals=0),
        compiler_params=ALL_VMEM,
        name="local_mixer",
    )(queries, keys, values, gate, corr, speed.reshape(heads, 1), plog)


def entry_state_kernel(
    t_ref, i_ref, s_ref, own, peer, ypack, zpack,
    send_c, recv_c, send_y, recv_y, send_yc, recv_yc,
    send_r, recv_r, send_l, recv_l, send_rc, recv_rc, send_lc, recv_lc,
):
    heads, d, _ = t_ref.shape
    half = d // 2
    nz, ny = zpack.shape[0], ypack.shape[0]
    z, y, c = lax.axis_index("ep_0"), lax.axis_index("ep_1"), lax.axis_index("ep_2")
    other = {"ep_2": 1 - c}
    right, left = {"ep_0": lax.rem(z + 1, nz)}, {"ep_0": lax.rem(z + nz - 1, nz)}
    across = [{"ep_1": lax.rem(y + k, ny)} for k in range(1, ny)]

    barrier = pltpu.get_barrier_semaphore()
    for who in (other, right, left, *across):
        pl.semaphore_signal(barrier, inc=1, device_id=who, device_id_type=MESH)
    pl.semaphore_wait(barrier, 3 + len(across))

    def send(src, dst, send_sem, recv_sem, who):
        return pltpu.make_async_remote_copy(
            src_ref=src, dst_ref=dst, send_sem=send_sem, recv_sem=recv_sem,
            device_id=who, device_id_type=MESH,
        )

    def store(ref, h, both):
        both = both.astype(BF16)
        ref[0, h] = both[:half]
        ref[1, h] = both[half:]

    def load(ref, h):
        return jnp.concatenate([ref[0, h], ref[1, h]], 0)

    def after(pack, so_far):
        hi, lo = halves(so_far)
        t = pack[:, :d]
        return mm(jnp.concatenate([t, t], 1), jnp.concatenate([hi, lo], 0))

    def added(pack):
        return pack[:, d:].astype(F32)

    nothing = jnp.zeros((d, d), F32)
    for h in range(heads):
        store(own, h, jnp.concatenate([t_ref[h], i_ref[h]], 1))
    swap = send(own, peer, send_c, recv_c, other)
    swap.start()
    swap.wait()
    for h in range(heads):
        mine, theirs = load(own, h), load(peer, h)
        early = jnp.where(c == 0, mine.astype(F32), theirs.astype(F32)).astype(BF16)
        late = jnp.where(c == 0, theirs.astype(F32), mine.astype(F32)).astype(BF16)
        both = mm(late[:, :d], early) + jnp.concatenate([nothing, added(late)], 1)
        store(ypack.at[y], h, both)

    out = [
        send(ypack.at[y, c], ypack.at[y, c], send_y.at[k - 1], recv_y.at[k - 1], across[k - 1])
        for k in range(1, ny)
    ]
    for copy in out:
        copy.start()
    over = []
    for k in range(1, ny):
        slot = ypack.at[lax.rem(y + ny - k, ny), c]
        out[k - 1].wait_recv()
        over.append(send(slot, slot, send_yc.at[k - 1], recv_yc.at[k - 1], other))
        over[-1].start()
    for copy in out:
        copy.wait_send()
    for copy in over:
        copy.wait()
    for h in range(heads):
        both = load(ypack.at[0], h).astype(F32)
        for k in range(1, ny):
            pack = load(ypack.at[k], h)
            both = after(pack, both) + jnp.concatenate([nothing, added(pack)], 1)
        store(zpack.at[z], h, both)

    def going(r, h, sign, who, send_sem, recv_sem):
        slot = zpack.at[lax.rem(z + nz - sign * (r - 1), nz), c, h]
        return send(slot, slot, send_sem.at[r - 1, h], recv_sem.at[r - 1, h], who)

    def shared_with_other(r, h, sign, send_sem, recv_sem):
        slot = zpack.at[lax.rem(z + nz - sign * r, nz), c, h]
        return send(slot, slot, send_sem.at[r - 1, h], recv_sem.at[r - 1, h], other)

    rings = (
        (nz // 2, 1, right, send_r, recv_r, send_rc, recv_rc),
        ((nz - 1) // 2, -1, left, send_l, recv_l, send_lc, recv_lc),
    )
    pending = []
    for rounds, sign, who, ss, rs, _, _ in rings:
        for h in range(heads):
            if rounds > 0:
                going(1, h, sign, who, ss, rs).start()
    for r in range(1, nz // 2 + 1):
        for h in range(heads):
            for rounds, sign, who, ss, rs, sc, rc in rings:
                if r > rounds:
                    continue
                copy = going(r, h, sign, who, ss, rs)
                copy.wait_recv()
                pending.append((copy, False))
                if r < rounds:
                    going(r + 1, h, sign, who, ss, rs).start()
                hand = shared_with_other(r, h, sign, sc, rc)
                hand.start()
                pending.append((hand, True))
    for copy, both_ways in pending:
        copy.wait_send()
        if both_ways:
            copy.wait_recv()

    for h in range(heads):
        s_ref[h] = nothing
    for k in range(nz - 1):
        for h in range(heads):
            pack = load(zpack.at[k], h)
            s_ref[h] = jnp.where(k < z, after(pack, s_ref[h]) + added(pack), s_ref[h])
    for k in range(ny - 1):
        for h in range(heads):
            pack = load(ypack.at[k], h)
            s_ref[h] = jnp.where(k < y, after(pack, s_ref[h]) + added(pack), s_ref[h])
    for h in range(heads):
        pack = load(peer, h)
        s_ref[h] = jnp.where(c == 1, after(pack, s_ref[h]) + added(pack), s_ref[h])


def entry_state(trans, inject):
    heads, d, _ = trans.shape
    nz, ny = lax.axis_size("ep_0"), lax.axis_size("ep_1")
    half = (2, heads, d // 2, 2 * d)
    dma = pltpu.SemaphoreType.DMA
    rounds = max(nz // 2, 1)
    vmem = pl.BlockSpec(memory_space=pltpu.VMEM)
    return pl.pallas_call(
        entry_state_kernel,
        in_specs=[vmem, vmem],
        out_specs=vmem,
        out_shape=jax.ShapeDtypeStruct((heads, d, d), F32),
        scratch_shapes=[
            pltpu.VMEM(half, BF16),
            pltpu.VMEM(half, BF16),
            pltpu.VMEM((ny, *half), BF16),
            pltpu.VMEM((nz, *half), BF16),
            dma, dma,
            dma((max(ny - 1, 1),)), dma((max(ny - 1, 1),)), dma((max(ny - 1, 1),)), dma((max(ny - 1, 1),)),
            *[dma((rounds, heads)) for _ in range(8)],
        ],
        compiler_params=pltpu.CompilerParams(
            collective_id=0, has_side_effects=True, vmem_limit_bytes=67_043_328
        ),
        cost_estimate=pl.CostEstimate(flops=30_000_000_000, bytes_accessed=4_000_000, transcendentals=0),
        name="entry_state",
    )(trans, inject)


def parts_kernel(peers, me_ref, qt_ref, ol_ref, state_ref, gain_ref, w_ref, *refs):
    far = peers // 2
    near = [r for r in range(peers) if r != far]
    count = len(near)
    hbm, refs = refs[: count + 3], refs[count + 3 :]
    out_refs, far_b, (x, gate, up, down, sems) = refs[:peers], refs[peers], refs[peers + 1 :]
    heads, rows, _ = qt_ref.shape
    tile = rows // peers
    spots = [x.at[r * tile : (r + 1) * tile] for r in range(count)] + [gate, up, down]
    copies = [
        pltpu.make_async_copy(src, dst, sems.at[k]) for k, (src, dst) in enumerate(zip(hbm, spots))
    ]
    for copy in copies:
        copy.start()
    turns = [
        pl.ds(pl.multiple_of(lax.rem(me_ref[0] + r, peers) * tile, tile), tile)
        for r in range(peers)
    ]
    normed = []
    for h in range(heads):
        qt = jnp.concatenate([qt_ref[h, at, :] for at in turns], 0)
        ol = jnp.concatenate([ol_ref[h, at, :] for at in turns], 0)
        out = dot3(qt, state_ref[h]) + ol
        out = out * lax.rsqrt(jnp.mean(out * out, axis=1, keepdims=True) + EPS) * gain_ref[...]
        normed.append(out.astype(BF16))
    mixer = mm(jnp.concatenate(normed, 1), w_ref[...]).astype(BF16)
    for r in near:
        out_refs[r][:tile] = mixer[r * tile : (r + 1) * tile]
    out_refs[far][...] = mixer[far * tile : far * tile + tile // 2]
    far_b[...] = mixer[far * tile + tile // 2 : (far + 1) * tile]
    for copy in copies:
        copy.wait()
    hidden = gated(mm(x[...], gate[...]), mm(x[...], up[...]))
    shared = mm(hidden, down[...]).astype(BF16)
    for k, r in enumerate(near):
        out_refs[r][tile:] = shared[k * tile : (k + 1) * tile]


def parts_for_peers(me, qt, ol, state, gain, w, tokens, gate, up, down):
    _, rows, d = qt.shape
    width = w.shape[1]
    peers = len(tokens) + 1
    tile = rows // peers
    vmem = pl.BlockSpec(memory_space=pltpu.VMEM)
    kept = (*tokens, gate, up, down)
    return pl.pallas_call(
        functools.partial(parts_kernel, peers),
        in_specs=[pl.BlockSpec(memory_space=pltpu.SMEM)]
        + [vmem] * 5
        + [pl.BlockSpec(memory_space=pl.ANY)] * len(kept),
        out_specs=[vmem] * (peers + 1),
        out_shape=[
            jax.ShapeDtypeStruct((tile // 2 if r in (peers // 2, peers) else 2 * tile, width), BF16)
            for r in range(peers + 1)
        ],
        scratch_shapes=[
            pltpu.VMEM((len(tokens) * tile, width), BF16),
            pltpu.VMEM(gate.shape, BF16),
            pltpu.VMEM(up.shape, BF16),
            pltpu.VMEM(down.shape, BF16),
            pltpu.SemaphoreType.DMA((len(kept),)),
        ],
        cost_estimate=pl.CostEstimate(flops=6_000_000_000, bytes_accessed=12_000_000, transcendentals=0),
        compiler_params=ALL_VMEM,
        name="parts_for_peers",
    )(me, qt, ol, state, gain.reshape(1, d), w, *kept)


def shared_part_kernel(x_ref, gate_ref, up_ref, down_hbm, out_ref, down, sem):
    load = pltpu.make_async_copy(down_hbm, down, sem)
    load.start()
    x = x_ref[...]
    hidden = gated(mm(x, gate_ref[...]), mm(x, up_ref[...]))
    load.wait()
    out_ref[...] = mm(hidden, down[...]).astype(BF16)


def shared_part(x, gate, up, down):
    vmem = pl.BlockSpec(memory_space=pltpu.VMEM)
    return pl.pallas_call(
        shared_part_kernel,
        in_specs=[vmem] * 3 + [pl.BlockSpec(memory_space=pl.ANY)],
        out_specs=vmem,
        out_shape=jax.ShapeDtypeStruct((x.shape[0], down.shape[1]), BF16),
        scratch_shapes=[pltpu.VMEM(down.shape, BF16), pltpu.SemaphoreType.DMA],
        cost_estimate=pl.CostEstimate(flops=1_000_000_000, bytes_accessed=4_000_000, transcendentals=0),
        compiler_params=ALL_VMEM,
        name="shared_part",
    )(x, gate, up, down)


def near_experts_kernel(in_ref, *refs):
    shards_ = len(refs) // 3 - 2
    hbm, (x_ref, out_ref, gates, ups, downs) = refs[: 3 * shards_], refs[3 * shards_ : -1]
    sems = refs[-1]
    rows, width = x_ref.shape
    cuts = width // LANES
    tile = 128
    copies = [
        [
            pltpu.make_async_copy(hbm[3 * m + k], held.at[m], sems.at[m, k])
            for k, held in enumerate((gates, ups, downs))
        ]
        for m in range(shards_)
    ]
    for shard in copies:
        for copy in shard:
            copy.start()
    for t in range(rows // tile):
        x_ref[t * tile : (t + 1) * tile, :] = gathered(
            in_ref[t * tile * cuts : (t + 1) * tile * cuts, :], cuts
        )
    for m in range(shards_):
        for copy in copies[m]:
            copy.wait()
        x = x_ref[...]
        part = mm(gated(mm(x, gates[m]), mm(x, ups[m])), downs[m])
        out_ref[...] = part if m == 0 else out_ref[...] + part


def near_experts(spread_in, shards_):
    weights = [w for shard in shards_ for w in shard]
    width, hidden = shards_[0][0].shape
    rows = spread_in.shape[0] * LANES // width
    count = len(shards_)
    vmem = pl.BlockSpec(memory_space=pltpu.VMEM)
    return pl.pallas_call(
        near_experts_kernel,
        in_specs=[vmem] + [pl.BlockSpec(memory_space=pl.ANY)] * len(weights),
        out_specs=[vmem, vmem],
        out_shape=[
            jax.ShapeDtypeStruct((rows, width), BF16),
            jax.ShapeDtypeStruct((rows, width), F32),
        ],
        scratch_shapes=[
            pltpu.VMEM((count, width, hidden), BF16),
            pltpu.VMEM((count, width, hidden), BF16),
            pltpu.VMEM((count, hidden, width), BF16),
            pltpu.SemaphoreType.DMA((count, 3)),
        ],
        cost_estimate=pl.CostEstimate(flops=5_000_000_000, bytes_accessed=16_000_000, transcendentals=0),
        compiler_params=ALL_VMEM,
        name="near_experts",
    )(spread_in, *weights)


def far_hidden_kernel(x_ref, gate_ref, up_ref, out_ref):
    x = x_ref[...]
    out_ref[...] = gated(mm(x, gate_ref[...]), mm(x, up_ref[...]))


def far_hidden(x, gate, up):
    vmem = pl.BlockSpec(memory_space=pltpu.VMEM)
    return pl.pallas_call(
        far_hidden_kernel,
        in_specs=[vmem] * 3,
        out_specs=vmem,
        out_shape=jax.ShapeDtypeStruct((x.shape[0], gate.shape[1]), BF16),
        cost_estimate=pl.CostEstimate(flops=1_500_000_000, bytes_accessed=4_000_000, transcendentals=0),
        compiler_params=ALL_VMEM,
        name="far_hidden",
    )(x, gate, up)


def far_out_kernel(hidden_ref, near_ref, down0_ref, down1_ref, out_ref, near, down, ready, sems):
    rows, width = near.shape
    cuts = width // LANES
    half = down.shape[0] // 2
    tile = rows // ready.shape[0]
    spans = [slice(t * tile, (t + 1) * tile) for t in range(ready.shape[0])]
    loads = [
        pltpu.make_async_copy(down0_ref, down.at[:half], sems.at[0]),
        pltpu.make_async_copy(down1_ref, down.at[half:], sems.at[1]),
    ] + [
        pltpu.make_async_copy(near_ref.at[at], near.at[at], sems.at[2 + t])
        for t, at in enumerate(spans)
    ]
    for copy in loads:
        copy.start()
    for copy in loads[:2]:
        copy.wait()
    stores = []
    for t, at in enumerate(spans):
        part = mm(hidden_ref[at, :], down[...])
        loads[2 + t].wait()
        ready[t] = spread(near[at, :] + part)
        stores.append(
            pltpu.make_async_copy(
                ready.at[t],
                out_ref.at[t * tile * cuts : (t + 1) * tile * cuts],
                sems.at[2 + len(spans) + t],
            )
        )
        stores[-1].start()
    for copy in stores:
        copy.wait()


def far_out(hidden, near, down0, down1):
    rows, width = near.shape
    cuts = width // LANES
    tiles = rows // 128
    hbm = pl.BlockSpec(memory_space=pl.ANY)
    return pl.pallas_call(
        far_out_kernel,
        in_specs=[pl.BlockSpec(memory_space=pltpu.VMEM), hbm, hbm, hbm],
        out_specs=hbm,
        out_shape=jax.ShapeDtypeStruct((rows * cuts, LANES), BF16),
        scratch_shapes=[
            pltpu.VMEM((rows, width), F32),
            pltpu.VMEM((2 * down0.shape[0], width), BF16),
            pltpu.VMEM((tiles, 128 * cuts, LANES), BF16),
            pltpu.SemaphoreType.DMA((2 + 2 * tiles,)),
        ],
        cost_estimate=pl.CostEstimate(flops=1_500_000_000, bytes_accessed=8_000_000, transcendentals=0),
        name="far_out",
    )(hidden, near, down0, down1)


def interleaving(cuts, back=False):
    i = lax.broadcasted_iota(jnp.int32, (8 * cuts, 8 * cuts), 1 if back else 0)
    j = lax.broadcasted_iota(jnp.int32, (8 * cuts, 8 * cuts), 0 if back else 1)
    return ((lax.div(i, cuts) == lax.rem(j, 8)) & (lax.rem(i, cuts) == lax.div(j, 8))).astype(BF16)


def spread(values):
    rows, width = values.shape
    cuts = width // LANES
    order = interleaving(cuts)
    blocks = [
        jnp.concatenate(
            [values[g : g + 8, c * LANES : (c + 1) * LANES] for c in range(cuts)], 0
        ).astype(BF16)
        for g in range(0, rows, 8)
    ]
    out = []
    for g in range(0, len(blocks), 2):
        two = mm(order, jnp.concatenate(blocks[g : g + 2], 1)).astype(BF16)
        out += [two[:, :LANES], two[:, LANES:]]
    return jnp.concatenate(out, 0)


def gathered(tall, cuts):
    order = interleaving(cuts, back=True)
    size = 8 * cuts
    blocks = [tall[g : g + size] for g in range(0, tall.shape[0], size)]
    out = []
    for g in range(0, len(blocks), 2):
        two = mm(order, jnp.concatenate(blocks[g : g + 2], 1))
        out += [two[:, :LANES], two[:, LANES:]]
    return jnp.concatenate(
        [jnp.concatenate([x[c * 8 : (c + 1) * 8] for x in out], 0) for c in range(cuts)], 1
    ).astype(BF16)


def dispatch_kernel(capacity, x_ref, gain_ref, routes_ref, weight_ref, xn_ref, out_ref, mix_ref):
    tokens, width = x_ref.shape
    slots = mix_ref.shape[1]
    x = x_ref[...].astype(F32)
    xn = (x * lax.rsqrt(jnp.mean(x * x, axis=1, keepdims=True) + EPS) * gain_ref[...]).astype(BF16)
    xn_ref[...] = xn
    expert = lax.broadcasted_iota(jnp.int32, (LANES, tokens), 0)
    first, second = expert == routes_ref[0:1, :], expert == routes_ref[1:2, :]
    chosen = (first | second).astype(BF16)
    token = lax.broadcasted_iota(jnp.int32, (tokens, tokens), 0)
    later = lax.broadcasted_iota(jnp.int32, (tokens, tokens), 1)
    place = mm(chosen, (token < later).astype(BF16)) + (expert * capacity).astype(F32)
    s0 = jnp.sum(jnp.where(first, place, 0.0), axis=0, keepdims=True)
    s1 = jnp.sum(jnp.where(second, place, 0.0), axis=0, keepdims=True)
    step = 128
    cuts = width // LANES
    for base in range(0, slots, step):
        slot = (lax.broadcasted_iota(jnp.int32, (step, tokens), 0) + base).astype(F32)
        is0, is1 = slot == s0, slot == s1
        out_ref[base * cuts : (base + step) * cuts, :] = spread(mm((is0 | is1).astype(BF16), xn))
        mix = jnp.where(is0, weight_ref[0:1, :], 0.0) + jnp.where(is1, weight_ref[1:2, :], 0.0)
        mix_ref[:, base : base + step] = mix.T


def dispatch(x, gain, routes, weight, slots, capacity):
    tokens, width = x.shape
    cuts = width // LANES
    return pl.pallas_call(
        functools.partial(dispatch_kernel, capacity),
        out_shape=[
            jax.ShapeDtypeStruct((tokens, width), BF16),
            jax.ShapeDtypeStruct((slots * cuts, LANES), BF16),
            jax.ShapeDtypeStruct((tokens, slots), F32),
        ],
        name="dispatch",
    )(x, gain.reshape(1, width), routes, weight)


def sums_kernel(*refs):
    *part_refs, mixer_ref, shared_ref = refs
    tokens = mixer_ref.shape[0]
    mixer, shared = [part_refs[0][at].astype(F32) for at in (slice(tokens), slice(tokens, None))]
    for part in part_refs[1:]:
        mixer = mixer + part[:tokens].astype(F32)
        shared = shared + part[tokens:].astype(F32)
    mixer_ref[...] = mixer.astype(BF16)
    shared_ref[...] = shared


def sums_of_parts(parts):
    tokens, width = parts[0].shape[0] // 2, parts[0].shape[1]
    tile = 512
    out = pl.BlockSpec((tokens, tile), lambda c: (0, c))
    return pl.pallas_call(
        sums_kernel,
        grid=(width // tile,),
        in_specs=[pl.BlockSpec((2 * tokens, tile), lambda c: (0, c))] * len(parts),
        out_specs=[out, out],
        out_shape=[
            jax.ShapeDtypeStruct((tokens, width), BF16),
            jax.ShapeDtypeStruct((tokens, width), F32),
        ],
        cost_estimate=pl.CostEstimate(flops=1_000_000_000, bytes_accessed=6_000_000, transcendentals=0),
        compiler_params=ALL_VMEM,
        name="sums_of_parts",
    )(*parts)


def joined_kernel(right_ref, left_ref, a_ref, b_ref, right_out, left_out):
    half = a_ref.shape[0]
    rows = right_ref.shape[0]
    right_out[:half] = (right_ref[:half].astype(F32) + a_ref[...].astype(F32)).astype(BF16)
    right_out[half:] = right_ref[half:]
    left_out[:half] = left_ref[:half]
    left_out[half : 2 * half] = (
        left_ref[half : 2 * half].astype(F32) + b_ref[...].astype(F32)
    ).astype(BF16)
    left_out[2 * half : rows] = left_ref[2 * half : rows]


def joined(right, left, a, b):
    rows, width = right.shape
    tile = 512
    whole = pl.BlockSpec((rows, tile), lambda c: (0, c))
    half = pl.BlockSpec((a.shape[0], tile), lambda c: (0, c))
    return pl.pallas_call(
        joined_kernel,
        grid=(width // tile,),
        in_specs=[whole, whole, half, half],
        out_specs=[whole, whole],
        out_shape=[jax.ShapeDtypeStruct(right.shape, BF16)] * 2,
        cost_estimate=pl.CostEstimate(flops=500_000_000, bytes_accessed=5_000_000, transcendentals=0),
        compiler_params=ALL_VMEM,
        name="joined",
    )(right, left, a, b)


def combine_kernel(
    shared_hbm, late_hbm, back_hbm, mix_hbm, out_hbm, shared, late, back, mix, out, sems
):
    tiles = back.shape[0]
    width = shared.shape[1]
    cuts = width // LANES
    tile = back.shape[1] // cuts
    loads = [
        pltpu.make_async_copy(
            back_hbm.at[t * tile * cuts : (t + 1) * tile * cuts], back.at[t], sems.at[t]
        )
        for t in range(tiles)
    ]
    loads.insert(1, pltpu.make_async_copy(mix_hbm, mix, sems.at[tiles]))
    loads.append(pltpu.make_async_copy(shared_hbm, shared, sems.at[tiles + 1]))
    loads.append(pltpu.make_async_copy(late_hbm, late, sems.at[tiles + 2]))
    for copy in loads:
        copy.start()
    rows = []
    for t, count in enumerate((2,) + (1,) * (tiles - 1)):
        for _ in range(count):
            loads.pop(0).wait()
        rows.append(gathered(back[t], cuts))
    for copy in loads:
        copy.wait()
    rows = jnp.concatenate(rows, 0)
    hi, lo = halves(mix[...])
    both = jnp.concatenate([hi, lo], 1)
    stores = []
    for k in range(2):
        at = slice(k * width // 2, (k + 1) * width // 2)
        part = jnp.concatenate([rows[:, at], rows[:, at]], 0)
        total = shared[:, at] + late[:, at].astype(F32)
        out[:, at] = (total + mm(both, part)).astype(BF16)
        stores.append(pltpu.make_async_copy(out.at[:, at], out_hbm.at[:, at], sems.at[tiles + 3 + k]))
        stores[-1].start()
    for copy in stores:
        copy.wait()


def combine(shared, late, back, mix):
    tokens, width = shared.shape
    cuts = width // LANES
    tile = 128
    tiles = mix.shape[1] // tile
    hbm = pl.BlockSpec(memory_space=pl.ANY)
    return pl.pallas_call(
        combine_kernel,
        in_specs=[hbm] * 4,
        out_specs=hbm,
        out_shape=jax.ShapeDtypeStruct((tokens, width), BF16),
        scratch_shapes=[
            pltpu.VMEM((tokens, width), F32),
            pltpu.VMEM((tokens, width), BF16),
            pltpu.VMEM((tiles, tile * cuts, LANES), BF16),
            pltpu.VMEM(mix.shape, F32),
            pltpu.VMEM((tokens, width), BF16),
            pltpu.SemaphoreType.DMA((tiles + 5,)),
        ],
        compiler_params=ALL_VMEM,
        name="combine",
    )(shared, late, back, mix)


def ring(axis):
    peers = lax.axis_size(axis)
    return (
        [(i, (i + 1) % peers) for i in range(peers)],
        [(i, (i - 1) % peers) for i in range(peers)],
    )


def neighbours_shards(shard, axis):
    right, left = ring(axis)
    from_left = [lax.ppermute(w, axis, right) for w in shard]
    from_right = [lax.ppermute(w, axis, left) for w in shard]
    return from_left, from_right


def far_shard(from_left, from_right, axis):
    right, left = ring(axis)
    half = from_left[2].shape[0] // 2
    return (
        lax.ppermute(from_left[0], axis, right),
        lax.ppermute(from_right[1], axis, left),
        lax.ppermute(from_left[2][:half], axis, right),
        lax.ppermute(from_right[2][half:], axis, left),
    )


def gated(gate_val, up_val):
    return (jax.nn.silu(gate_val) * up_val).astype(BF16)


def shards(
    queries,
    keys,
    values,
    decay_gate_logits,
    correction_logits,
    head_decay_speed,
    position_log_decay,
    head_output_gain,
    mixer_output_weight,
    expert_input_tokens,
    expert_norm_gain,
    routes,
    chosen_expert_weight,
    routed_gate_weight,
    routed_up_weight,
    routed_down_weight,
    common_gate_weight,
    common_up_weight,
    common_down_weight,
):
    experts = lax.axis_size(EP)
    tokens, _ = expert_input_tokens.shape
    own = (routed_gate_weight[0], routed_up_weight[0], routed_down_weight[0])
    from_left, from_right = neighbours_shards(own, "tp")

    capacity = 3 * tokens * routes.shape[1] // (2 * experts)
    xn, outgoing, mix = dispatch(
        expert_input_tokens,
        expert_norm_gain,
        routes.T,
        chosen_expert_weight.T,
        experts * capacity,
        capacity,
    )

    def to_peers(x):
        parts = x.reshape(experts, -1, LANES)
        return lax.all_to_all(parts, EP, split_axis=0, concat_axis=0, tiled=True).reshape(-1, LANES)

    peers = lax.axis_size("tp")

    def shift(r):
        return [(i, (i + r) % peers) for i in range(peers)]

    arrived = to_peers(outgoing)
    opposite = peers // 2
    near_peers = [r for r in range(1, peers) if r != opposite]
    group = [xn] + [lax.ppermute(xn, "tp", shift(peers - r)) for r in near_peers]

    qt, ol, trans, inject = local_mixer(
        queries,
        keys,
        values,
        decay_gate_logits.T,
        correction_logits.T,
        head_decay_speed,
        position_log_decay.T,
    )
    state = entry_state(trans, inject)
    state, from_left, from_right = lax.optimization_barrier((state, from_left, from_right))
    far = far_shard(from_left, from_right, "tp")
    me = lax.axis_index("tp").astype(jnp.int32).reshape(1)
    parts = parts_for_peers(
        me,
        qt,
        ol,
        state,
        head_output_gain,
        mixer_output_weight,
        group,
        common_gate_weight,
        common_up_weight,
        common_down_weight,
    )
    rows, near = near_experts(arrived, (own, from_left, from_right))
    hidden = far_hidden(rows, *far[:2])
    parts, far, near, hidden, xn = lax.optimization_barrier((parts, far, near, hidden, xn))
    far_xn = lax.ppermute(xn, "tp", shift(opposite))
    far_a = lax.ppermute(parts[opposite], "tp", shift(1))
    far_b = lax.ppermute(parts[peers], "tp", shift(peers - 1))
    slot_sums = far_out(hidden, near, *far[2:])
    back = to_peers(slot_sums)
    far_xn, far_a, slot_sums = lax.optimization_barrier((far_xn, far_a, slot_sums))
    to_right, to_left = joined(parts[1], parts[peers - 1], far_a, far_b)
    got = [
        parts[0],
        lax.ppermute(to_right, "tp", shift(1)),
        lax.ppermute(to_left, "tp", shift(peers - 1)),
    ]
    late = shared_part(far_xn, common_gate_weight, common_up_weight, common_down_weight)
    far_shared = lax.ppermute(late, "tp", shift(opposite))
    mixer_out, shared = sums_of_parts(got)
    return (mixer_out, combine(shared, far_shared, back, mix))


def solution(mesh):
    finer = Mesh(mesh.devices.reshape(8, 4, 2, mesh.shape["tp"]), ("ep_0", "ep_1", "ep_2", "tp"))
    placed = (
        P(EP, "tp"),
        P(EP, "tp"),
        P(EP, "tp"),
        P(EP, "tp"),
        P(EP, "tp"),
        P("tp"),
        P(EP, "tp"),
        P(),
        P("tp", None),
        P(EP_TP, None),
        P(),
        P(EP_TP, None),
        P(EP_TP, None),
        P(EP, None, "tp"),
        P(EP, None, "tp"),
        P(EP, "tp", None),
        P(None, "tp"),
        P(None, "tp"),
        P("tp", None),
    )
    return jax.shard_map(
        shards,
        mesh=finer,
        in_specs=placed,
        out_specs=(P(EP_TP, None), P(EP_TP, None)),
        check_vma=False,
    )
```
